512 devices in a mesh: ep: 32 (over z, x), tp: 16 (over y, core).
Axes of the slice: x: 4, y: 8, z: 8, core: 2. Of those that a mesh axis runs over, the one named last changes fastest.
Arguments:
- query_rows: bfloat16 [16384, 3072], P('ep', 'tp'), may hold values from -6 to 6
- key_rows: bfloat16 [16384, 1024], P('ep', 'tp'), may hold values from -6 to 6
- value_rows: bfloat16 [16384, 1024], P('ep', 'tp'), may hold values from -6 to 6
- query_gain: float32 [48, 64], P('tp'), may hold values from 0.4 to 48
- key_gain: float32 [16, 64], P('tp'), may hold values from 0.1 to 1.9
- sink_logits: float32 [48], P('tp'), may hold values from 1 to 6
- out_weight: bfloat16 [3072, 2048], P('tp'), may hold values from -0.109375 to 0.109375
- expert_input: bfloat16 [16384, 2048], P(('ep', 'tp')), may hold values from -6 to 6
- expert_gain: float32 [2048], replicated, may hold values from 0.1 to 1.9
- routes: int32 [16384, 2], P(('ep', 'tp')), may hold values from 0 to 31, all different within a row; in each aligned block of 32 rows (0 to 31, 32 to 63, ...) at most 3 rows name the same one
- route_logits: float32 [16384, 2], P(('ep', 'tp')), may hold values from -6 to 6
- gate_weight: bfloat16 [32, 2048, 2048], P('ep', None, 'tp'), may hold values from -0.375 to 0.375
- up_weight: bfloat16 [32, 2048, 2048], P('ep', None, 'tp'), may hold values from -0.375 to 0.375
- down_weight: bfloat16 [32, 2048, 2048], P('ep', 'tp'), may hold values from -0.01953125 to 0.01953125
Outputs:
- attended: bfloat16 [16384, 2048], P(('ep', 'tp'))
- expert_mix: bfloat16 [16384, 2048], P(('ep', 'tp'))
The draws below stay inside these ranges and needn't reach their ends.
Inputs may be any that keep to these rules, and one draw needn't show every extreme that they name: `routes`: each row names 2 different experts; in the rows of one device no expert is named more than 3 times, and in some device one expert is named exactly 3 times.
All inputs are finite; a program needn't handle non-finite values.
Results may differ from the reference program's by a relative error of at most 0.017.
The reference program's roundings to bfloat16 on the way count: a program that leaves them out, or rounds other values in their place, can miss the bound.
Values may be sent and summed in bfloat16 or wider, within the bound.
A program may use at most 64 MiB of HBM per device.

```python
import math
import jax
import jax.numpy as jnp
import numpy as np
from jax import lax

WIDTH = 2048
QHEADS = 48
KVHEADS = 16
HEADDIM = 64
FFN = 2048
EXPERTS = 32
TOPK = 2
WINDOW = 128
TOKENS = 16384
ROWS_DEV = 32
CAP = 3
N_TP = 16


def draw_query_gain(key, part):
    head_key, spread_key = jax.random.split(key)
    head_scale = jnp.exp(jax.random.uniform(head_key, (QHEADS, 1), jnp.float32, math.log(0.7), math.log(3.0)))
    spread = 1.0 + 0.18 * jax.random.uniform(spread_key, (QHEADS, HEADDIM), jnp.float32, -1.0, 1.0)
    return head_scale * spread


def levels(stream_key, dims, pieces, least, high):
    factor_of = 1.0
    for dim, parts in pieces:
        draws = jax.random.uniform(jax.random.fold_in(jax.random.fold_in(stream_key, 6), dim), (parts,), jnp.float32, least / len(pieces), high / len(pieces))
        factor_of = factor_of * jnp.repeat(jnp.exp(draws), dims[dim] // parts).reshape((-1,) + (1,) * (len(dims) - 1 - dim))
    return factor_of


def assign_block(own_key, own, number, rows, number_of, top, bound, lean):
    sequence = jax.random.permutation(own_key, number_of)
    packed, ordinary = load_shares(number_of, rows * top, bound, lean, True), load_shares(number_of, rows * top, bound, lean, False)
    places = jnp.arange(number_of)

    def named(lengths, rotation):
        used = int((lengths > 0).sum())
        fixed = max(1, used // 4)
        passed = fixed + (places - fixed + rotation * (used - fixed)) % max(1, number_of - fixed)
        return jnp.zeros((number_of,), jnp.int32).at[sequence[jnp.where(places < fixed, places, passed)]].set(jnp.asarray(lengths, jnp.int32))

    lengths = jnp.where(number % 4 == 0, named(packed, number // 4), named(ordinary, number - number // 4 - 1))
    mixed = jax.random.permutation(jax.random.fold_in(own, 3), number_of)
    source_of, receiver = mixed[0:number_of // 2 * 2:2], mixed[1:number_of // 2 * 2:2]
    room = jnp.minimum(lengths[source_of] - 1, bound - lengths[receiver]) // 2
    room = jnp.where((source_of == sequence[0]) | (receiver == sequence[0]) | (lengths[receiver] == 0), 0, jnp.maximum(room, 0))
    passed = jax.random.randint(jax.random.fold_in(own, 4), (number_of // 2,), 0, 1 << 20) % (room + 1)
    lengths = lengths.at[source_of].add(-passed).at[receiver].add(passed)
    labels = jnp.searchsorted(jnp.cumsum(lengths), jnp.arange(rows * top), side="right").astype(jnp.int32)
    table = labels.reshape(top, rows).T
    table = table[jax.random.permutation(jax.random.fold_in(own, 1), rows)]
    rotation = jax.random.randint(jax.random.fold_in(own, 2), (rows, 1), 0, top)
    return jnp.take_along_axis(table, (jnp.arange(top)[None, :] + rotation) % top, axis=1)


def load_shares(amount, total, most, skew, full):
    loads = [(1 << 20) // math.isqrt(standing ** skew) + 1 for standing in range(1, amount + 1)]
    largest = most if full else min(most, max(-(-total // amount), total * loads[0] // sum(loads)))
    least = 1 if total - largest >= amount - 1 else 0
    given, spare = [largest] + [least] * (amount - 1), total - largest - least * (amount - 1)
    while spare > 0:
        free = [i for i in range(1, amount) if given[i] < largest] or [i for i in range(1, amount) if given[i] < most]
        whole, remaining = sum([loads[i] for i in free]), spare
        for i in free:
            extra = min(most - given[i], max(1, remaining * loads[i] // whole), spare)
            given[i] = given[i] + extra
            spare = spare - extra
    return np.array(given)


def normal_values(key, shape, scale, reach, pieces=(), kind=jnp.bfloat16):
    array = jax.random.normal(key, shape, jnp.float32) * scale
    if len(pieces) > 0:
        array = levels(key, shape, pieces, -0.22, 0.18) * array
    return jnp.clip(array, min=-reach, max=reach).astype(kind)


def setup_inputs(seed: int = 0) -> dict:
    arg_keys = jax.random.split(jax.random.key(seed), 15)
    query_rows = normal_values(arg_keys[0], (TOKENS, QHEADS * HEADDIM), 1.0, 6.0, ((0, 32), (1, 16)))
    key_rows = normal_values(arg_keys[1], (TOKENS, KVHEADS * HEADDIM), 1.0, 6.0, ((0, 32), (1, 16)))
    value_rows = normal_values(arg_keys[2], (TOKENS, KVHEADS * HEADDIM), 1.0, 6.0, ((0, 32), (1, 16)))
    query_gain = draw_query_gain(jax.random.fold_in(arg_keys[14], 71), 0)
    key_gain = jnp.clip(1.0 + 0.18 * jax.random.normal(arg_keys[4], (KVHEADS, HEADDIM), jnp.float32), 0.1, 1.9)
    sink_logits = jnp.clip(1.0 + 5.0 * jax.random.uniform(arg_keys[5], (QHEADS,), jnp.float32) ** levels(arg_keys[5], (QHEADS,), ((0, 16),), -0.2, 0.2), 1.0, 6.0)
    out_weight = normal_values(arg_keys[6], (QHEADS * HEADDIM, WIDTH), (QHEADS * HEADDIM) ** -0.5, 0.109375, ((0, 16),))
    expert_input = normal_values(arg_keys[7], (TOKENS, WIDTH), 1.0, 6.0, ((0, 512),))
    expert_gain = jnp.clip(1.0 + 0.18 * jax.random.normal(arg_keys[8], (WIDTH,), jnp.float32), 0.1, 1.9)
    routes_keys = jax.random.split(jax.random.fold_in(arg_keys[9], 1), TOKENS // ROWS_DEV)
    routes_turns = jax.random.permutation(jax.random.fold_in(arg_keys[9], 3), TOKENS // ROWS_DEV)
    routes = jax.vmap(lambda own, number: assign_block(jax.random.fold_in(arg_keys[9], 2), own, number, ROWS_DEV, EXPERTS, TOPK, CAP, 1))(routes_keys, routes_turns).reshape((TOKENS, TOPK))
    route_logits = normal_values(arg_keys[10], (TOKENS, TOPK), 1.0, 6.0, ((0, 512),), jnp.float32)
    gate_weight = normal_values(arg_keys[11], (EXPERTS, WIDTH, FFN), (WIDTH // 9) ** -0.5, 0.375, ((0, 32), (2, 16)))
    up_weight = normal_values(arg_keys[12], (EXPERTS, WIDTH, FFN), (WIDTH // 9) ** -0.5, 0.375, ((0, 32), (2, 16)))
    down_weight = normal_values(arg_keys[13], (EXPERTS, FFN, WIDTH), (45 * FFN) ** -0.5, 0.01953125, ((0, 32), (1, 16)))
    return dict(query_rows=query_rows, key_rows=key_rows, value_rows=value_rows, query_gain=query_gain, key_gain=key_gain, sink_logits=sink_logits, out_weight=out_weight, expert_input=expert_input, expert_gain=expert_gain, routes=routes, route_logits=route_logits, gate_weight=gate_weight, up_weight=up_weight, down_weight=down_weight)


EPSILON = 1e-06
CLAMP_LIMIT = 7.0
ACT_SLOPE = 1.702
NEGATIVE = -1e+30

def head_norm(row_data, gain_table):
    head_count, head_size = gain_table.shape
    widened = row_data.astype(jnp.float32).reshape(row_data.shape[0], head_count, head_size)
    scaled = widened * lax.rsqrt(lax.optimization_barrier(jnp.mean(widened * widened, axis=-1, keepdims=True)) + EPSILON)
    return (scaled * gain_table).astype(jnp.bfloat16)

def band(padded, blocks):
    tiled = padded.reshape((blocks + 1, WINDOW) + padded.shape[1:])
    return jnp.concatenate([tiled[:-1], tiled[1:]], axis=1)

def blockwise_product(left, right):
    row_total = left.shape[0]
    inner_width = left.shape[1] // N_TP
    left_parts = jnp.transpose(left.reshape(row_total, N_TP, inner_width), (1, 0, 2))
    right_parts = right.reshape(N_TP, inner_width, right.shape[1])

    def accumulate(running, operands):
        left_part, right_part = operands
        partial_value = jnp.dot(left_part, right_part, preferred_element_type=jnp.float32).astype(jnp.bfloat16)
        partial_value = lax.optimization_barrier(partial_value)
        return (running + partial_value.astype(jnp.float32), None)
    running, unused = lax.scan(accumulate, jnp.zeros((row_total, right.shape[1]), jnp.float32), (left_parts, right_parts))
    return running.astype(jnp.bfloat16)

def attention(query_rows, key_rows, value_rows, query_gain, key_gain, sink_logits):
    seq_rows = query_rows.shape[0]
    blocks = seq_rows // WINDOW
    group_size = QHEADS // KVHEADS
    query_hat = head_norm(query_rows, query_gain).reshape(blocks, WINDOW, KVHEADS, group_size, HEADDIM)
    key_hat = head_norm(key_rows, key_gain)
    value_hat = value_rows.reshape(seq_rows, KVHEADS, HEADDIM)
    leading = jnp.zeros((WINDOW, KVHEADS, HEADDIM), jnp.bfloat16)
    key_band = band(jnp.concatenate([leading, key_hat], axis=0), blocks)
    value_band = band(jnp.concatenate([leading, value_hat], axis=0), blocks)
    query_pos = jnp.arange(WINDOW, dtype=jnp.int32)[:, None]
    key_pos = jnp.arange(2 * WINDOW, dtype=jnp.int32)[None, :]
    distance = query_pos + WINDOW - key_pos
    inside = (distance >= 0) & (distance < WINDOW)
    first_block = (jnp.arange(blocks, dtype=jnp.int32) == 0)[:, None, None]
    allowed = inside[None] & ~(first_block & (key_pos < WINDOW)[None])

    def one_head(operands):
        query_part, key_part, value_part, sink_part = operands
        scores = jnp.einsum('bqgd,bjd->bgqj', query_part.astype(jnp.float32), key_part.astype(jnp.float32), precision=lax.Precision.HIGHEST) * HEADDIM ** (-0.5)
        scores = jnp.where(allowed[:, None], scores, NEGATIVE)
        sink_table = sink_part.reshape(1, group_size, 1, 1)
        highest = jnp.maximum(lax.optimization_barrier(jnp.max(scores, axis=-1, keepdims=True)), sink_table)
        weights = jnp.exp(scores - highest)
        total = lax.optimization_barrier(jnp.sum(weights, axis=-1, keepdims=True)) + jnp.exp(sink_table - highest)
        rounded = lax.optimization_barrier(weights.astype(jnp.bfloat16))
        mixed = jnp.einsum('bgqj,bjd->bgqd', rounded.astype(jnp.float32), value_part.astype(jnp.float32), precision=lax.Precision.HIGHEST)
        return (mixed / total).astype(jnp.bfloat16)
    heads_out = lax.map(one_head, (jnp.transpose(query_hat, (2, 0, 1, 3, 4)), jnp.transpose(key_band, (2, 0, 1, 3)), jnp.transpose(value_band, (2, 0, 1, 3)), sink_logits.reshape(KVHEADS, group_size)))
    return jnp.transpose(heads_out, (1, 3, 0, 2, 4)).reshape(seq_rows, QHEADS * HEADDIM)

def slot_maps(route_block):
    flat_routes = route_block.reshape(-1).astype(jnp.int32)
    expert_hot = (flat_routes[:, None] == jnp.arange(EXPERTS, dtype=jnp.int32)[None, :]).astype(jnp.int32)
    before = jnp.cumsum(expert_hot, axis=0) - expert_hot
    return (flat_routes, lax.optimization_barrier(jnp.sum(before * expert_hot, axis=1)).astype(jnp.int32))

def experts_part(expert_input, expert_gain, routes, route_logits, gate_weight, up_weight, down_weight):
    token_count = expert_input.shape[0]
    block_count = token_count // ROWS_DEV
    widened = expert_input.astype(jnp.float32)
    normed = (widened * lax.rsqrt(lax.optimization_barrier(jnp.mean(widened * widened, axis=-1, keepdims=True)) + EPSILON) * expert_gain).astype(jnp.bfloat16)
    route_weight = jax.nn.softmax(route_logits, axis=-1)
    flat_routes, position = jax.vmap(slot_maps)(routes.reshape(block_count, ROWS_DEV, TOPK))
    row_index = jnp.repeat(jnp.arange(ROWS_DEV, dtype=jnp.int32), TOPK)
    block_index = jnp.arange(block_count, dtype=jnp.int32)[:, None]
    sources = jnp.broadcast_to(row_index[None], flat_routes.shape) + block_index * ROWS_DEV
    table = jnp.full((block_count, EXPERTS, CAP), -1, jnp.int32).at[block_index, flat_routes, position].set(sources)
    tables = jnp.transpose(table, (1, 0, 2)).reshape(EXPERTS, block_count * CAP)

    def one_expert(operands):
        slot_index, gate_part, up_part, down_part = operands
        picked = jnp.where((slot_index >= 0)[:, None], normed[jnp.maximum(slot_index, 0).astype(jnp.int32)], jnp.zeros((), jnp.bfloat16))
        gate_pre = jnp.dot(picked, gate_part, preferred_element_type=jnp.float32)
        up_pre = jnp.dot(picked, up_part, preferred_element_type=jnp.float32)
        clipped = jnp.minimum(gate_pre, CLAMP_LIMIT)
        linear = jnp.clip(up_pre, -CLAMP_LIMIT, CLAMP_LIMIT)
        hidden_units = (clipped * jax.nn.sigmoid(ACT_SLOPE * clipped) * (linear + 1.0)).astype(jnp.bfloat16)
        return blockwise_product(hidden_units, down_part)
    outputs = lax.map(one_expert, (tables, gate_weight, up_weight, down_weight))
    slot_place = (block_index * CAP + position).astype(jnp.int32)
    gathered = outputs[flat_routes, slot_place]
    weighted = gathered.astype(jnp.float32).reshape(block_count, ROWS_DEV, TOPK, WIDTH) * route_weight.reshape(block_count, ROWS_DEV, TOPK, 1)
    return lax.optimization_barrier(jnp.sum(weighted, axis=2)).reshape(token_count, WIDTH).astype(jnp.bfloat16)

def reference(query_rows, key_rows, value_rows, query_gain, key_gain, sink_logits, out_weight, expert_input, expert_gain, routes, route_logits, gate_weight, up_weight, down_weight):
    heads_out = attention(query_rows, key_rows, value_rows, query_gain, key_gain, sink_logits)
    attended = blockwise_product(heads_out, out_weight)
    expert_mix = experts_part(expert_input, expert_gain, routes, route_logits, gate_weight, up_weight, down_weight)
    return (attended, expert_mix)
```

```python
import jax
import jax.numpy as jnp
from jax import lax
from jax.experimental import pallas as pl
from jax.experimental.pallas import tpu as pltpu
from jax.sharding import PartitionSpec as P

EXPERTS = 32
WINDOW = 128


EPSILON = 1e-06
CLAMP_LIMIT = 7.0
ACT_SLOPE = 1.702
NEGATIVE = -1e30


def shifted(value, axis, steps):
    count = lax.axis_size(axis)
    initial, last = (max(0, -steps), min(count, count - steps))
    return lax.ppermute(value, axis, [(source, source + steps) for source in range(initial, last)])


def head_norm(row_data, gain_table):
    head_count, head_size = gain_table.shape
    widened = row_data.astype(jnp.float32).reshape(row_data.shape[0], head_count, head_size)
    scaled = widened * lax.rsqrt(jnp.mean(widened * widened, axis=-1, keepdims=True) + EPSILON)
    return (scaled * gain_table).astype(jnp.bfloat16)


def band(padded, blocks):
    tiled = padded.reshape((blocks + 1, WINDOW) + padded.shape[1:])
    return jnp.concatenate([tiled[:-1], tiled[1:]], axis=1)


def attend(query_rows, key_rows, value_rows, query_gain, key_gain, sink_logits):
    seq_rows = query_rows.shape[0]
    key_heads, head_size = key_gain.shape
    group_size = query_gain.shape[0] // key_heads
    blocks = seq_rows // WINDOW
    query_hat = head_norm(query_rows, query_gain).reshape(
        blocks, WINDOW, key_heads, group_size, head_size
    )
    key_hat = head_norm(key_rows, key_gain)
    value_hat = value_rows.reshape(seq_rows, key_heads, head_size)
    tail_rows = jnp.stack([key_hat[seq_rows - WINDOW :], value_hat[seq_rows - WINDOW :]])
    earlier = shifted(tail_rows, "ep", 1)
    key_band = band(jnp.concatenate([earlier[0], key_hat], axis=0), blocks)
    value_band = band(jnp.concatenate([earlier[1], value_hat], axis=0), blocks)
    query_pos = lax.broadcasted_iota(jnp.int32, (WINDOW, 2 * WINDOW), 0)
    key_pos = lax.broadcasted_iota(jnp.int32, (WINDOW, 2 * WINDOW), 1)
    distance = query_pos + WINDOW - key_pos
    inside = (distance >= 0) & (distance < WINDOW)
    first_block = (lax.broadcasted_iota(jnp.int32, (blocks, 1, 1), 0) == 0) & (
        lax.axis_index("ep") == 0
    )
    allowed = inside[None] & ~(first_block & (key_pos < WINDOW)[None])
    scores = jnp.einsum(
        "bqkgd,bjkd->bkgqj", query_hat, key_band, preferred_element_type=jnp.float32
    ) * head_size ** (-0.5)
    scores = jnp.where(allowed[:, None, None], scores, NEGATIVE)
    sink_table = sink_logits.reshape(1, key_heads, group_size, 1, 1)
    highest = jnp.maximum(jnp.max(scores, axis=-1, keepdims=True), sink_table)
    weights = jnp.exp(scores - highest)
    total = jnp.sum(weights, axis=-1, keepdims=True) + jnp.exp(sink_table - highest)
    mixed = jnp.einsum(
        "bkgqj,bjkd->bkgqd",
        weights.astype(jnp.bfloat16),
        value_band,
        preferred_element_type=jnp.float32,
    )
    mixed = (mixed / total).astype(jnp.bfloat16)
    return jnp.transpose(mixed, (0, 3, 1, 2, 4)).reshape(seq_rows, -1)


def slot_maps(route_block, capacity):
    flat_routes = route_block.reshape(-1)
    expert_hot = (flat_routes[:, None] == lax.broadcasted_iota(jnp.int32, (1, EXPERTS), 1)).astype(
        jnp.int32
    )
    before = jnp.cumsum(expert_hot, axis=0) - expert_hot
    position = jnp.sum(before * expert_hot, axis=1)
    place_hot = (position[:, None] == lax.broadcasted_iota(jnp.int32, (1, capacity), 1)).astype(
        jnp.float32
    )
    row_total, fanout = route_block.shape
    return (
        expert_hot.astype(jnp.float32).reshape(row_total, fanout, EXPERTS),
        place_hot.reshape(row_total, fanout, capacity),
    )


def dispatch_matrix(route_block, capacity):
    expert_hot, place_hot = slot_maps(route_block, capacity)
    return jnp.einsum("rke,rkc->ecr", expert_hot, place_hot).astype(jnp.bfloat16)


def combine_matrix(route_block, route_weight, capacity):
    expert_hot, place_hot = slot_maps(route_block, capacity)
    return jnp.einsum("rke,rkc,rk->rec", expert_hot, place_hot, route_weight)


CHAINS = ((0, 1, 4), (0, -1, 3), (1, 1, 3), (1, -1, 4))
HOPS = {}
for _half, _way, _far in CHAINS:
    for _hop in range(1, _far + 1):
        HOPS[_half, _way, _hop] = len(HOPS)
VMEM_LIMIT = 60 * 1024 * 1024


def remote(source, target, send_sem, recv_sem, where):
    return pltpu.make_async_remote_copy(
        src_ref=source,
        dst_ref=target,
        send_sem=send_sem,
        recv_sem=recv_sem,
        device_id=where,
        device_id_type=pl.DeviceIdType.MESH,
    )


def greet(places):
    barrier = pltpu.get_barrier_semaphore()
    for place in places:
        pl.semaphore_signal(
            barrier, inc=1, device_id=place, device_id_type=pl.DeviceIdType.MESH
        )
    pl.semaphore_wait(barrier, len(places))


def exchange_kernel(axis, count, x_ref, out_ref, send_sem, recv_sem):
    me = lax.axis_index(axis)
    barrier = pltpu.get_barrier_semaphore()

    def hello(step, carry):
        place = {axis: lax.rem(me + step, count)}
        pl.semaphore_signal(
            barrier, inc=1, device_id=place, device_id_type=pl.DeviceIdType.MESH
        )
        return carry

    lax.fori_loop(1, count, hello, 0)
    pl.semaphore_wait(barrier, count - 1)

    def copy_for(step):
        peer = lax.rem(me + step, count)
        return remote(
            x_ref.at[peer], out_ref.at[me], send_sem.at[step], recv_sem.at[step], {axis: peer}
        )

    def begin(step, carry):
        copy_for(step).start()
        return carry

    def end(step, carry):
        copy_for(step).wait()
        return carry

    lax.fori_loop(1, count, begin, 0)
    out_ref[me] = x_ref[me]
    lax.fori_loop(1, count, end, 0)


def exchange(value, axis, collective_id):
    count = value.shape[0]
    return pl.pallas_call(
        lambda *refs: exchange_kernel(axis, count, *refs),
        out_shape=jax.ShapeDtypeStruct(value.shape, value.dtype),
        in_specs=[pl.BlockSpec(memory_space=pltpu.VMEM)],
        out_specs=pl.BlockSpec(memory_space=pltpu.VMEM),
        scratch_shapes=[
            pltpu.SemaphoreType.DMA((count,)),
            pltpu.SemaphoreType.DMA((count,)),
        ],
        compiler_params=pltpu.CompilerParams(
            collective_id=collective_id, has_side_effects=True
        ),
        cost_estimate=pl.CostEstimate(
            flops=100000000, bytes_accessed=2 * value.size * 2, transcendentals=0
        ),
        name="exchange_" + axis,
    )(value)


def ring_kernel(
    x_ref,
    gate_ref,
    up_ref,
    down_ref,
    out_ref,
    w1,
    w2,
    xbuf,
    pbuf,
    rbuf,
    wl_sem,
    ws_sem,
    wr_sem,
    gs_sem,
    gr_sem,
    ss_sem,
    sr_sem,
):
    tp = lax.axis_index("tp")
    ring = lax.axis_size("tp") // 2
    core = lax.rem(tp, 2)
    spot = lax.div(tp, 2)
    ahead = {"tp": lax.rem(spot + 1, ring) * 2 + core}
    behind = {"tp": lax.rem(spot + ring - 1, ring) * 2 + core}
    partner = {"tp": spot * 2 + (1 - core)}
    rows = x_ref.shape[0]
    part = rows // 2
    inner = down_ref.shape[1]
    local = [
        pltpu.make_async_copy(gate_ref.at[0], w1.at[:, pl.ds(0, inner)], wl_sem.at[0]),
        pltpu.make_async_copy(up_ref.at[0], w1.at[:, pl.ds(2 * inner, inner)], wl_sem.at[1]),
        pltpu.make_async_copy(down_ref.at[0], w2.at[pl.ds(0, inner)], wl_sem.at[2]),
    ]
    for copy in local:
        copy.start()
    greet((ahead, behind, partner))

    def half_rows(half):
        return pl.ds(half * part, part)

    def gather_copy(half, way, hop):
        slot = (-way * (hop - 1)) % ring
        source = x_ref.at[half_rows(half)] if hop == 1 else xbuf.at[slot, half_rows(half)]
        number = HOPS[half, way, hop]
        return remote(
            source,
            xbuf.at[(-way * hop) % ring, half_rows(half)],
            gs_sem.at[number],
            gr_sem.at[number],
            ahead if way == 1 else behind,
        )

    def sum_copy(half, way, hop):
        number = HOPS[half, way, hop]
        return remote(
            pbuf.at[(way * hop) % ring, half_rows(half)],
            rbuf.at[number],
            ss_sem.at[number],
            sr_sem.at[number],
            ahead if way == 1 else behind,
        )

    for half, way in ((0, 1), (1, -1), (1, 1), (0, -1)):
        gather_copy(half, way, 1).start()
    shared = [
        remote(
            gate_ref.at[0], w1.at[:, pl.ds(inner, inner)], ws_sem.at[0], wr_sem.at[0], partner
        ),
        remote(
            up_ref.at[0], w1.at[:, pl.ds(3 * inner, inner)], ws_sem.at[1], wr_sem.at[1], partner
        ),
        remote(down_ref.at[0], w2.at[pl.ds(inner, inner)], ws_sem.at[2], wr_sem.at[2], partner),
    ]
    for copy in shared:
        copy.start()
    for copy in local:
        copy.wait()
    for copy in shared:
        copy.wait_recv()

    def experts(rows_in, slot):
        pre = jnp.dot(rows_in, w1[...], preferred_element_type=jnp.float32)
        clipped = jnp.minimum(pre[:, : 2 * inner], CLAMP_LIMIT)
        linear = jnp.clip(pre[:, 2 * inner :], -CLAMP_LIMIT, CLAMP_LIMIT)
        hidden = (clipped * jax.nn.sigmoid(ACT_SLOPE * clipped) * (linear + 1.0)).astype(
            jnp.bfloat16
        )
        width = w2.shape[1]
        step = width // 4
        for at in range(0, width, step):
            pbuf[slot, :, at : at + step] = jnp.dot(
                hidden, w2[:, at : at + step], preferred_element_type=jnp.float32
            ).astype(jnp.bfloat16)

    experts(x_ref[...], 0)
    for hop in range(1, 5):
        for half, way, far in ((0, 1, 4), (1, -1, 4), (1, 1, 3), (0, -1, 3)):
            if hop <= far:
                gather_copy(half, way, hop).wait_recv()
                if hop < far:
                    gather_copy(half, way, hop + 1).start()
        if hop < 4:

            def both(index, carry, hop=hop):
                slot = hop + index * (ring - 2 * hop)
                experts(xbuf[slot], slot)
                return carry

            lax.fori_loop(0, 2, both, 0)
        else:
            experts(xbuf[4], 4)
        if hop >= 3:
            for half, way, far in ((0, 1, 4), (1, -1, 4), (1, 1, 3), (0, -1, 3)):
                if far == hop:
                    sum_copy(half, way, far).start()
    for left in (3, 2, 1, 0):
        for half, way, far in ((1, 1, 3), (0, -1, 3), (0, 1, 4), (1, -1, 4)):
            hop = far - (4 - left) + 1
            if hop < 1:
                continue
            sum_copy(half, way, hop).wait_recv()
            if hop > 1:
                slot = (way * (hop - 1)) % ring
                at = half_rows(half)
                pbuf[slot, at] = (
                    pbuf[slot, at].astype(jnp.float32)
                    + rbuf[HOPS[half, way, hop]].astype(jnp.float32)
                ).astype(jnp.bfloat16)
                sum_copy(half, way, hop - 1).start()
    for half in range(2):
        at = half_rows(half)
        out_ref[at] = (
            pbuf[0, at].astype(jnp.float32)
            + rbuf[HOPS[half, 1, 1]].astype(jnp.float32)
            + rbuf[HOPS[half, -1, 1]].astype(jnp.float32)
        ).astype(jnp.bfloat16)
    for copy in shared:
        copy.wait_send()
    for half, way, hop in HOPS:
        gather_copy(half, way, hop).wait_send()
        sum_copy(half, way, hop).wait_send()


def ring_experts(x, gate_weight, up_weight, down_weight):
    rows, width = x.shape
    inner = down_weight.shape[1]
    ring = lax.axis_size("tp") // 2
    copies = len(HOPS)
    dma = pltpu.SemaphoreType.DMA
    return pl.pallas_call(
        ring_kernel,
        out_shape=jax.ShapeDtypeStruct(x.shape, x.dtype),
        in_specs=[pl.BlockSpec(memory_space=pltpu.VMEM)]
        + [pl.BlockSpec(memory_space=pl.ANY)] * 3,
        out_specs=pl.BlockSpec(memory_space=pltpu.VMEM),
        scratch_shapes=[
            pltpu.VMEM((width, 4 * inner), jnp.bfloat16),
            pltpu.VMEM((2 * inner, width), jnp.bfloat16),
            pltpu.VMEM((ring, rows, width), jnp.bfloat16),
            pltpu.VMEM((ring, rows, width), jnp.bfloat16),
            pltpu.VMEM((copies, rows // 2, width), jnp.bfloat16),
            dma((3,)),
            dma((3,)),
            dma((3,)),
            dma((copies,)),
            dma((copies,)),
            dma((copies,)),
            dma((copies,)),
        ],
        compiler_params=pltpu.CompilerParams(
            collective_id=3, has_side_effects=True, vmem_limit_bytes=VMEM_LIMIT
        ),
        cost_estimate=pl.CostEstimate(
            flops=2500000000, bytes_accessed=8000000, transcendentals=200000
        ),
        name="ring_experts",
    )(x, gate_weight, up_weight, down_weight)


def on_device(
    query_rows,
    key_rows,
    value_rows,
    query_gain,
    key_gain,
    sink_logits,
    out_weight,
    expert_input,
    expert_gain,
    routes,
    route_logits,
    gate_weight,
    up_weight,
    down_weight,
):
    heads_out = attend(query_rows, key_rows, value_rows, query_gain, key_gain, sink_logits)
    attended = lax.psum_scatter(
        jnp.dot(heads_out, out_weight, preferred_element_type=jnp.float32).astype(jnp.bfloat16),
        "tp",
        scatter_dimension=0,
        tiled=True,
    )
    own_rows = expert_input.shape[0]
    fanout = routes.shape[1]
    capacity = (3 * own_rows * fanout + 2 * EXPERTS - 1) // (2 * EXPERTS)
    ep_size = lax.axis_size("ep")
    widened = expert_input.astype(jnp.float32)
    normed = (
        widened
        * lax.rsqrt(jnp.mean(widened * widened, axis=-1, keepdims=True) + EPSILON)
        * expert_gain
    ).astype(jnp.bfloat16)
    route_weight = jax.nn.softmax(route_logits, axis=-1)
    combine = combine_matrix(routes, route_weight, capacity)
    sender = dispatch_matrix(routes, capacity)
    slot_rows = jnp.einsum(
        "ecr,rd->ecd", sender, normed, preferred_element_type=jnp.float32
    ).astype(jnp.bfloat16)
    messages = slot_rows.reshape(ep_size, -1, 128)
    arrived = exchange(messages, "ep", 1)
    width = expert_input.shape[1]
    summed = ring_experts(arrived.reshape(-1, width), gate_weight, up_weight, down_weight)
    returned = exchange(summed.reshape(messages.shape), "ep", 2)
    returned = returned.reshape(EXPERTS, capacity, width)
    expert_mix = jnp.einsum("rec,ecd->rd", combine, returned.astype(jnp.float32)).astype(
        jnp.bfloat16
    )
    return (attended, expert_mix)


def solution(mesh):
    placed = (
        P("ep", "tp"),
        P("ep", "tp"),
        P("ep", "tp"),
        P("tp", None),
        P("tp", None),
        P("tp"),
        P("tp", None),
        P(("ep", "tp"), None),
        P(),
        P(("ep", "tp"), None),
        P(("ep", "tp"), None),
        P("ep", None, "tp"),
        P("ep", None, "tp"),
        P("ep", "tp", None),
    )
    return jax.shard_map(
        on_device,
        mesh=mesh,
        in_specs=placed,
        out_specs=(P(("ep", "tp"), None), P(("ep", "tp"), None)),
        check_vma=False,
    )
```

```python
import jax
import jax.numpy as jnp
from jax import lax
from jax.experimental import pallas as pl
from jax.experimental.pallas import tpu as pltpu
from jax.sharding import PartitionSpec as P

EXPERTS = 32
WINDOW = 128


EPSILON = 1e-06
CLAMP_LIMIT = 7.0
ACT_SLOPE = 1.702
NEGATIVE = -1e30


def shifted(value, axis, steps):
    count = lax.axis_size(axis)
    initial, last = (max(0, -steps), min(count, count - steps))
    return lax.ppermute(value, axis, [(source, source + steps) for source in range(initial, last)])


def head_norm(row_data, gain_table):
    head_count, head_size = gain_table.shape
    widened = row_data.astype(jnp.float32).reshape(row_data.shape[0], head_count, head_size)
    scaled = widened * lax.rsqrt(jnp.mean(widened * widened, axis=-1, keepdims=True) + EPSILON)
    return (scaled * gain_table).astype(jnp.bfloat16)


def band(padded, blocks):
    tiled = padded.reshape((blocks + 1, WINDOW) + padded.shape[1:])
    return jnp.concatenate([tiled[:-1], tiled[1:]], axis=1)


def attend(query_rows, key_rows, value_rows, query_gain, key_gain, sink_logits):
    seq_rows = query_rows.shape[0]
    key_heads, head_size = key_gain.shape
    group_size = query_gain.shape[0] // key_heads
    blocks = seq_rows // WINDOW
    query_hat = head_norm(query_rows, query_gain).reshape(
        blocks, WINDOW, key_heads, group_size, head_size
    )
    key_hat = head_norm(key_rows, key_gain)
    value_hat = value_rows.reshape(seq_rows, key_heads, head_size)
    tail_rows = jnp.stack([key_hat[seq_rows - WINDOW :], value_hat[seq_rows - WINDOW :]])
    earlier = shifted(tail_rows, "ep", 1)
    key_band = band(jnp.concatenate([earlier[0], key_hat], axis=0), blocks)
    value_band = band(jnp.concatenate([earlier[1], value_hat], axis=0), blocks)
    query_pos = lax.broadcasted_iota(jnp.int32, (WINDOW, 2 * WINDOW), 0)
    key_pos = lax.broadcasted_iota(jnp.int32, (WINDOW, 2 * WINDOW), 1)
    distance = query_pos + WINDOW - key_pos
    inside = (distance >= 0) & (distance < WINDOW)
    first_block = (lax.broadcasted_iota(jnp.int32, (blocks, 1, 1), 0) == 0) & (
        lax.axis_index("ep") == 0
    )
    allowed = inside[None] & ~(first_block & (key_pos < WINDOW)[None])
    scores = jnp.einsum(
        "bqkgd,bjkd->bkgqj", query_hat, key_band, preferred_element_type=jnp.float32
    ) * head_size ** (-0.5)
    scores = jnp.where(allowed[:, None, None], scores, NEGATIVE)
    sink_table = sink_logits.reshape(1, key_heads, group_size, 1, 1)
    highest = jnp.maximum(jnp.max(scores, axis=-1, keepdims=True), sink_table)
    weights = jnp.exp(scores - highest)
    total = jnp.sum(weights, axis=-1, keepdims=True) + jnp.exp(sink_table - highest)
    mixed = jnp.einsum(
        "bkgqj,bjkd->bkgqd",
        weights.astype(jnp.bfloat16),
        value_band,
        preferred_element_type=jnp.float32,
    )
    mixed = (mixed / total).astype(jnp.bfloat16)
    return jnp.transpose(mixed, (0, 3, 1, 2, 4)).reshape(seq_rows, -1)


def slot_maps(route_block, capacity):
    flat_routes = route_block.reshape(-1)
    expert_hot = (flat_routes[:, None] == lax.broadcasted_iota(jnp.int32, (1, EXPERTS), 1)).astype(
        jnp.int32
    )
    before = jnp.cumsum(expert_hot, axis=0) - expert_hot
    position = jnp.sum(before * expert_hot, axis=1)
    place_hot = (position[:, None] == lax.broadcasted_iota(jnp.int32, (1, capacity), 1)).astype(
        jnp.float32
    )
    row_total, fanout = route_block.shape
    return (
        expert_hot.astype(jnp.float32).reshape(row_total, fanout, EXPERTS),
        place_hot.reshape(row_total, fanout, capacity),
    )


def dispatch_matrix(route_block, capacity):
    expert_hot, place_hot = slot_maps(route_block, capacity)
    return jnp.einsum("rke,rkc->ecr", expert_hot, place_hot).astype(jnp.bfloat16)


def combine_matrix(route_block, route_weight, capacity):
    expert_hot, place_hot = slot_maps(route_block, capacity)
    return jnp.einsum("rke,rkc,rk->rec", expert_hot, place_hot, route_weight)


CHAINS = ((0, 1, 4), (0, -1, 3), (1, 1, 3), (1, -1, 4))
HOPS = {}
for _half, _way, _far in CHAINS:
    for _hop in range(1, _far + 1):
        HOPS[_half, _way, _hop] = len(HOPS)
X_RING = 4
VMEM_LIMIT = 60 * 1024 * 1024


def remote(source, target, send_sem, recv_sem, where):
    return pltpu.make_async_remote_copy(
        src_ref=source,
        dst_ref=target,
        send_sem=send_sem,
        recv_sem=recv_sem,
        device_id=where,
        device_id_type=pl.DeviceIdType.MESH,
    )


def greet(places):
    barrier = pltpu.get_barrier_semaphore()
    for place in places:
        pl.semaphore_signal(
            barrier, inc=1, device_id=place, device_id_type=pl.DeviceIdType.MESH
        )
    pl.semaphore_wait(barrier, len(places))


def neighbours():
    tp = lax.axis_index("tp")
    ring = lax.axis_size("tp") // 2
    core, spot = lax.rem(tp, 2), lax.div(tp, 2)
    ahead = {"tp": lax.rem(spot + 1, ring) * 2 + core}
    behind = {"tp": lax.rem(spot + ring - 1, ring) * 2 + core}
    partner = {"tp": spot * 2 + (1 - core)}
    return ring, core, spot, ahead, behind, partner


def exchange_order(count):
    long = count // X_RING
    turns = [1, long - 1, 2, long - 2, 3, long - 3, long // 2, 0]
    return [
        (along, across) for across in (0, 1, X_RING - 1, 2) for along in turns if along or across
    ]


def ep_place(me, offset):
    along, across = offset
    z, x = lax.div(me, X_RING), lax.rem(me, X_RING)
    return (
        lax.rem(z + along, lax.axis_size("ep") // X_RING) * X_RING + lax.rem(x + across, X_RING)
    )


def exchange_copies(x_ref, out_ref, send_sem, recv_sem):
    me = lax.axis_index("ep")
    copies = []
    for number, offset in enumerate(exchange_order(lax.axis_size("ep"))):
        peer = ep_place(me, offset)
        copies.append(
            remote(
                x_ref.at[peer],
                out_ref.at[me],
                send_sem.at[number],
                recv_sem.at[number],
                {"ep": peer},
            )
        )
    return copies


def exchange_kernel(x_ref, out_ref, send_sem, recv_sem):
    me = lax.axis_index("ep")
    greet([{"ep": ep_place(me, offset)} for offset in exchange_order(lax.axis_size("ep"))])
    copies = exchange_copies(x_ref, out_ref, send_sem, recv_sem)
    for copy in copies:
        copy.start()
    out_ref[me] = x_ref[me]
    for copy in copies:
        copy.wait()


def exchange(value, collective_id):
    count = value.shape[0]
    return pl.pallas_call(
        exchange_kernel,
        out_shape=jax.ShapeDtypeStruct(value.shape, value.dtype),
        in_specs=[pl.BlockSpec(memory_space=pltpu.VMEM)],
        out_specs=pl.BlockSpec(memory_space=pltpu.VMEM),
        scratch_shapes=[
            pltpu.SemaphoreType.DMA((count,)),
            pltpu.SemaphoreType.DMA((count,)),
        ],
        compiler_params=pltpu.CompilerParams(
            collective_id=collective_id, has_side_effects=True
        ),
        name="exchange_ep",
    )(value)


def finish_kernel(
    x_ref,
    part_ref,
    out_ref,
    attended_ref,
    swapped,
    pair,
    rbuf,
    send_sem,
    recv_sem,
    swap_sem,
    ss_sem,
    sr_sem,
):
    me = lax.axis_index("ep")
    ring, core, spot, ahead, behind, partner = neighbours()
    rows = attended_ref.shape[0]
    part = rows // 2
    greet(
        [ahead, behind, partner]
        + [{"ep": ep_place(me, offset)} for offset in exchange_order(lax.axis_size("ep"))]
    )
    swap = remote(part_ref.at[:, 1 - core], swapped, swap_sem.at[0], swap_sem.at[1], partner)
    swap.start()
    copies = exchange_copies(x_ref, out_ref, send_sem, recv_sem)
    for copy in copies:
        copy.start()
    out_ref[me] = x_ref[me]

    def half_rows(half):
        return pl.ds(half * part, part)

    def sum_copy(half, way, hop):
        number = HOPS[half, way, hop]
        return remote(
            pair.at[(way * hop) % ring, half_rows(half)],
            rbuf.at[number],
            ss_sem.at[number],
            sr_sem.at[number],
            ahead if way == 1 else behind,
        )

    swap.wait_recv()
    for slot in (4, 3, 5, 2, 6, 1, 7, 0):
        owner = lax.rem(spot + slot, ring)
        pair[slot] = (
            part_ref[owner, core].astype(jnp.float32) + swapped[owner].astype(jnp.float32)
        ).astype(jnp.bfloat16)
        if slot == 4:
            sum_copy(0, 1, 4).start()
            sum_copy(1, -1, 4).start()
        if slot == 3:
            sum_copy(1, 1, 3).start()
        if slot == 5:
            sum_copy(0, -1, 3).start()
    for left in (3, 2, 1, 0):
        for half, way, far in ((0, 1, 4), (1, -1, 4), (1, 1, 3), (0, -1, 3)):
            hop = far - (4 - left) + 1
            if hop < 1:
                continue
            sum_copy(half, way, hop).wait_recv()
            if hop > 1:
                slot = (way * (hop - 1)) % ring
                at = half_rows(half)
                pair[slot, at] = (
                    pair[slot, at].astype(jnp.float32)
                    + rbuf[HOPS[half, way, hop]].astype(jnp.float32)
                ).astype(jnp.bfloat16)
                sum_copy(half, way, hop - 1).start()
    for half in range(2):
        at = half_rows(half)
        attended_ref[at] = (
            pair[0, at].astype(jnp.float32)
            + rbuf[HOPS[half, 1, 1]].astype(jnp.float32)
            + rbuf[HOPS[half, -1, 1]].astype(jnp.float32)
        ).astype(jnp.bfloat16)
    swap.wait_send()
    for half, way, hop in HOPS:
        sum_copy(half, way, hop).wait_send()
    for copy in copies:
        copy.wait()


def finish(value, partial_rows):
    count = value.shape[0]
    ring = lax.axis_size("tp") // 2
    rows, width = partial_rows.shape[0] // (2 * ring), partial_rows.shape[1]
    dma = pltpu.SemaphoreType.DMA
    return pl.pallas_call(
        finish_kernel,
        out_shape=(
            jax.ShapeDtypeStruct(value.shape, value.dtype),
            jax.ShapeDtypeStruct((rows, width), jnp.bfloat16),
        ),
        in_specs=[pl.BlockSpec(memory_space=pltpu.VMEM)] * 2,
        out_specs=[pl.BlockSpec(memory_space=pltpu.VMEM)] * 2,
        scratch_shapes=[
            pltpu.VMEM((ring, rows, width), jnp.bfloat16),
            pltpu.VMEM((ring, rows, width), jnp.bfloat16),
            pltpu.VMEM((len(HOPS), rows // 2, width), jnp.bfloat16),
            dma((count,)),
            dma((count,)),
            dma((2,)),
            dma((len(HOPS),)),
            dma((len(HOPS),)),
        ],
        compiler_params=pltpu.CompilerParams(
            collective_id=2, has_side_effects=True, vmem_limit_bytes=VMEM_LIMIT
        ),
        name="finish",
    )(value, partial_rows.reshape(ring, 2, rows, width))


def ring_kernel(
    x_ref,
    gate_ref,
    up_ref,
    down_ref,
    out_ref,
    w1,
    w2,
    xbuf,
    pbuf,
    rbuf,
    wl_sem,
    ws_sem,
    wr_sem,
    gs_sem,
    gr_sem,
    ss_sem,
    sr_sem,
):
    ring, core, spot, ahead, behind, partner = neighbours()
    rows = x_ref.shape[0]
    part = rows // 2
    inner = down_ref.shape[1]
    local = [
        pltpu.make_async_copy(gate_ref.at[0], w1.at[:, pl.ds(0, inner)], wl_sem.at[0]),
        pltpu.make_async_copy(up_ref.at[0], w1.at[:, pl.ds(2 * inner, inner)], wl_sem.at[1]),
        pltpu.make_async_copy(down_ref.at[0], w2.at[pl.ds(0, inner)], wl_sem.at[2]),
    ]
    for copy in local:
        copy.start()
    greet((ahead, behind, partner))

    def half_rows(half):
        return pl.ds(half * part, part)

    def gather_copy(half, way, hop):
        slot = (-way * (hop - 1)) % ring
        source = x_ref.at[half_rows(half)] if hop == 1 else xbuf.at[slot, half_rows(half)]
        number = HOPS[half, way, hop]
        return remote(
            source,
            xbuf.at[(-way * hop) % ring, half_rows(half)],
            gs_sem.at[number],
            gr_sem.at[number],
            ahead if way == 1 else behind,
        )

    def sum_copy(half, way, hop):
        number = HOPS[half, way, hop]
        return remote(
            pbuf.at[(way * hop) % ring, half_rows(half)],
            rbuf.at[number],
            ss_sem.at[number],
            sr_sem.at[number],
            ahead if way == 1 else behind,
        )

    for half, way in ((0, 1), (1, -1), (1, 1), (0, -1)):
        gather_copy(half, way, 1).start()
    shared = [
        remote(
            gate_ref.at[0], w1.at[:, pl.ds(inner, inner)], ws_sem.at[0], wr_sem.at[0], partner
        ),
        remote(
            up_ref.at[0], w1.at[:, pl.ds(3 * inner, inner)], ws_sem.at[1], wr_sem.at[1], partner
        ),
        remote(down_ref.at[0], w2.at[pl.ds(inner, inner)], ws_sem.at[2], wr_sem.at[2], partner),
    ]
    for copy in shared:
        copy.start()
    for copy in local:
        copy.wait()
    for copy in shared:
        copy.wait_recv()

    def experts(rows_in, slot):
        pre = jnp.dot(rows_in, w1[...], preferred_element_type=jnp.float32)
        clipped = jnp.minimum(pre[:, : 2 * inner], CLAMP_LIMIT)
        linear = jnp.clip(pre[:, 2 * inner :], -CLAMP_LIMIT, CLAMP_LIMIT)
        hidden = (clipped * jax.nn.sigmoid(ACT_SLOPE * clipped) * (linear + 1.0)).astype(
            jnp.bfloat16
        )
        width = w2.shape[1]
        step = width // 4
        for at in range(0, width, step):
            pbuf[slot, :, at : at + step] = jnp.dot(
                hidden, w2[:, at : at + step], preferred_element_type=jnp.float32
            ).astype(jnp.bfloat16)

    experts(x_ref[...], 0)
    for hop in range(1, 5):
        for half, way, far in ((0, 1, 4), (1, -1, 4), (1, 1, 3), (0, -1, 3)):
            if hop <= far:
                gather_copy(half, way, hop).wait_recv()
                if hop < far:
                    gather_copy(half, way, hop + 1).start()
        if hop < 4:

            def both(index, carry, hop=hop):
                slot = hop + index * (ring - 2 * hop)
                experts(xbuf[slot], slot)
                return carry

            lax.fori_loop(0, 2, both, 0)
        else:
            experts(xbuf[4], 4)
        if hop >= 3:
            for half, way, far in ((0, 1, 4), (1, -1, 4), (1, 1, 3), (0, -1, 3)):
                if far == hop:
                    sum_copy(half, way, far).start()
    for left in (3, 2, 1, 0):
        for half, way, far in ((1, 1, 3), (0, -1, 3), (0, 1, 4), (1, -1, 4)):
            hop = far - (4 - left) + 1
            if hop < 1:
                continue
            sum_copy(half, way, hop).wait_recv()
            if hop > 1:
                slot = (way * (hop - 1)) % ring
                at = half_rows(half)
                pbuf[slot, at] = (
                    pbuf[slot, at].astype(jnp.float32)
                    + rbuf[HOPS[half, way, hop]].astype(jnp.float32)
                ).astype(jnp.bfloat16)
                sum_copy(half, way, hop - 1).start()
    for half in range(2):
        at = half_rows(half)
        out_ref[at] = (
            pbuf[0, at].astype(jnp.float32)
            + rbuf[HOPS[half, 1, 1]].astype(jnp.float32)
            + rbuf[HOPS[half, -1, 1]].astype(jnp.float32)
        ).astype(jnp.bfloat16)
    for copy in shared:
        copy.wait_send()
    for half, way, hop in HOPS:
        gather_copy(half, way, hop).wait_send()
        sum_copy(half, way, hop).wait_send()


def ring_experts(x, gate_weight, up_weight, down_weight):
    rows, width = x.shape
    inner = down_weight.shape[1]
    ring = lax.axis_size("tp") // 2
    copies = len(HOPS)
    dma = pltpu.SemaphoreType.DMA
    return pl.pallas_call(
        ring_kernel,
        out_shape=jax.ShapeDtypeStruct(x.shape, x.dtype),
        in_specs=[pl.BlockSpec(memory_space=pltpu.VMEM)]
        + [pl.BlockSpec(memory_space=pl.ANY)] * 3,
        out_specs=pl.BlockSpec(memory_space=pltpu.VMEM),
        scratch_shapes=[
            pltpu.VMEM((width, 4 * inner), jnp.bfloat16),
            pltpu.VMEM((2 * inner, width), jnp.bfloat16),
            pltpu.VMEM((ring, rows, width), jnp.bfloat16),
            pltpu.VMEM((ring, rows, width), jnp.bfloat16),
            pltpu.VMEM((copies, rows // 2, width), jnp.bfloat16),
            dma((3,)),
            dma((3,)),
            dma((3,)),
            dma((copies,)),
            dma((copies,)),
            dma((copies,)),
            dma((copies,)),
        ],
        compiler_params=pltpu.CompilerParams(
            collective_id=3, has_side_effects=True, vmem_limit_bytes=VMEM_LIMIT
        ),
        cost_estimate=pl.CostEstimate(
            flops=2500000000, bytes_accessed=8000000, transcendentals=200000
        ),
        name="ring_experts",
    )(x, gate_weight, up_weight, down_weight)


def on_device(
    query_rows,
    key_rows,
    value_rows,
    query_gain,
    key_gain,
    sink_logits,
    out_weight,
    expert_input,
    expert_gain,
    routes,
    route_logits,
    gate_weight,
    up_weight,
    down_weight,
):
    heads_out = attend(query_rows, key_rows, value_rows, query_gain, key_gain, sink_logits)
    partial_rows = jnp.dot(heads_out, out_weight, preferred_element_type=jnp.float32).astype(
        jnp.bfloat16
    )
    own_rows = expert_input.shape[0]
    fanout = routes.shape[1]
    capacity = (3 * own_rows * fanout + 2 * EXPERTS - 1) // (2 * EXPERTS)
    ep_size = lax.axis_size("ep")
    widened = expert_input.astype(jnp.float32)
    normed = (
        widened
        * lax.rsqrt(jnp.mean(widened * widened, axis=-1, keepdims=True) + EPSILON)
        * expert_gain
    ).astype(jnp.bfloat16)
    route_weight = jax.nn.softmax(route_logits, axis=-1)
    combine = combine_matrix(routes, route_weight, capacity)
    sender = dispatch_matrix(routes, capacity)
    slot_rows = jnp.einsum(
        "ecr,rd->ecd", sender, normed, preferred_element_type=jnp.float32
    ).astype(jnp.bfloat16)
    messages = slot_rows.reshape(ep_size, -1, 128)
    arrived = exchange(messages, 1)
    width = expert_input.shape[1]
    summed = ring_experts(arrived.reshape(-1, width), gate_weight, up_weight, down_weight)
    returned, attended = finish(summed.reshape(messages.shape), partial_rows)
    returned = returned.reshape(EXPERTS, capacity, width)
    expert_mix = jnp.einsum("rec,ecd->rd", combine, returned.astype(jnp.float32)).astype(
        jnp.bfloat16
    )
    return (attended, expert_mix)


def solution(mesh):
    placed = (
        P("ep", "tp"),
        P("ep", "tp"),
        P("ep", "tp"),
        P("tp", None),
        P("tp", None),
        P("tp"),
        P("tp", None),
        P(("ep", "tp"), None),
        P(),
        P(("ep", "tp"), None),
        P(("ep", "tp"), None),
        P("ep", None, "tp"),
        P("ep", None, "tp"),
        P("ep", "tp", None),
    )
    return jax.shard_map(
        on_device,
        mesh=mesh,
        in_specs=placed,
        out_specs=(P(("ep", "tp"), None), P(("ep", "tp"), None)),
        check_vma=False,
    )
```

```python
import jax
import jax.numpy as jnp
from jax import lax
from jax.experimental import pallas as pl
from jax.experimental.pallas import tpu as pltpu
from jax.sharding import PartitionSpec as P

EXPERTS = 32
WINDOW = 128


EPSILON = 1e-06
CLAMP_LIMIT = 7.0
ACT_SLOPE = 1.702
NEGATIVE = -1e30


def shifted(value, axis, steps):
    count = lax.axis_size(axis)
    initial, last = (max(0, -steps), min(count, count - steps))
    return lax.ppermute(value, axis, [(source, source + steps) for source in range(initial, last)])


def head_norm(row_data, gain_table):
    head_count, head_size = gain_table.shape
    widened = row_data.astype(jnp.float32).reshape(row_data.shape[0], head_count, head_size)
    scaled = widened * lax.rsqrt(jnp.mean(widened * widened, axis=-1, keepdims=True) + EPSILON)
    return (scaled * gain_table).astype(jnp.bfloat16)


def band(padded, blocks):
    tiled = padded.reshape((blocks + 1, WINDOW) + padded.shape[1:])
    return jnp.concatenate([tiled[:-1], tiled[1:]], axis=1)


def attend(query_rows, key_rows, value_rows, query_gain, key_gain, sink_logits):
    seq_rows = query_rows.shape[0]
    key_heads, head_size = key_gain.shape
    group_size = query_gain.shape[0] // key_heads
    blocks = seq_rows // WINDOW
    query_hat = head_norm(query_rows, query_gain).reshape(
        blocks, WINDOW, key_heads, group_size, head_size
    )
    key_hat = head_norm(key_rows, key_gain)
    value_hat = value_rows.reshape(seq_rows, key_heads, head_size)
    tail_rows = jnp.stack([key_hat[seq_rows - WINDOW :], value_hat[seq_rows - WINDOW :]])
    earlier = shifted(tail_rows, "ep", 1)
    key_band = band(jnp.concatenate([earlier[0], key_hat], axis=0), blocks)
    value_band = band(jnp.concatenate([earlier[1], value_hat], axis=0), blocks)
    query_pos = lax.broadcasted_iota(jnp.int32, (WINDOW, 2 * WINDOW), 0)
    key_pos = lax.broadcasted_iota(jnp.int32, (WINDOW, 2 * WINDOW), 1)
    distance = query_pos + WINDOW - key_pos
    inside = (distance >= 0) & (distance < WINDOW)
    first_block = (lax.broadcasted_iota(jnp.int32, (blocks, 1, 1), 0) == 0) & (
        lax.axis_index("ep") == 0
    )
    allowed = inside[None] & ~(first_block & (key_pos < WINDOW)[None])
    scores = jnp.einsum(
        "bqkgd,bjkd->bkgqj", query_hat, key_band, preferred_element_type=jnp.float32
    ) * head_size ** (-0.5)
    scores = jnp.where(allowed[:, None, None], scores, NEGATIVE)
    sink_table = sink_logits.reshape(1, key_heads, group_size, 1, 1)
    highest = jnp.maximum(jnp.max(scores, axis=-1, keepdims=True), sink_table)
    weights = jnp.exp(scores - highest)
    total = jnp.sum(weights, axis=-1, keepdims=True) + jnp.exp(sink_table - highest)
    mixed = jnp.einsum(
        "bkgqj,bjkd->bkgqd",
        weights.astype(jnp.bfloat16),
        value_band,
        preferred_element_type=jnp.float32,
    )
    mixed = (mixed / total).astype(jnp.bfloat16)
    return jnp.transpose(mixed, (0, 3, 1, 2, 4)).reshape(seq_rows, -1)


def slot_maps(route_block, capacity):
    flat_routes = route_block.reshape(-1)
    expert_hot = (flat_routes[:, None] == lax.broadcasted_iota(jnp.int32, (1, EXPERTS), 1)).astype(
        jnp.int32
    )
    before = jnp.cumsum(expert_hot, axis=0) - expert_hot
    position = jnp.sum(before * expert_hot, axis=1)
    place_hot = (position[:, None] == lax.broadcasted_iota(jnp.int32, (1, capacity), 1)).astype(
        jnp.float32
    )
    row_total, fanout = route_block.shape
    return (
        expert_hot.astype(jnp.float32).reshape(row_total, fanout, EXPERTS),
        place_hot.reshape(row_total, fanout, capacity),
    )


def dispatch_matrix(route_block, capacity):
    expert_hot, place_hot = slot_maps(route_block, capacity)
    return jnp.einsum("rke,rkc->ecr", expert_hot, place_hot).astype(jnp.bfloat16)


def combine_matrix(route_block, route_weight, capacity):
    expert_hot, place_hot = slot_maps(route_block, capacity)
    return jnp.einsum("rke,rkc,rk->rec", expert_hot, place_hot, route_weight)


CHAINS = ((0, 1, 4), (1, -1, 4), (1, 1, 3), (0, -1, 3))
HOPS = {}
for _half, _way, _far in CHAINS:
    for _hop in range(1, _far + 1):
        HOPS[_half, _way, _hop] = len(HOPS)
X_RING = 4
GROUPS = 2
LANES = 128
VMEM_LIMIT = 60 * 1024 * 1024


def remote(source, target, send_sem, recv_sem, where):
    return pltpu.make_async_remote_copy(
        src_ref=source,
        dst_ref=target,
        send_sem=send_sem,
        recv_sem=recv_sem,
        device_id=where,
        device_id_type=pl.DeviceIdType.MESH,
    )


def greet(places):
    barrier = pltpu.get_barrier_semaphore()
    for place in places:
        pl.semaphore_signal(
            barrier, inc=1, device_id=place, device_id_type=pl.DeviceIdType.MESH
        )
    pl.semaphore_wait(barrier, len(places))


def exchange_order(count):
    long = count // X_RING
    order = [(0, across) for across in (0, 1, X_RING - 1, 2)]
    for level in range(1, long // 2):
        for across in (0, 1, X_RING - 1, 2):
            order += [(level, across), (long - level, across)]
    return order + [(long // 2, across) for across in (0, 1, X_RING - 1, 2)]


def ep_place(me, offset, sign=1):
    across_count = X_RING
    along_count = lax.axis_size("ep") // X_RING
    z, x = lax.div(me, across_count), lax.rem(me, across_count)
    along = (sign * offset[0]) % along_count
    across = (sign * offset[1]) % across_count
    return lax.rem(z + along, along_count) * across_count + lax.rem(x + across, across_count)


def layer_kernel(
    x_ref,
    gate_ref,
    up_ref,
    down_ref,
    part_ref,
    back_ref,
    attended_ref,
    w1,
    w2,
    abuf,
    turn,
    xbuf,
    pbuf,
    rbuf,
    sbuf,
    swapped,
    pair,
    prbuf,
    wl_sem,
    ws_sem,
    wr_sem,
    es_sem,
    er_sem,
    bs_sem,
    br_sem,
    gs_sem,
    gr_sem,
    ss_sem,
    sr_sem,
    swap_sem,
    ps_sem,
    pr_sem,
):
    me = lax.axis_index("ep")
    count = lax.axis_size("ep")
    tp = lax.axis_index("tp")
    ring = lax.axis_size("tp") // 2
    core, spot = lax.rem(tp, 2), lax.div(tp, 2)
    ahead = {"tp": lax.rem(spot + 1, ring) * 2 + core}
    behind = {"tp": lax.rem(spot + ring - 1, ring) * 2 + core}
    partner = {"tp": spot * 2 + (1 - core)}
    order = exchange_order(count)
    inner = down_ref.shape[1]
    members = count // GROUPS
    rows, width = xbuf.shape[2], xbuf.shape[3]
    strip = width // LANES

    local = [
        pltpu.make_async_copy(gate_ref.at[0], w1.at[:, pl.ds(0, inner)], wl_sem.at[0]),
        pltpu.make_async_copy(up_ref.at[0], w1.at[:, pl.ds(2 * inner, inner)], wl_sem.at[1]),
        pltpu.make_async_copy(down_ref.at[0], w2.at[pl.ds(0, inner)], wl_sem.at[2]),
    ]
    for copy in local:
        copy.start()
    greet(
        [ahead, behind, partner] + [{"ep": ep_place(me, offset)} for offset in order[1:]]
    )

    def out_copy(number):
        peer = ep_place(me, order[number])
        return remote(
            x_ref.at[peer], abuf.at[number], es_sem.at[number], er_sem.at[number], {"ep": peer}
        )

    def back_copy(number):
        peer = ep_place(me, order[number], -1)
        return remote(
            sbuf.at[number], back_ref.at[me], bs_sem.at[number], br_sem.at[number], {"ep": peer}
        )

    def half_columns(half):
        return pl.ds(half * (width // 2), width // 2)

    def toward(way):
        return ahead if way == 1 else behind

    def gather_copy(group, half, way, hop):
        number = HOPS[half, way, hop]
        return remote(
            xbuf.at[group, (-way * (hop - 1)) % ring, :, half_columns(half)],
            xbuf.at[group, (-way * hop) % ring, :, half_columns(half)],
            gs_sem.at[group, number],
            gr_sem.at[group, number],
            toward(way),
        )

    def sum_copy(group, half, way, hop):
        number = HOPS[half, way, hop]
        return remote(
            pbuf.at[group, (way * hop) % ring, :, half_columns(half)],
            rbuf.at[group, number],
            ss_sem.at[group, number],
            sr_sem.at[group, number],
            toward(way),
        )

    def pair_copy(half, way, hop):
        number = HOPS[half, way, hop]
        return remote(
            pair.at[(way * hop) % ring, :, half_columns(half)],
            prbuf.at[number],
            ps_sem.at[number],
            pr_sem.at[number],
            toward(way),
        )

    def running(buffer, received, copy_of, left):
        for half, way, far in CHAINS:
            hop = far - 3 + left
            if hop < 1:
                continue
            copy_of(half, way, hop).wait_recv()
            if hop > 1:
                slot = (way * (hop - 1)) % ring
                at = half_columns(half)
                buffer[slot, :, at] = (
                    buffer[slot, :, at].astype(jnp.float32)
                    + received[HOPS[half, way, hop]].astype(jnp.float32)
                ).astype(jnp.bfloat16)
                copy_of(half, way, hop - 1).start()

    def summed(buffer, received, half):
        return (
            buffer[0, :, half_columns(half)].astype(jnp.float32)
            + received[HOPS[half, 1, 1]].astype(jnp.float32)
            + received[HOPS[half, -1, 1]].astype(jnp.float32)
        )

    def experts(group, slot):
        pre = jnp.dot(xbuf[group, slot], w1[...], preferred_element_type=jnp.float32)
        clipped = jnp.minimum(pre[:, : 2 * inner], CLAMP_LIMIT)
        linear = jnp.clip(pre[:, 2 * inner :], -CLAMP_LIMIT, CLAMP_LIMIT)
        hidden = (clipped * jax.nn.sigmoid(ACT_SLOPE * clipped) * (linear + 1.0)).astype(
            jnp.bfloat16
        )
        step = width // 4
        for at in range(0, width, step):
            pbuf[group, slot, :, at : at + step] = jnp.dot(
                hidden, w2[:, at : at + step], preferred_element_type=jnp.float32
            ).astype(jnp.bfloat16)

    def arrive(group):
        for number in range(group * members, (group + 1) * members):
            if number > 0:
                out_copy(number).wait_recv()
        messages = abuf[group * members : (group + 1) * members]
        turn[...] = messages.astype(jnp.float32).reshape(turn.shape)
        for at in range(strip):
            xbuf[group, 0, :, at * LANES : (at + 1) * LANES] = turn[
                pl.ds(at, rows, stride=strip), :
            ].astype(jnp.bfloat16)
        for half, way, far in CHAINS:
            gather_copy(group, half, way, 1).start()

    def gather(group, hop):
        for half, way, far in CHAINS:
            if hop <= far:
                gather_copy(group, half, way, hop).wait_recv()
                if hop < far:
                    gather_copy(group, half, way, hop + 1).start()
        if hop < 4:

            def both(index, carry):
                experts(group, hop + index * (ring - 2 * hop))
                return carry

            lax.fori_loop(0, 2, both, 0)
        else:
            experts(group, 4)
        for half, way, far in CHAINS:
            if far == hop:
                sum_copy(group, half, way, far).start()

    def collect(group, left):
        running(
            pbuf.at[group],
            rbuf.at[group],
            lambda half, way, hop: sum_copy(group, half, way, hop),
            left,
        )

    def give_back(group):
        for half in range(2):
            total = summed(pbuf.at[group], rbuf.at[group], half)
            for at in range(strip // 2):
                turn[pl.ds(half * (strip // 2) + at, rows, stride=strip), :] = total[
                    :, at * LANES : (at + 1) * LANES
                ]
        sbuf[group * members : (group + 1) * members] = (
            turn[...].reshape(members, -1, LANES).astype(jnp.bfloat16)
        )
        for number in range(group * members, (group + 1) * members):
            if number > 0:
                back_copy(number).start()

    for number in range(1, count):
        out_copy(number).start()
    swap = remote(part_ref.at[:, 1 - core], swapped, swap_sem.at[0], swap_sem.at[1], partner)
    swap.start()
    shared = [
        remote(
            gate_ref.at[0], w1.at[:, pl.ds(inner, inner)], ws_sem.at[0], wr_sem.at[0], partner
        ),
        remote(
            up_ref.at[0], w1.at[:, pl.ds(3 * inner, inner)], ws_sem.at[1], wr_sem.at[1], partner
        ),
        remote(down_ref.at[0], w2.at[pl.ds(inner, inner)], ws_sem.at[2], wr_sem.at[2], partner),
    ]
    for copy in shared:
        copy.start()
    abuf[0] = x_ref[me]
    swap.wait_recv()
    for slot in (4, 3, 5, 2, 6, 1, 7, 0):
        owner = lax.rem(spot + slot, ring)
        pair[slot] = (
            part_ref[owner, core].astype(jnp.float32) + swapped[owner].astype(jnp.float32)
        ).astype(jnp.bfloat16)
        for half, way, far in CHAINS:
            if (way * far) % ring == slot:
                pair_copy(half, way, far).start()
    running(pair, prbuf, pair_copy, 3)
    running(pair, prbuf, pair_copy, 2)
    arrive(0)
    for copy in local:
        copy.wait()
    for copy in shared:
        copy.wait_recv()
    experts(0, 0)
    running(pair, prbuf, pair_copy, 1)
    gather(0, 1)
    running(pair, prbuf, pair_copy, 0)
    for half in range(2):
        attended_ref[:, half_columns(half)] = summed(pair, prbuf, half).astype(jnp.bfloat16)
    arrive(1)
    gather(0, 2)
    experts(1, 0)
    gather(1, 1)
    gather(0, 3)
    gather(1, 2)
    gather(0, 4)
    gather(1, 3)
    collect(0, 3)
    gather(1, 4)
    collect(0, 2)
    collect(1, 3)
    collect(0, 1)
    collect(1, 2)
    collect(0, 0)
    give_back(0)
    collect(1, 1)
    collect(1, 0)
    give_back(1)
    back_ref[me] = sbuf[0]
    swap.wait_send()
    for copy in shared:
        copy.wait_send()
    for half, way, hop in HOPS:
        pair_copy(half, way, hop).wait_send()
        for group in range(GROUPS):
            gather_copy(group, half, way, hop).wait_send()
            sum_copy(group, half, way, hop).wait_send()
    for number in range(1, count):
        out_copy(number).wait_send()
        back_copy(number).wait()


def layer(messages, gate_weight, up_weight, down_weight, partial_rows):
    count = messages.shape[0]
    width = gate_weight.shape[1]
    inner = down_weight.shape[1]
    ring = lax.axis_size("tp") // 2
    own = partial_rows.shape[0] // (2 * ring)
    rows = messages.size // width // GROUPS
    hops = len(HOPS)
    dma = pltpu.SemaphoreType.DMA

    def scratch(*shape):
        return pltpu.VMEM(shape, jnp.bfloat16)

    return pl.pallas_call(
        layer_kernel,
        out_shape=(
            jax.ShapeDtypeStruct(messages.shape, messages.dtype),
            jax.ShapeDtypeStruct((own, width), jnp.bfloat16),
        ),
        in_specs=[pl.BlockSpec(memory_space=pltpu.VMEM)]
        + [pl.BlockSpec(memory_space=pl.ANY)] * 3
        + [pl.BlockSpec(memory_space=pltpu.VMEM)],
        out_specs=[pl.BlockSpec(memory_space=pltpu.VMEM)] * 2,
        scratch_shapes=[
            scratch(width, 4 * inner),
            scratch(2 * inner, width),
            scratch(*messages.shape),
            pltpu.VMEM((messages.size // LANES // GROUPS, LANES), jnp.float32),
            scratch(GROUPS, ring, rows, width),
            scratch(GROUPS, ring, rows, width),
            scratch(GROUPS, hops, rows, width // 2),
            scratch(*messages.shape),
            scratch(ring, own, width),
            scratch(ring, own, width),
            scratch(hops, own, width // 2),
            dma((3,)),
            dma((3,)),
            dma((3,)),
            dma((count,)),
            dma((count,)),
            dma((count,)),
            dma((count,)),
            dma((GROUPS, hops)),
            dma((GROUPS, hops)),
            dma((GROUPS, hops)),
            dma((GROUPS, hops)),
            dma((2,)),
            dma((hops,)),
            dma((hops,)),
        ],
        compiler_params=pltpu.CompilerParams(
            collective_id=1, has_side_effects=True, vmem_limit_bytes=VMEM_LIMIT
        ),
        name="layer",
    )(messages, gate_weight, up_weight, down_weight, partial_rows.reshape(ring, 2, own, width))


def on_device(
    query_rows,
    key_rows,
    value_rows,
    query_gain,
    key_gain,
    sink_logits,
    out_weight,
    expert_input,
    expert_gain,
    routes,
    route_logits,
    gate_weight,
    up_weight,
    down_weight,
):
    heads_out = attend(query_rows, key_rows, value_rows, query_gain, key_gain, sink_logits)
    partial_rows = jnp.dot(heads_out, out_weight, preferred_element_type=jnp.float32).astype(
        jnp.bfloat16
    )
    own_rows = expert_input.shape[0]
    fanout = routes.shape[1]
    capacity = (3 * own_rows * fanout + 2 * EXPERTS - 1) // (2 * EXPERTS)
    ep_size = lax.axis_size("ep")
    widened = expert_input.astype(jnp.float32)
    normed = (
        widened
        * lax.rsqrt(jnp.mean(widened * widened, axis=-1, keepdims=True) + EPSILON)
        * expert_gain
    ).astype(jnp.bfloat16)
    route_weight = jax.nn.softmax(route_logits, axis=-1)
    combine = combine_matrix(routes, route_weight, capacity)
    sender = dispatch_matrix(routes, capacity)
    slot_rows = jnp.einsum(
        "ecr,rd->ecd", sender, normed, preferred_element_type=jnp.float32
    ).astype(jnp.bfloat16)
    messages = slot_rows.reshape(ep_size, -1, 128)
    returned, attended = layer(messages, gate_weight, up_weight, down_weight, partial_rows)
    returned = returned.reshape(EXPERTS, capacity, -1)
    expert_mix = jnp.einsum("rec,ecd->rd", combine, returned.astype(jnp.float32)).astype(
        jnp.bfloat16
    )
    return (attended, expert_mix)


def solution(mesh):
    placed = (
        P("ep", "tp"),
        P("ep", "tp"),
        P("ep", "tp"),
        P("tp", None),
        P("tp", None),
        P("tp"),
        P("tp", None),
        P(("ep", "tp"), None),
        P(),
        P(("ep", "tp"), None),
        P(("ep", "tp"), None),
        P("ep", None, "tp"),
        P("ep", None, "tp"),
        P("ep", "tp", None),
    )
    return jax.shard_map(
        on_device,
        mesh=mesh,
        in_specs=placed,
        out_specs=(P(("ep", "tp"), None), P(("ep", "tp"), None)),
        check_vma=False,
    )
```

```python
import jax
import jax.numpy as jnp
from jax import lax
from jax.experimental import pallas as pl
from jax.experimental.pallas import tpu as pltpu
from jax.sharding import PartitionSpec as P

WINDOW = 128
EPSILON = 1e-06
CLAMP_LIMIT = 7.0
ACT_SLOPE = 1.702
NEGATIVE = -1e30
CHAINS = ((0, 1, 4), (1, -1, 4), (1, 1, 3), (0, -1, 3))
HOPS = {}
for _half, _way, _far in CHAINS:
    for _hop in range(1, _far + 1):
        HOPS[_half, _way, _hop] = len(HOPS)
X_RING = 4
GROUPS = 2
LANES = 128
VMEM_LIMIT = 60 * 1024 * 1024


def remote(source, target, send_sem, recv_sem, where):
    return pltpu.make_async_remote_copy(
        src_ref=source,
        dst_ref=target,
        send_sem=send_sem,
        recv_sem=recv_sem,
        device_id=where,
        device_id_type=pl.DeviceIdType.MESH,
    )


def column(row):
    size = row.shape[1]
    square = (size, size)
    diagonal = lax.broadcasted_iota(jnp.int32, square, 0) == lax.broadcasted_iota(
        jnp.int32, square, 1
    )
    return jnp.sum(jnp.where(diagonal, jnp.broadcast_to(row, square), 0.0), axis=1, keepdims=True)


def head_norm(rows, gain_row):
    widened = rows.astype(jnp.float32)
    scaled = widened * lax.rsqrt(jnp.mean(widened * widened, axis=0, keepdims=True) + EPSILON)
    return (scaled * column(gain_row)).astype(jnp.bfloat16)


def contract_rows(left, right):
    return lax.dot_general(
        left, right, (((0,), (0,)), ((), ())), preferred_element_type=jnp.float32
    )


def exchange_order(count):
    long = count // X_RING
    order = [(0, across) for across in (0, 1, X_RING - 1, 2)]
    for level in range(1, long // 2):
        for across in (0, 1, X_RING - 1, 2):
            order += [(level, across), (long - level, across)]
    return order + [(long // 2, across) for across in (0, 1, X_RING - 1, 2)]


def ep_place(me, offset, sign=1):
    across_count = X_RING
    along_count = lax.axis_size("ep") // X_RING
    z, x = lax.div(me, across_count), lax.rem(me, across_count)
    along = (sign * offset[0]) % along_count
    across = (sign * offset[1]) % across_count
    return lax.rem(z + along, along_count) * across_count + lax.rem(x + across, across_count)


def layer_kernel(
    query_ref,
    key_ref,
    value_ref,
    query_gain_ref,
    key_gain_ref,
    sink_ref,
    project_ref,
    input_ref,
    input_gain_ref,
    routes_ref,
    logits_ref,
    gate_ref,
    up_ref,
    down_ref,
    attended_ref,
    mix_ref,
    x_ref,
    back_ref,
    keys,
    values,
    queries,
    heads,
    part_ref,
    w1,
    w2,
    abuf,
    turn,
    xbuf,
    pbuf,
    rbuf,
    sbuf,
    swapped,
    pair,
    prbuf,
    wl_sem,
    ws_sem,
    wr_sem,
    es_sem,
    er_sem,
    bs_sem,
    br_sem,
    gs_sem,
    gr_sem,
    ss_sem,
    sr_sem,
    swap_sem,
    ps_sem,
    pr_sem,
    hs_sem,
    hr_sem,
):
    me = lax.axis_index("ep")
    count = lax.axis_size("ep")
    tp = lax.axis_index("tp")
    ring = lax.axis_size("tp") // 2
    core, spot = lax.rem(tp, 2), lax.div(tp, 2)
    ahead = {"tp": lax.rem(spot + 1, ring) * 2 + core}
    behind = {"tp": lax.rem(spot + ring - 1, ring) * 2 + core}
    partner = {"tp": spot * 2 + (1 - core)}
    order = exchange_order(count)
    inner = down_ref.shape[1]
    members = count // GROUPS
    rows, width = xbuf.shape[2], xbuf.shape[3]
    strip = width // LANES

    local = [
        pltpu.make_async_copy(gate_ref.at[0], w1.at[:, pl.ds(0, inner)], wl_sem.at[0]),
        pltpu.make_async_copy(up_ref.at[0], w1.at[:, pl.ds(2 * inner, inner)], wl_sem.at[1]),
        pltpu.make_async_copy(down_ref.at[0], w2.at[pl.ds(0, inner)], wl_sem.at[2]),
    ]
    for copy in local:
        copy.start()
    peers = [ahead, behind, partner] + [{"ep": ep_place(me, offset)} for offset in order[1:]]
    barrier = pltpu.get_barrier_semaphore()
    for place in peers:
        pl.semaphore_signal(
            barrier, inc=1, device_id=place, device_id_type=pl.DeviceIdType.MESH
        )

    def out_copy(number):
        peer = ep_place(me, order[number])
        return remote(
            x_ref.at[peer], abuf.at[number], es_sem.at[number], er_sem.at[number], {"ep": peer}
        )

    def back_copy(number):
        peer = ep_place(me, order[number], -1)
        return remote(
            sbuf.at[number], back_ref.at[me], bs_sem.at[number], br_sem.at[number], {"ep": peer}
        )

    def half_columns(half):
        return pl.ds(half * (width // 2), width // 2)

    def toward(way):
        return ahead if way == 1 else behind

    def gather_copy(group, half, way, hop):
        number = HOPS[half, way, hop]
        return remote(
            xbuf.at[group, (-way * (hop - 1)) % ring, :, half_columns(half)],
            xbuf.at[group, (-way * hop) % ring, :, half_columns(half)],
            gs_sem.at[group, number],
            gr_sem.at[group, number],
            toward(way),
        )

    def sum_copy(group, half, way, hop):
        number = HOPS[half, way, hop]
        return remote(
            pbuf.at[group, (way * hop) % ring, :, half_columns(half)],
            rbuf.at[group, number],
            ss_sem.at[group, number],
            sr_sem.at[group, number],
            toward(way),
        )

    def pair_copy(half, way, hop):
        number = HOPS[half, way, hop]
        return remote(
            pair.at[(way * hop) % ring, :, half_columns(half)],
            prbuf.at[number],
            ps_sem.at[number],
            pr_sem.at[number],
            toward(way),
        )

    def running(buffer, received, copy_of, left):
        for half, way, far in CHAINS:
            hop = far - 3 + left
            if hop < 1:
                continue
            copy_of(half, way, hop).wait_recv()
            if hop > 1:
                slot = (way * (hop - 1)) % ring
                at = half_columns(half)
                buffer[slot, :, at] = (
                    buffer[slot, :, at].astype(jnp.float32)
                    + received[HOPS[half, way, hop]].astype(jnp.float32)
                ).astype(jnp.bfloat16)
                copy_of(half, way, hop - 1).start()

    def summed(buffer, received, half):
        return (
            buffer[0, :, half_columns(half)].astype(jnp.float32)
            + received[HOPS[half, 1, 1]].astype(jnp.float32)
            + received[HOPS[half, -1, 1]].astype(jnp.float32)
        )

    def experts(group, slot):
        pre = jnp.dot(xbuf[group, slot], w1[...], preferred_element_type=jnp.float32)
        clipped = jnp.minimum(pre[:, : 2 * inner], CLAMP_LIMIT)
        linear = jnp.clip(pre[:, 2 * inner :], -CLAMP_LIMIT, CLAMP_LIMIT)
        hidden = (clipped * jax.nn.sigmoid(ACT_SLOPE * clipped) * (linear + 1.0)).astype(
            jnp.bfloat16
        )
        step = width // 4
        for at in range(0, width, step):
            pbuf[group, slot, :, at : at + step] = jnp.dot(
                hidden, w2[:, at : at + step], preferred_element_type=jnp.float32
            ).astype(jnp.bfloat16)

    def arrive(group):
        for number in range(group * members, (group + 1) * members):
            if number > 0:
                out_copy(number).wait_recv()
        messages = abuf[group * members : (group + 1) * members]
        turn[: rows * strip] = messages.astype(jnp.float32).reshape(rows * strip, LANES)
        for at in range(strip):
            xbuf[group, 0, :, at * LANES : (at + 1) * LANES] = turn[
                pl.ds(at, rows, stride=strip), :
            ].astype(jnp.bfloat16)
        for half, way, far in CHAINS:
            gather_copy(group, half, way, 1).start()

    def gather(group, hop):
        for half, way, far in CHAINS:
            if hop <= far:
                gather_copy(group, half, way, hop).wait_recv()
                if hop < far:
                    gather_copy(group, half, way, hop + 1).start()
        if hop < 4:

            def both(index, carry):
                experts(group, hop + index * (ring - 2 * hop))
                return carry

            lax.fori_loop(0, 2, both, 0)
        else:
            experts(group, 4)
        for half, way, far in CHAINS:
            if far == hop:
                sum_copy(group, half, way, far).start()

    def collect(group, left):
        running(
            pbuf.at[group],
            rbuf.at[group],
            lambda half, way, hop: sum_copy(group, half, way, hop),
            left,
        )

    def give_back(group):
        for half in range(2):
            total = summed(pbuf.at[group], rbuf.at[group], half)
            for at in range(strip // 2):
                turn[pl.ds(half * (strip // 2) + at, rows, stride=strip), :] = total[
                    :, at * LANES : (at + 1) * LANES
                ]
        sbuf[group * members : (group + 1) * members] = (
            turn[: rows * strip].reshape(members, -1, LANES).astype(jnp.bfloat16)
        )
        for number in range(group * members, (group + 1) * members):
            if number > 0:
                back_copy(number).start()

    head_size = key_ref.shape[0]
    group_heads = query_ref.shape[0] // head_size
    seq_rows = key_ref.shape[1]
    blocks = seq_rows // WINDOW
    slots = count * x_ref.shape[1] // strip
    capacity = x_ref.shape[1] // strip
    tokens = input_ref.shape[0]

    keys[:, WINDOW:] = head_norm(key_ref[...], key_gain_ref[...])
    values[:, WINDOW:] = value_ref[...]

    given = input_ref[...].astype(jnp.float32)
    normed = (
        given
        * lax.rsqrt(jnp.mean(given * given, axis=-1, keepdims=True) + EPSILON)
        * input_gain_ref[...]
    ).astype(jnp.bfloat16)
    place = lax.broadcasted_iota(jnp.int32, (slots, tokens), 0)
    offset = [place - capacity * routes_ref[copy : copy + 1, :] for copy in range(2)]
    named = [(gap >= 0) & (gap < capacity) for gap in offset]
    hot = [jnp.where(flag, 1.0, 0.0) for flag in named]
    square = (tokens, tokens)
    before = jnp.where(
        lax.broadcasted_iota(jnp.int32, square, 0) < lax.broadcasted_iota(jnp.int32, square, 1),
        1.0,
        0.0,
    ).astype(jnp.bfloat16)
    taken = jnp.dot(
        (hot[0] + hot[1]).astype(jnp.bfloat16), before, preferred_element_type=jnp.float32
    )
    picked = [
        jnp.where(flag & (taken == gap.astype(jnp.float32)), 1.0, 0.0)
        for flag, gap in zip(named, offset)
    ]
    logits = logits_ref[...]
    top_logit = jnp.max(logits, axis=0, keepdims=True)
    raised = jnp.exp(logits - top_logit)
    share = raised / jnp.sum(raised, axis=0, keepdims=True)
    weighted = picked[0] * share[0:1, :] + picked[1] * share[1:2, :]
    coarse = weighted.astype(jnp.bfloat16)
    fine = (weighted - coarse.astype(jnp.float32)).astype(jnp.bfloat16)
    sender = (picked[0] + picked[1]).astype(jnp.bfloat16)
    step = width // 4
    for at in range(0, width, step):
        slot_rows = jnp.dot(sender, normed[:, at : at + step], preferred_element_type=jnp.float32)
        for lane in range(0, step, LANES):
            turn[pl.ds((at + lane) // LANES, slots, stride=strip), :] = slot_rows[
                :, lane : lane + LANES
            ]
    x_ref[...] = turn[...].reshape(x_ref.shape).astype(jnp.bfloat16)

    pl.semaphore_wait(barrier, len(peers))
    following = {"ep": lax.rem(me + 1, count)}
    halo = [
        remote(
            buffer.at[:, pl.ds(seq_rows, WINDOW)],
            buffer.at[:, pl.ds(0, WINDOW)],
            hs_sem.at[index],
            hr_sem.at[index],
            following,
        )
        for index, buffer in enumerate((keys, values))
    ]
    for copy in halo:
        copy.start()
    for number in range(1, count):
        out_copy(number).start()
    shared = [
        remote(
            gate_ref.at[0], w1.at[:, pl.ds(inner, inner)], ws_sem.at[0], wr_sem.at[0], partner
        ),
        remote(
            up_ref.at[0], w1.at[:, pl.ds(3 * inner, inner)], ws_sem.at[1], wr_sem.at[1], partner
        ),
        remote(down_ref.at[0], w2.at[pl.ds(inner, inner)], ws_sem.at[2], wr_sem.at[2], partner),
    ]
    for copy in shared:
        copy.start()
    abuf[0] = x_ref[me]

    for head in range(group_heads):
        hat = head_norm(
            query_ref[head * head_size : (head + 1) * head_size, :],
            query_gain_ref[head : head + 1, :],
        )
        for block in range(blocks):
            queries[block, :, head * WINDOW : (head + 1) * WINDOW] = hat[
                :, block * WINDOW : (block + 1) * WINDOW
            ]
    band = (2 * WINDOW, WINDOW)
    key_pos = lax.broadcasted_iota(jnp.int32, band, 0)
    distance = lax.broadcasted_iota(jnp.int32, band, 1) + WINDOW - key_pos
    inside = (distance >= 0) & (distance < WINDOW)
    inside_first = inside & ((key_pos >= WINDOW) | (me > 0))

    def attend(block):
        at = pl.ds(block * WINDOW, 2 * WINDOW)
        scores = contract_rows(keys[:, at], queries[block]) * head_size**-0.5
        allowed = inside_first if block == 0 else inside
        for head in range(group_heads):
            lanes = slice(head * WINDOW, (head + 1) * WINDOW)
            own = jnp.where(allowed, scores[:, lanes], NEGATIVE)
            sink = jnp.full((1, WINDOW), sink_ref[0, head], jnp.float32)
            highest = jnp.maximum(jnp.max(own, axis=0, keepdims=True), sink)
            weights = jnp.exp(own - highest)
            total = jnp.sum(weights, axis=0, keepdims=True) + jnp.exp(sink - highest)
            mixed = jnp.dot(
                values[:, at], weights.astype(jnp.bfloat16), preferred_element_type=jnp.float32
            )
            heads[head * head_size : (head + 1) * head_size, block * WINDOW : (block + 1) * WINDOW] = (
                mixed / total
            ).astype(jnp.bfloat16)

    def project(block):
        owners = WINDOW // tokens // 2
        rows_in = heads[:, block * WINDOW : (block + 1) * WINDOW]
        for at in range(0, width, step):
            part_ref[block * owners : (block + 1) * owners, :, :, at : at + step] = (
                contract_rows(rows_in, project_ref[:, at : at + step])
                .astype(jnp.bfloat16)
                .reshape(owners, 2, tokens, step)
            )

    for block in range(1, blocks):
        attend(block)
        project(block)
    for copy in halo:
        copy.wait_recv()
    attend(0)
    project(0)
    swap = remote(part_ref.at[:, 1 - core], swapped, swap_sem.at[0], swap_sem.at[1], partner)
    swap.start()
    arrive(0)
    for copy in local:
        copy.wait()
    for copy in shared:
        copy.wait_recv()
    experts(0, 0)
    swap.wait_recv()
    for slot in (4, 3, 5, 2, 6, 1, 7, 0):
        owner = lax.rem(spot + slot, ring)
        pair[slot] = (
            part_ref[owner, core].astype(jnp.float32) + swapped[owner].astype(jnp.float32)
        ).astype(jnp.bfloat16)
        for half, way, far in CHAINS:
            if (way * far) % ring == slot:
                pair_copy(half, way, far).start()
    gather(0, 1)
    arrive(1)
    running(pair, prbuf, pair_copy, 3)
    gather(0, 2)
    experts(1, 0)
    running(pair, prbuf, pair_copy, 2)
    gather(1, 1)
    gather(0, 3)
    running(pair, prbuf, pair_copy, 1)
    gather(1, 2)
    gather(0, 4)
    running(pair, prbuf, pair_copy, 0)
    for half in range(2):
        attended_ref[:, half_columns(half)] = summed(pair, prbuf, half).astype(jnp.bfloat16)
    gather(1, 3)
    collect(0, 3)
    gather(1, 4)
    collect(0, 2)
    collect(1, 3)
    collect(0, 1)
    collect(1, 2)
    collect(0, 0)
    give_back(0)
    collect(1, 1)
    collect(1, 0)
    give_back(1)
    back_ref[me] = sbuf[0]
    swap.wait_send()
    for copy in shared + halo:
        copy.wait_send()
    for half, way, hop in HOPS:
        pair_copy(half, way, hop).wait_send()
        for group in range(GROUPS):
            gather_copy(group, half, way, hop).wait_send()
            sum_copy(group, half, way, hop).wait_send()
    for number in range(1, count):
        out_copy(number).wait_send()
        back_copy(number).wait()
    turn[...] = back_ref[...].astype(jnp.float32).reshape(turn.shape)
    for at in range(strip):
        came = turn[pl.ds(at, slots, stride=strip), :].astype(jnp.bfloat16)
        mix_ref[:, at * LANES : (at + 1) * LANES] = (
            contract_rows(coarse, came) + contract_rows(fine, came)
        ).astype(jnp.bfloat16)


def on_device(
    query_rows,
    key_rows,
    value_rows,
    query_gain,
    key_gain,
    sink_logits,
    out_weight,
    expert_input,
    expert_gain,
    routes,
    route_logits,
    gate_weight,
    up_weight,
    down_weight,
):
    own, width = expert_input.shape
    fanout = routes.shape[1]
    count = lax.axis_size("ep")
    capacity = (3 * own * fanout + 2 * count - 1) // (2 * count)
    inner = down_weight.shape[1]
    ring = lax.axis_size("tp") // 2
    rows = count * capacity // GROUPS
    seq_rows, query_width = query_rows.shape
    head_size = key_rows.shape[1]
    message = (count, capacity * width // LANES, LANES)
    hops = len(HOPS)
    dma = pltpu.SemaphoreType.DMA
    vmem = pl.BlockSpec(memory_space=pltpu.VMEM)

    def scratch(*shape):
        return pltpu.VMEM(shape, jnp.bfloat16)

    return pl.pallas_call(
        layer_kernel,
        out_shape=(jax.ShapeDtypeStruct((own, width), jnp.bfloat16),) * 2,
        in_specs=[vmem] * 5
        + [pl.BlockSpec(memory_space=pltpu.SMEM)]
        + [vmem] * 5
        + [pl.BlockSpec(memory_space=pl.ANY)] * 3,
        out_specs=[vmem] * 2,
        scratch_shapes=[
            scratch(*message),
            scratch(*message),
            scratch(head_size, seq_rows + WINDOW),
            scratch(head_size, seq_rows + WINDOW),
            scratch(seq_rows // WINDOW, head_size, query_width // head_size * WINDOW),
            scratch(query_width, seq_rows),
            scratch(ring, 2, own, width),
            scratch(width, 4 * inner),
            scratch(2 * inner, width),
            scratch(*message),
            pltpu.VMEM((count * capacity * width // LANES, LANES), jnp.float32),
            scratch(GROUPS, ring, rows, width),
            scratch(GROUPS, ring, rows, width),
            scratch(GROUPS, hops, rows, width // 2),
            scratch(*message),
            scratch(ring, own, width),
            scratch(ring, own, width),
            scratch(hops, own, width // 2),
            dma((3,)),
            dma((3,)),
            dma((3,)),
            dma((count,)),
            dma((count,)),
            dma((count,)),
            dma((count,)),
            dma((GROUPS, hops)),
            dma((GROUPS, hops)),
            dma((GROUPS, hops)),
            dma((GROUPS, hops)),
            dma((2,)),
            dma((hops,)),
            dma((hops,)),
            dma((2,)),
            dma((2,)),
        ],
        compiler_params=pltpu.CompilerParams(
            collective_id=1, has_side_effects=True, vmem_limit_bytes=VMEM_LIMIT
        ),
        name="layer",
    )(
        query_rows.T,
        key_rows.T,
        value_rows.T,
        query_gain,
        key_gain,
        sink_logits.reshape(1, -1),
        out_weight,
        expert_input,
        expert_gain.reshape(1, -1),
        routes.T,
        route_logits.T,
        gate_weight,
        up_weight,
        down_weight,
    )


def solution(mesh):
    placed = (
        P("ep", "tp"),
        P("ep", "tp"),
        P("ep", "tp"),
        P("tp", None),
        P("tp", None),
        P("tp"),
        P("tp", None),
        P(("ep", "tp"), None),
        P(),
        P(("ep", "tp"), None),
        P(("ep", "tp"), None),
        P("ep", None, "tp"),
        P("ep", None, "tp"),
        P("ep", "tp", None),
    )
    return jax.shard_map(
        on_device,
        mesh=mesh,
        in_specs=placed,
        out_specs=(P(("ep", "tp"), None), P(("ep", "tp"), None)),
        check_vma=False,
    )
```

```python
import heapq

import jax
import jax.numpy as jnp
from jax import lax
from jax.experimental import pallas as pl
from jax.experimental.pallas import tpu as pltpu
from jax.sharding import PartitionSpec as P

WINDOW = 128
EPSILON = 1e-06
CLAMP_LIMIT = 7.0
ACT_SLOPE = 1.702
NEGATIVE = -1e30
CHAINS = ((0, 1, 4), (1, -1, 4), (1, 1, 3), (0, -1, 3))
HOPS = {}
for _half, _way, _far in CHAINS:
    for _hop in range(1, _far + 1):
        HOPS[_half, _way, _hop] = len(HOPS)
X_RING = 4
GROUPS = 4
LANES = 128
VMEM_LIMIT = 60 * 1024 * 1024


def remote(source, target, send_sem, recv_sem, where):
    return pltpu.make_async_remote_copy(
        src_ref=source,
        dst_ref=target,
        send_sem=send_sem,
        recv_sem=recv_sem,
        device_id=where,
        device_id_type=pl.DeviceIdType.MESH,
    )


def column(row):
    size = row.shape[1]
    square = (size, size)
    diagonal = lax.broadcasted_iota(jnp.int32, square, 0) == lax.broadcasted_iota(
        jnp.int32, square, 1
    )
    return jnp.sum(jnp.where(diagonal, jnp.broadcast_to(row, square), 0.0), axis=1, keepdims=True)


def head_norm(rows, gain_row):
    widened = rows.astype(jnp.float32)
    scaled = widened * lax.rsqrt(jnp.mean(widened * widened, axis=0, keepdims=True) + EPSILON)
    return (scaled * column(gain_row)).astype(jnp.bfloat16)


def contract_rows(left, right):
    return lax.dot_general(
        left, right, (((0,), (0,)), ((), ())), preferred_element_type=jnp.float32
    )


def exchange_order(count):
    long = count // X_RING
    order = [(0, across) for across in (0, 1, X_RING - 1, 2)]
    for level in range(1, long // 2):
        for across in (0, 1, X_RING - 1, 2):
            order += [(level, across), (long - level, across)]
    order += [(long // 2, across) for across in (0, 1, X_RING - 1, 2)]
    quarter = count // 4
    return order[:quarter] + order[2 * quarter :] + order[quarter : 2 * quarter]


def plan():
    wire = {"gather": 2.1 * 2 / GROUPS, "sum": 2.1 * 2 / GROUPS, "pair": 1.4}
    delay = 2.0
    free = {1: 0.0, -1: 0.0}
    coming, ready, steps = [], [], []
    serial = iter(range(1 << 20))
    done = set()
    left = {}

    def send(now, kind, group, half, way, hop):
        free[way] = max(free[way], now) + wire[kind]
        heapq.heappush(coming, (free[way] + delay, next(serial), (kind, group, half, way, hop)))

    def task(rank, name, cost):
        heapq.heappush(ready, (rank, next(serial), name, cost))

    for group in range(GROUPS):
        when = 3.0 + 10.0 * group / (GROUPS - 1)
        heapq.heappush(coming, (when, next(serial), ("arrive", group)))
    heapq.heappush(coming, (4.0, next(serial), ("halo",)))
    for block in (1, 2, 3):
        task(0, ("attend", block), 1.7)
    attended = 0
    now = 0.0
    blocked = []
    while coming or ready or blocked:
        arrived = coming and coming[0][0] <= now
        if not arrived and ready:
            rank, _, name, cost = heapq.heappop(ready)
            steps.append(name)
            now += cost
            done.add(name)
            if name[0] == "attend":
                attended += 1
                if attended == 4:
                    steps.append(("swap",))
                    heapq.heappush(coming, (now + 3.5, next(serial), ("swapped",)))
            elif name[0] == "experts":
                _, group, hop = name
                for half, way, far in CHAINS:
                    if hop and far == hop:
                        steps.append(("start", group, half, way, far))
                        send(now, "sum", group, half, way, far)
            for entry in blocked:
                heapq.heappush(coming, entry)
            blocked = []
            continue
        if not coming:
            break
        when, number, event = heapq.heappop(coming)
        now = max(now, when)
        if event[0] == "sum":
            _, group, half, way, hop = event
            if ("experts", group, hop - 1) not in done:
                blocked.append((when, number, event))
                continue
        steps.append(event)
        if event[0] == "arrive":
            now += 0.6
            for half, way, far in CHAINS:
                send(now, "gather", event[1], half, way, 1)
            task(2 + event[1], ("experts", event[1], 0), 0.9)
        elif event[0] == "halo":
            task(1, ("attend", 0), 1.7)
        elif event[0] == "swapped":
            now += 0.6
            for half, way, far in CHAINS:
                send(now, "pair", 0, half, way, far)
        elif event[0] == "gather":
            _, group, half, way, hop = event
            now += 0.05
            if (half, way, hop + 1) in HOPS:
                send(now, "gather", group, half, way, hop + 1)
            key = ("gather", group, hop)
            left[key] = left.get(key, 0) + 1
            if left[key] == (4 if hop < 4 else 2):
                task(2 + group, ("experts", group, hop), 1.6 if hop < 4 else 0.9)
        else:
            kind, group, half, way, hop = event
            now += 0.2
            if hop > 1:
                send(now, kind, group, half, way, hop - 1)
            else:
                key = (kind, group)
                left[key] = left.get(key, 0) + 1
                if left[key] == 4:
                    steps.append(("finish", kind, group))
                    now += 0.8
    return steps


def ep_place(me, offset, sign=1):
    across_count = X_RING
    along_count = lax.axis_size("ep") // X_RING
    z, x = lax.div(me, across_count), lax.rem(me, across_count)
    along = (sign * offset[0]) % along_count
    across = (sign * offset[1]) % across_count
    return lax.rem(z + along, along_count) * across_count + lax.rem(x + across, across_count)


def layer_kernel(
    query_ref,
    key_ref,
    value_ref,
    query_gain_ref,
    key_gain_ref,
    sink_ref,
    project_ref,
    input_ref,
    input_gain_ref,
    routes_ref,
    logits_ref,
    gate_ref,
    up_ref,
    down_ref,
    attended_ref,
    mix_ref,
    x_ref,
    back_ref,
    keys,
    values,
    queries,
    heads,
    part_ref,
    w1,
    w2,
    abuf,
    turn,
    xbuf,
    pbuf,
    rbuf,
    sbuf,
    swapped,
    pair,
    prbuf,
    wl_sem,
    ws_sem,
    wr_sem,
    es_sem,
    er_sem,
    bs_sem,
    br_sem,
    gs_sem,
    gr_sem,
    ss_sem,
    sr_sem,
    swap_sem,
    ps_sem,
    pr_sem,
    hs_sem,
    hr_sem,
):
    me = lax.axis_index("ep")
    count = lax.axis_size("ep")
    tp = lax.axis_index("tp")
    ring = lax.axis_size("tp") // 2
    core, spot = lax.rem(tp, 2), lax.div(tp, 2)
    ahead = {"tp": lax.rem(spot + 1, ring) * 2 + core}
    behind = {"tp": lax.rem(spot + ring - 1, ring) * 2 + core}
    partner = {"tp": spot * 2 + (1 - core)}
    order = exchange_order(count)
    inner = down_ref.shape[1]
    members = count // GROUPS
    rows, width = xbuf.shape[2], xbuf.shape[3]
    strip = width // LANES

    local = [
        pltpu.make_async_copy(gate_ref.at[0], w1.at[:, pl.ds(0, inner)], wl_sem.at[0]),
        pltpu.make_async_copy(up_ref.at[0], w1.at[:, pl.ds(2 * inner, inner)], wl_sem.at[1]),
        pltpu.make_async_copy(down_ref.at[0], w2.at[pl.ds(0, inner)], wl_sem.at[2]),
    ]
    for copy in local:
        copy.start()
    peers = [ahead, behind, partner] + [{"ep": ep_place(me, offset)} for offset in order[1:]]
    barrier = pltpu.get_barrier_semaphore()
    for place in peers:
        pl.semaphore_signal(
            barrier, inc=1, device_id=place, device_id_type=pl.DeviceIdType.MESH
        )

    def out_copy(number):
        peer = ep_place(me, order[number])
        return remote(
            x_ref.at[peer], abuf.at[number], es_sem.at[number], er_sem.at[number], {"ep": peer}
        )

    def back_copy(number):
        peer = ep_place(me, order[number], -1)
        return remote(
            sbuf.at[number], back_ref.at[me], bs_sem.at[number], br_sem.at[number], {"ep": peer}
        )

    def half_columns(half):
        return pl.ds(half * (width // 2), width // 2)

    def toward(way):
        return ahead if way == 1 else behind

    def gather_copy(group, half, way, hop):
        number = HOPS[half, way, hop]
        return remote(
            xbuf.at[group, (-way * (hop - 1)) % ring, :, half_columns(half)],
            xbuf.at[group, (-way * hop) % ring, :, half_columns(half)],
            gs_sem.at[group, number],
            gr_sem.at[group, number],
            toward(way),
        )

    def sum_copy(group, half, way, hop):
        number = HOPS[half, way, hop]
        return remote(
            pbuf.at[group, (way * hop) % ring, :, half_columns(half)],
            rbuf.at[group, number],
            ss_sem.at[group, number],
            sr_sem.at[group, number],
            toward(way),
        )

    def pair_copy(half, way, hop):
        number = HOPS[half, way, hop]
        return remote(
            pair.at[(way * hop) % ring, :, half_columns(half)],
            prbuf.at[number],
            ps_sem.at[number],
            pr_sem.at[number],
            toward(way),
        )

    def carry_on(buffer, received, copy_of, half, way, hop):
        copy_of(half, way, hop).wait_recv()
        if hop > 1:
            slot = (way * (hop - 1)) % ring
            at = half_columns(half)
            buffer[slot, :, at] = (
                buffer[slot, :, at].astype(jnp.float32)
                + received[HOPS[half, way, hop]].astype(jnp.float32)
            ).astype(jnp.bfloat16)
            copy_of(half, way, hop - 1).start()

    def summed(buffer, received, half):
        return (
            buffer[0, :, half_columns(half)].astype(jnp.float32)
            + received[HOPS[half, 1, 1]].astype(jnp.float32)
            + received[HOPS[half, -1, 1]].astype(jnp.float32)
        )

    def experts(group, slot):
        pre = jnp.dot(xbuf[group, slot], w1[...], preferred_element_type=jnp.float32)
        clipped = jnp.minimum(pre[:, : 2 * inner], CLAMP_LIMIT)
        linear = jnp.clip(pre[:, 2 * inner :], -CLAMP_LIMIT, CLAMP_LIMIT)
        hidden = (clipped * jax.nn.sigmoid(ACT_SLOPE * clipped) * (linear + 1.0)).astype(
            jnp.bfloat16
        )
        step = width // 4
        for at in range(0, width, step):
            pbuf[group, slot, :, at : at + step] = jnp.dot(
                hidden, w2[:, at : at + step], preferred_element_type=jnp.float32
            ).astype(jnp.bfloat16)

    def arrive(group):
        for number in range(group * members, (group + 1) * members):
            if number > 0:
                out_copy(number).wait_recv()
        messages = abuf[group * members : (group + 1) * members]
        turn[: rows * strip] = messages.astype(jnp.float32).reshape(rows * strip, LANES)
        for at in range(strip):
            xbuf[group, 0, :, at * LANES : (at + 1) * LANES] = turn[
                pl.ds(at, rows, stride=strip), :
            ].astype(jnp.bfloat16)
        for half, way, far in CHAINS:
            gather_copy(group, half, way, 1).start()

    def compute(group, hop):
        if hop in (0, 4):
            experts(group, hop)
            return

        def both(index, carry):
            experts(group, hop + index * (ring - 2 * hop))
            return carry

        lax.fori_loop(0, 2, both, 0)

    def give_back(group):
        for half in range(2):
            total = summed(pbuf.at[group], rbuf.at[group], half)
            for at in range(strip // 2):
                turn[pl.ds(half * (strip // 2) + at, rows, stride=strip), :] = total[
                    :, at * LANES : (at + 1) * LANES
                ]
        sbuf[group * members : (group + 1) * members] = (
            turn[: rows * strip].reshape(members, -1, LANES).astype(jnp.bfloat16)
        )
        for number in range(group * members, (group + 1) * members):
            if number > 0:
                back_copy(number).start()

    head_size = key_ref.shape[0]
    group_heads = query_ref.shape[0] // head_size
    seq_rows = key_ref.shape[1]
    blocks = seq_rows // WINDOW
    slots = count * x_ref.shape[1] // strip
    capacity = x_ref.shape[1] // strip
    tokens = input_ref.shape[0]

    keys[:, WINDOW:] = head_norm(key_ref[...], key_gain_ref[...])
    values[:, WINDOW:] = value_ref[...]

    given = input_ref[...].astype(jnp.float32)
    normed = (
        given
        * lax.rsqrt(jnp.mean(given * given, axis=-1, keepdims=True) + EPSILON)
        * input_gain_ref[...]
    ).astype(jnp.bfloat16)
    place = lax.broadcasted_iota(jnp.int32, (slots, tokens), 0)
    offset = [place - capacity * routes_ref[copy : copy + 1, :] for copy in range(2)]
    named = [(gap >= 0) & (gap < capacity) for gap in offset]
    hot = [jnp.where(flag, 1.0, 0.0) for flag in named]
    square = (tokens, tokens)
    before = jnp.where(
        lax.broadcasted_iota(jnp.int32, square, 0) < lax.broadcasted_iota(jnp.int32, square, 1),
        1.0,
        0.0,
    ).astype(jnp.bfloat16)
    taken = jnp.dot(
        (hot[0] + hot[1]).astype(jnp.bfloat16), before, preferred_element_type=jnp.float32
    )
    picked = [
        jnp.where(flag & (taken == gap.astype(jnp.float32)), 1.0, 0.0)
        for flag, gap in zip(named, offset)
    ]
    logits = logits_ref[...]
    top_logit = jnp.max(logits, axis=0, keepdims=True)
    raised = jnp.exp(logits - top_logit)
    share = raised / jnp.sum(raised, axis=0, keepdims=True)
    weighted = picked[0] * share[0:1, :] + picked[1] * share[1:2, :]
    coarse = weighted.astype(jnp.bfloat16)
    fine = (weighted - coarse.astype(jnp.float32)).astype(jnp.bfloat16)
    sender = (picked[0] + picked[1]).astype(jnp.bfloat16)
    step = width // 4
    for at in range(0, width, step):
        slot_rows = jnp.dot(sender, normed[:, at : at + step], preferred_element_type=jnp.float32)
        for lane in range(0, step, LANES):
            turn[pl.ds((at + lane) // LANES, slots, stride=strip), :] = slot_rows[
                :, lane : lane + LANES
            ]
    x_ref[...] = turn[...].reshape(x_ref.shape).astype(jnp.bfloat16)

    pl.semaphore_wait(barrier, len(peers))
    following = {"ep": lax.rem(me + 1, count)}
    halo = [
        remote(
            buffer.at[:, pl.ds(seq_rows, WINDOW)],
            buffer.at[:, pl.ds(0, WINDOW)],
            hs_sem.at[index],
            hr_sem.at[index],
            following,
        )
        for index, buffer in enumerate((keys, values))
    ]
    for copy in halo:
        copy.start()
    for number in range(1, count):
        out_copy(number).start()
    shared = [
        remote(
            gate_ref.at[0], w1.at[:, pl.ds(inner, inner)], ws_sem.at[0], wr_sem.at[0], partner
        ),
        remote(
            up_ref.at[0], w1.at[:, pl.ds(3 * inner, inner)], ws_sem.at[1], wr_sem.at[1], partner
        ),
        remote(down_ref.at[0], w2.at[pl.ds(inner, inner)], ws_sem.at[2], wr_sem.at[2], partner),
    ]
    for copy in shared:
        copy.start()
    abuf[0] = x_ref[me]

    for head in range(group_heads):
        hat = head_norm(
            query_ref[head * head_size : (head + 1) * head_size, :],
            query_gain_ref[head : head + 1, :],
        )
        for block in range(blocks):
            queries[block, :, head * WINDOW : (head + 1) * WINDOW] = hat[
                :, block * WINDOW : (block + 1) * WINDOW
            ]
    band = (2 * WINDOW, WINDOW)
    key_pos = lax.broadcasted_iota(jnp.int32, band, 0)
    distance = lax.broadcasted_iota(jnp.int32, band, 1) + WINDOW - key_pos
    inside = (distance >= 0) & (distance < WINDOW)
    inside_first = inside & ((key_pos >= WINDOW) | (me > 0))

    def attend(block):
        at = pl.ds(block * WINDOW, 2 * WINDOW)
        scores = contract_rows(keys[:, at], queries[block]) * head_size**-0.5
        allowed = inside_first if block == 0 else inside
        for head in range(group_heads):
            lanes = slice(head * WINDOW, (head + 1) * WINDOW)
            own = jnp.where(allowed, scores[:, lanes], NEGATIVE)
            sink = jnp.full((1, WINDOW), sink_ref[0, head], jnp.float32)
            highest = jnp.maximum(jnp.max(own, axis=0, keepdims=True), sink)
            weights = jnp.exp(own - highest)
            total = jnp.sum(weights, axis=0, keepdims=True) + jnp.exp(sink - highest)
            mixed = jnp.dot(
                values[:, at], weights.astype(jnp.bfloat16), preferred_element_type=jnp.float32
            )
            heads[head * head_size : (head + 1) * head_size, block * WINDOW : (block + 1) * WINDOW] = (
                mixed / total
            ).astype(jnp.bfloat16)

    def project(block):
        owners = WINDOW // tokens // 2
        rows_in = heads[:, block * WINDOW : (block + 1) * WINDOW]
        for at in range(0, width, step):
            part_ref[block * owners : (block + 1) * owners, :, :, at : at + step] = (
                contract_rows(rows_in, project_ref[:, at : at + step])
                .astype(jnp.bfloat16)
                .reshape(owners, 2, tokens, step)
            )

    swap = remote(part_ref.at[:, 1 - core], swapped, swap_sem.at[0], swap_sem.at[1], partner)
    weights_wait = [copy.wait for copy in local] + [copy.wait_recv for copy in shared]
    for name, *rest in plan():
        if name == "attend":
            attend(*rest)
            project(*rest)
        elif name == "halo":
            for copy in halo:
                copy.wait_recv()
        elif name == "swap":
            swap.start()
        elif name == "swapped":
            swap.wait_recv()
            for slot in (4, 3, 5, 2, 6, 1, 7, 0):
                owner = lax.rem(spot + slot, ring)
                pair[slot] = (
                    part_ref[owner, core].astype(jnp.float32) + swapped[owner].astype(jnp.float32)
                ).astype(jnp.bfloat16)
                for half, way, far in CHAINS:
                    if (way * far) % ring == slot:
                        pair_copy(half, way, far).start()
        elif name == "arrive":
            arrive(*rest)
        elif name == "experts":
            while weights_wait:
                weights_wait.pop()()
            compute(*rest)
        elif name == "start":
            sum_copy(*rest).start()
        elif name == "gather":
            group, half, way, hop = rest
            gather_copy(group, half, way, hop).wait_recv()
            if (half, way, hop + 1) in HOPS:
                gather_copy(group, half, way, hop + 1).start()
        elif name == "pair":
            carry_on(pair, prbuf, pair_copy, *rest[1:])
        elif name == "sum":
            group = rest[0]
            carry_on(
                pbuf.at[group],
                rbuf.at[group],
                lambda half, way, hop, group=group: sum_copy(group, half, way, hop),
                *rest[1:],
            )
        elif name == "finish":
            if rest[0] == "pair":
                for half in range(2):
                    attended_ref[:, half_columns(half)] = summed(pair, prbuf, half).astype(
                        jnp.bfloat16
                    )
            else:
                give_back(rest[1])
    back_ref[me] = sbuf[0]
    swap.wait_send()
    for copy in shared + halo:
        copy.wait_send()
    for half, way, hop in HOPS:
        pair_copy(half, way, hop).wait_send()
        for group in range(GROUPS):
            gather_copy(group, half, way, hop).wait_send()
            sum_copy(group, half, way, hop).wait_send()
    for number in range(1, count):
        out_copy(number).wait_send()
        back_copy(number).wait()
    turn[...] = back_ref[...].astype(jnp.float32).reshape(turn.shape)
    for at in range(strip):
        came = turn[pl.ds(at, slots, stride=strip), :].astype(jnp.bfloat16)
        mix_ref[:, at * LANES : (at + 1) * LANES] = (
            contract_rows(coarse, came) + contract_rows(fine, came)
        ).astype(jnp.bfloat16)


def on_device(
    query_rows,
    key_rows,
    value_rows,
    query_gain,
    key_gain,
    sink_logits,
    out_weight,
    expert_input,
    expert_gain,
    routes,
    route_logits,
    gate_weight,
    up_weight,
    down_weight,
):
    own, width = expert_input.shape
    fanout = routes.shape[1]
    count = lax.axis_size("ep")
    capacity = (3 * own * fanout + 2 * count - 1) // (2 * count)
    inner = down_weight.shape[1]
    ring = lax.axis_size("tp") // 2
    rows = count * capacity // GROUPS
    seq_rows, query_width = query_rows.shape
    head_size = key_rows.shape[1]
    message = (count, capacity * width // LANES, LANES)
    hops = len(HOPS)
    dma = pltpu.SemaphoreType.DMA
    vmem = pl.BlockSpec(memory_space=pltpu.VMEM)

    def scratch(*shape):
        return pltpu.VMEM(shape, jnp.bfloat16)

    return pl.pallas_call(
        layer_kernel,
        out_shape=(jax.ShapeDtypeStruct((own, width), jnp.bfloat16),) * 2,
        in_specs=[vmem] * 5
        + [pl.BlockSpec(memory_space=pltpu.SMEM)]
        + [vmem] * 5
        + [pl.BlockSpec(memory_space=pl.ANY)] * 3,
        out_specs=[vmem] * 2,
        scratch_shapes=[
            scratch(*message),
            scratch(*message),
            scratch(head_size, seq_rows + WINDOW),
            scratch(head_size, seq_rows + WINDOW),
            scratch(seq_rows // WINDOW, head_size, query_width // head_size * WINDOW),
            scratch(query_width, seq_rows),
            scratch(ring, 2, own, width),
            scratch(width, 4 * inner),
            scratch(2 * inner, width),
            scratch(*message),
            pltpu.VMEM((count * capacity * width // LANES, LANES), jnp.float32),
            scratch(GROUPS, ring, rows, width),
            scratch(GROUPS, ring, rows, width),
            scratch(GROUPS, hops, rows, width // 2),
            scratch(*message),
            scratch(ring, own, width),
            scratch(ring, own, width),
            scratch(hops, own, width // 2),
            dma((3,)),
            dma((3,)),
            dma((3,)),
            dma((count,)),
            dma((count,)),
            dma((count,)),
            dma((count,)),
            dma((GROUPS, hops)),
            dma((GROUPS, hops)),
            dma((GROUPS, hops)),
            dma((GROUPS, hops)),
            dma((2,)),
            dma((hops,)),
            dma((hops,)),
            dma((2,)),
            dma((2,)),
        ],
        compiler_params=pltpu.CompilerParams(
            collective_id=1, has_side_effects=True, vmem_limit_bytes=VMEM_LIMIT
        ),
        name="layer",
    )(
        query_rows.T,
        key_rows.T,
        value_rows.T,
        query_gain,
        key_gain,
        sink_logits.reshape(1, -1),
        out_weight,
        expert_input,
        expert_gain.reshape(1, -1),
        routes.T,
        route_logits.T,
        gate_weight,
        up_weight,
        down_weight,
    )


def solution(mesh):
    placed = (
        P("ep", "tp"),
        P("ep", "tp"),
        P("ep", "tp"),
        P("tp", None),
        P("tp", None),
        P("tp"),
        P("tp", None),
        P(("ep", "tp"), None),
        P(),
        P(("ep", "tp"), None),
        P(("ep", "tp"), None),
        P("ep", None, "tp"),
        P("ep", None, "tp"),
        P("ep", "tp", None),
    )
    return jax.shard_map(
        on_device,
        mesh=mesh,
        in_specs=placed,
        out_specs=(P(("ep", "tp"), None), P(("ep", "tp"), None)),
        check_vma=False,
    )
```

```python
import heapq

import jax
import jax.numpy as jnp
from jax import lax
from jax.experimental import pallas as pl
from jax.experimental.pallas import tpu as pltpu
from jax.sharding import PartitionSpec as P

WINDOW = 128
EPSILON = 1e-06
CLAMP_LIMIT = 7.0
ACT_SLOPE = 1.702
NEGATIVE = -1e30
CHAINS = ((0, 1, 4), (1, -1, 4), (1, 1, 3), (0, -1, 3))
HOPS = {}
for _half, _way, _far in CHAINS:
    for _hop in range(1, _far + 1):
        HOPS[_half, _way, _hop] = len(HOPS)
X_RING = 4
GROUPS = 4
LANES = 128
FAR = 1024
PAD = 32
VMEM_LIMIT = 60 * 1024 * 1024


def remote(source, target, send_sem, recv_sem, where):
    return pltpu.make_async_remote_copy(
        src_ref=source,
        dst_ref=target,
        send_sem=send_sem,
        recv_sem=recv_sem,
        device_id=where,
        device_id_type=pl.DeviceIdType.MESH,
    )


def column(row):
    size = row.shape[1]
    square = (size, size)
    diagonal = lax.broadcasted_iota(jnp.int32, square, 0) == lax.broadcasted_iota(
        jnp.int32, square, 1
    )
    return jnp.sum(jnp.where(diagonal, jnp.broadcast_to(row, square), 0.0), axis=1, keepdims=True)


def head_norm(rows, gain_row):
    widened = rows.astype(jnp.float32)
    scaled = widened * lax.rsqrt(jnp.mean(widened * widened, axis=0, keepdims=True) + EPSILON)
    return (scaled * column(gain_row)).astype(jnp.bfloat16)


def contract_rows(left, right):
    return lax.dot_general(
        left, right, (((0,), (0,)), ((), ())), preferred_element_type=jnp.float32
    )


def exchange_order(count):
    long = count // X_RING
    order = [(0, across) for across in (0, 1, X_RING - 1, 2)]
    for level in range(1, long // 2):
        for across in (0, 1, X_RING - 1, 2):
            order += [(level, across), (long - level, across)]
    order += [(long // 2, across) for across in (0, 1, X_RING - 1, 2)]
    quarter = count // 4
    return order[:quarter] + order[2 * quarter :] + order[quarter : 2 * quarter]


def plan():
    low = 1.0 - FAR / 2048
    wire = {
        "gather": 2.25 * 2 / GROUPS,
        "sum": 2.25 * 2 / GROUPS * low,
        "pair": 1.5,
        "home": 1.5 * (1.0 - low),
    }
    plane = 13.0
    arrived_far = 0
    delay = 2.0
    free = {1: 0.0, -1: 0.0}
    coming, ready, steps = [], [], []
    serial = iter(range(1 << 20))
    done = set()
    left = {}

    def send(now, kind, group, half, way, hop):
        free[way] = max(free[way], now) + wire[kind]
        heapq.heappush(coming, (free[way] + delay, next(serial), (kind, group, half, way, hop)))

    def task(rank, name, cost):
        heapq.heappush(ready, (rank, next(serial), name, cost))

    for group in range(GROUPS):
        when = 3.0 + 10.0 * group / (GROUPS - 1)
        heapq.heappush(coming, (when, next(serial), ("arrive", group)))
    heapq.heappush(coming, (4.0, next(serial), ("halo",)))
    heapq.heappush(coming, (7.0, next(serial), ("tables",)))
    for block in (1, 2, 3):
        task(0, ("attend", block), 1.7)
    attended = 0
    now = 0.0
    blocked = []
    while coming or ready or blocked:
        arrived = coming and coming[0][0] <= now
        if not arrived and ready:
            rank, _, name, cost = heapq.heappop(ready)
            steps.append(name)
            now += cost
            done.add(name)
            if name[0] == "attend":
                attended += 1
                if attended == 4:
                    steps.append(("swap",))
                    heapq.heappush(coming, (now + 3.5, next(serial), ("swapped",)))
            elif name[0] == "experts":
                _, group, hop = name
                left[group] = left.get(group, 0) + 1
                if left[group] == 5:
                    steps.append(("send_far", group))
                    now += 0.5
                    plane = max(plane, now) + 69.0 / GROUPS * (1.0 - low)
                    heapq.heappush(coming, (plane + 4.0, next(serial), ("far", group)))
                for half, way, far in CHAINS:
                    if hop and far == hop:
                        steps.append(("start", group, half, way, far))
                        send(now, "sum", group, half, way, far)
            elif name[0] == "relay":
                for half, way, far in CHAINS:
                    send(now, "home", 0, half, way, far)
            for entry in blocked:
                heapq.heappush(coming, entry)
            blocked = []
            continue
        if not coming:
            break
        when, number, event = heapq.heappop(coming)
        now = max(now, when)
        if event[0] == "sum":
            _, group, half, way, hop = event
            if ("experts", group, hop - 1) not in done:
                blocked.append((when, number, event))
                continue
        steps.append(event)
        if event[0] == "arrive":
            now += 0.6
            for half, way, far in CHAINS:
                send(now, "gather", event[1], half, way, 1)
            task(2 + event[1], ("experts", event[1], 0), 0.9)
        elif event[0] == "halo":
            task(1, ("attend", 0), 1.7)
        elif event[0] == "tables":
            now += 1.0
        elif event[0] == "far":
            arrived_far += 1
            if arrived_far == GROUPS:
                task(1, ("relay",), 3.0)
        elif event[0] == "swapped":
            now += 0.6
            for half, way, far in CHAINS:
                send(now, "pair", 0, half, way, far)
        elif event[0] == "gather":
            _, group, half, way, hop = event
            now += 0.05
            if (half, way, hop + 1) in HOPS:
                send(now, "gather", group, half, way, hop + 1)
            key = ("gather", group, hop)
            left[key] = left.get(key, 0) + 1
            if left[key] == (4 if hop < 4 else 2):
                task(2 + group, ("experts", group, hop), 1.6 if hop < 4 else 0.9)
        else:
            kind, group, half, way, hop = event
            now += 0.2
            if hop > 1:
                send(now, kind, group, half, way, hop - 1)
            else:
                key = (kind, group)
                left[key] = left.get(key, 0) + 1
                if left[key] == 4:
                    steps.append(("finish", kind, group))
                    now += 0.8
    return steps


def ep_place(me, offset, sign=1):
    across_count = X_RING
    along_count = lax.axis_size("ep") // X_RING
    z, x = lax.div(me, across_count), lax.rem(me, across_count)
    along = (sign * offset[0]) % along_count
    across = (sign * offset[1]) % across_count
    return lax.rem(z + along, along_count) * across_count + lax.rem(x + across, across_count)


def layer_kernel(
    query_ref,
    key_ref,
    value_ref,
    query_gain_ref,
    key_gain_ref,
    sink_ref,
    project_ref,
    input_ref,
    input_gain_ref,
    routes_ref,
    logits_ref,
    gate_ref,
    up_ref,
    down_ref,
    attended_ref,
    mix_ref,
    x_ref,
    back_ref,
    keys,
    values,
    queries,
    heads,
    part_ref,
    w1,
    w2,
    abuf,
    turn,
    xbuf,
    pbuf,
    rbuf,
    sbuf,
    swapped,
    pair,
    prbuf,
    wl_sem,
    ws_sem,
    wr_sem,
    es_sem,
    er_sem,
    bs_sem,
    br_sem,
    gs_sem,
    gr_sem,
    ss_sem,
    sr_sem,
    swap_sem,
    ps_sem,
    pr_sem,
    hs_sem,
    hr_sem,
    wide,
    fsend,
    fbuf,
    tables,
    coarse_all,
    fine_all,
    mixed_part,
    qbuf,
    fs_sem,
    fr_sem,
    ts_sem,
    tr_sem,
    qs_sem,
    qr_sem,
):
    me = lax.axis_index("ep")
    count = lax.axis_size("ep")
    tp = lax.axis_index("tp")
    ring = lax.axis_size("tp") // 2
    core, spot = lax.rem(tp, 2), lax.div(tp, 2)
    ahead = {"tp": lax.rem(spot + 1, ring) * 2 + core}
    behind = {"tp": lax.rem(spot + ring - 1, ring) * 2 + core}
    partner = {"tp": spot * 2 + (1 - core)}
    order = exchange_order(count)
    inner = down_ref.shape[1]
    members = count // GROUPS
    rows, width = xbuf.shape[2], xbuf.shape[3]
    strip = width // LANES
    low = width - FAR
    low_strip = low // LANES

    def around(step):
        return {"tp": lax.rem(spot + step, ring) * 2 + core}

    local = [
        pltpu.make_async_copy(gate_ref.at[0], w1.at[:, pl.ds(0, inner)], wl_sem.at[0]),
        pltpu.make_async_copy(up_ref.at[0], w1.at[:, pl.ds(2 * inner, inner)], wl_sem.at[1]),
        pltpu.make_async_copy(down_ref.at[0], w2.at[pl.ds(0, inner)], wl_sem.at[2]),
    ]
    for copy in local:
        copy.start()
    peers = [around(step) for step in range(1, ring)] + [partner]
    peers += [{"ep": ep_place(me, offset)} for offset in order[1:]]
    barrier = pltpu.get_barrier_semaphore()
    for place in peers:
        pl.semaphore_signal(
            barrier, inc=1, device_id=place, device_id_type=pl.DeviceIdType.MESH
        )

    def out_copy(number):
        peer = ep_place(me, order[number])
        return remote(
            x_ref.at[peer], abuf.at[number], es_sem.at[number], er_sem.at[number], {"ep": peer}
        )

    def back_copy(number):
        peer = ep_place(me, order[number], -1)
        return remote(
            sbuf.at[number], back_ref.at[me], bs_sem.at[number], br_sem.at[number], {"ep": peer}
        )

    def half_columns(half):
        return pl.ds(half * (width // 2), width // 2)

    def low_columns(half):
        return pl.ds(half * (low // 2), low // 2)

    def toward(way):
        return ahead if way == 1 else behind

    def gather_copy(group, half, way, hop):
        number = HOPS[half, way, hop]
        return remote(
            xbuf.at[group, (-way * (hop - 1)) % ring, :, half_columns(half)],
            xbuf.at[group, (-way * hop) % ring, :, half_columns(half)],
            gs_sem.at[group, number],
            gr_sem.at[group, number],
            toward(way),
        )

    def sum_copy(group, half, way, hop):
        number = HOPS[half, way, hop]
        return remote(
            pbuf.at[group, (way * hop) % ring, :, low_columns(half)],
            rbuf.at[group, number],
            ss_sem.at[group, number],
            sr_sem.at[group, number],
            toward(way),
        )

    def pair_copy(half, way, hop):
        number = HOPS[half, way, hop]
        return remote(
            pair.at[(way * hop) % ring, :, half_columns(half)],
            prbuf.at[number],
            ps_sem.at[number],
            pr_sem.at[number],
            toward(way),
        )

    def far_copy(number):
        peer = ep_place(me, order[number], -1)
        return remote(
            fsend.at[number],
            fbuf.at[me, pl.ds(0, fsend.shape[1])],
            fs_sem.at[number],
            fr_sem.at[number],
            {"ep": peer},
        )

    def home_copy(half, way, hop):
        number = HOPS[half, way, hop]
        at = pl.ds(half * (FAR // 2), FAR // 2)
        return remote(
            mixed_part.at[lax.rem(spot + (way * hop) % ring, ring), :, at],
            qbuf.at[number],
            qs_sem.at[number],
            qr_sem.at[number],
            toward(way),
        )

    def table_copy(step):
        return remote(
            tables.at[0], tables.at[step], ts_sem.at[step], tr_sem.at[step], around(step)
        )

    def carry_on(buffer, received, copy_of, columns, half, way, hop):
        copy_of(half, way, hop).wait_recv()
        if hop > 1:
            slot = (way * (hop - 1)) % ring
            if columns is home_columns:
                slot = lax.rem(spot + slot, ring)
            at = columns(half)
            buffer[slot, :, at] = (
                buffer[slot, :, at].astype(jnp.float32)
                + received[HOPS[half, way, hop]].astype(jnp.float32)
            ).astype(jnp.bfloat16)
            copy_of(half, way, hop - 1).start()

    def home_columns(half):
        return pl.ds(half * (FAR // 2), FAR // 2)

    def summed(buffer, received, columns, half, own=0):
        return (
            buffer[own, :, columns(half)].astype(jnp.float32)
            + received[HOPS[half, 1, 1]].astype(jnp.float32)
            + received[HOPS[half, -1, 1]].astype(jnp.float32)
        )

    def experts(group, slot):
        pre = jnp.dot(xbuf[group, slot], w1[...], preferred_element_type=jnp.float32)
        clipped = jnp.minimum(pre[:, : 2 * inner], CLAMP_LIMIT)
        linear = jnp.clip(pre[:, 2 * inner :], -CLAMP_LIMIT, CLAMP_LIMIT)
        hidden = (clipped * jax.nn.sigmoid(ACT_SLOPE * clipped) * (linear + 1.0)).astype(
            jnp.bfloat16
        )
        step = width // 4
        for at in range(0, width, step):
            pbuf[group, slot, :, at : at + step] = jnp.dot(
                hidden, w2[:, at : at + step], preferred_element_type=jnp.float32
            ).astype(jnp.bfloat16)

    def arrive(group):
        for number in range(group * members, (group + 1) * members):
            if number > 0:
                out_copy(number).wait_recv()
        messages = abuf[group * members : (group + 1) * members]
        turn[: rows * strip] = messages.astype(jnp.float32).reshape(rows * strip, LANES)
        for at in range(strip):
            xbuf[group, 0, :, at * LANES : (at + 1) * LANES] = turn[
                pl.ds(at, rows, stride=strip), :
            ].astype(jnp.bfloat16)
        for half, way, far in CHAINS:
            gather_copy(group, half, way, 1).start()

    def compute(group, hop):
        if hop in (0, 4):
            experts(group, hop)
            return

        def both(index, carry):
            experts(group, hop + index * (ring - 2 * hop))
            return carry

        lax.fori_loop(0, 2, both, 0)

    def give_back(group):
        for half in range(2):
            total = summed(pbuf.at[group], rbuf.at[group], low_columns, half)
            for at in range(low_strip // 2):
                turn[pl.ds(half * (low_strip // 2) + at, rows, stride=low_strip), :] = total[
                    :, at * LANES : (at + 1) * LANES
                ]
        sbuf[group * members : (group + 1) * members] = (
            turn[: rows * low_strip].reshape(members, -1, LANES).astype(jnp.bfloat16)
        )
        for number in range(group * members, (group + 1) * members):
            if number > 0:
                back_copy(number).start()

    def send_far(group):
        for slot in range(ring):
            for at in range(FAR // LANES):
                wide[at, slot * rows : (slot + 1) * rows, :] = pbuf[
                    group, slot, :, low + at * LANES : low + (at + 1) * LANES
                ].astype(jnp.float32)
        for member in range(members):
            number = group * members + member
            for at in range(FAR // LANES):
                fsend[number, :, at * LANES : (at + 1) * LANES] = jnp.concatenate(
                    [
                        wide[at, pl.ds(member * capacity + place, ring, stride=rows), :]
                        for place in range(capacity)
                    ],
                    axis=0,
                ).astype(jnp.bfloat16)
            if number > 0:
                far_copy(number).start()
        if group == 0:
            fbuf[me, : fsend.shape[1]] = fsend[0]

    def relay():
        everything = fbuf[...].reshape(count * PAD, FAR)
        for at in range(0, FAR, 256):
            part = everything[:, at : at + 256]
            mixed_part[:, :, at : at + 256] = (
                (contract_rows(coarse_all[...], part) + contract_rows(fine_all[...], part))
                .astype(jnp.bfloat16)
                .reshape(ring, tokens, 256)
            )

    def spread_tables():
        table = tables[0]
        for step in range(1, ring):
            table_copy(step).wait_recv()
            table = table + tables[step]
        lane = lax.broadcasted_iota(jnp.int32, (1, ring * tokens), 1)
        turned = lax.rem(lax.div(lane, tokens) + ring - spot, ring).astype(jnp.float32)
        block = 256
        for at in range(0, count * PAD, block):
            spot_row = lax.broadcasted_iota(jnp.int32, (block, ring * tokens), 0).astype(
                jnp.float32
            ) + float(at)
            total = jnp.zeros((block, ring * tokens), jnp.float32)
            for copy in range(2):
                target = (
                    float(PAD) * table[copy : copy + 1]
                    + float(ring) * table[2 + copy : 3 + copy]
                    + turned
                )
                total += jnp.where(spot_row == target, table[4 + copy : 5 + copy], 0.0)
            rounded = total.astype(jnp.bfloat16)
            coarse_all[at : at + block] = rounded
            fine_all[at : at + block] = (total - rounded.astype(jnp.float32)).astype(jnp.bfloat16)

    head_size = key_ref.shape[0]
    group_heads = query_ref.shape[0] // head_size
    seq_rows = key_ref.shape[1]
    blocks = seq_rows // WINDOW
    slots = count * x_ref.shape[1] // strip
    capacity = x_ref.shape[1] // strip
    tokens = input_ref.shape[0]

    keys[:, WINDOW:] = head_norm(key_ref[...], key_gain_ref[...])
    values[:, WINDOW:] = value_ref[...]

    given = input_ref[...].astype(jnp.float32)
    normed = (
        given
        * lax.rsqrt(jnp.mean(given * given, axis=-1, keepdims=True) + EPSILON)
        * input_gain_ref[...]
    ).astype(jnp.bfloat16)
    place = lax.broadcasted_iota(jnp.int32, (slots, tokens), 0)
    offset = [place - capacity * routes_ref[copy : copy + 1, :] for copy in range(2)]
    named = [(gap >= 0) & (gap < capacity) for gap in offset]
    hot = [jnp.where(flag, 1.0, 0.0) for flag in named]
    square = (tokens, tokens)
    before = jnp.where(
        lax.broadcasted_iota(jnp.int32, square, 0) < lax.broadcasted_iota(jnp.int32, square, 1),
        1.0,
        0.0,
    ).astype(jnp.bfloat16)
    taken = jnp.dot(
        (hot[0] + hot[1]).astype(jnp.bfloat16), before, preferred_element_type=jnp.float32
    )
    picked = [
        jnp.where(flag & (taken == gap.astype(jnp.float32)), 1.0, 0.0)
        for flag, gap in zip(named, offset)
    ]
    logits = logits_ref[...]
    top_logit = jnp.max(logits, axis=0, keepdims=True)
    raised = jnp.exp(logits - top_logit)
    share = raised / jnp.sum(raised, axis=0, keepdims=True)
    weighted = picked[0] * share[0:1, :] + picked[1] * share[1:2, :]
    coarse = weighted.astype(jnp.bfloat16)
    fine = (weighted - coarse.astype(jnp.float32)).astype(jnp.bfloat16)
    sender = (picked[0] + picked[1]).astype(jnp.bfloat16)
    earlier = [
        jnp.sum(jnp.where(gap == 0, taken, 0.0), axis=0, keepdims=True) for gap in offset
    ]
    lines = [routes_ref[copy : copy + 1, :].astype(jnp.float32) for copy in range(2)]
    lines += earlier + [share[0:1, :], share[1:2, :]]
    line = lax.broadcasted_iota(jnp.int32, (8, tokens), 0)
    own_table = jnp.zeros((8, tokens), jnp.float32)
    for index, values_line in enumerate(lines):
        own_table = jnp.where(line == index, values_line, own_table)
    lane_owner = lax.div(lax.broadcasted_iota(jnp.int32, (8, ring * tokens), 1), tokens)
    tables[0] = jnp.where(lane_owner == spot, jnp.concatenate([own_table] * ring, axis=1), 0.0)
    fbuf[:, fsend.shape[1] :, :] = jnp.zeros(
        (count, PAD - fsend.shape[1], FAR), jnp.bfloat16
    )
    stride = width // 4
    for at in range(0, width, stride):
        slot_rows = jnp.dot(sender, normed[:, at : at + stride], preferred_element_type=jnp.float32)
        for lane in range(0, stride, LANES):
            turn[pl.ds((at + lane) // LANES, slots, stride=strip), :] = slot_rows[
                :, lane : lane + LANES
            ]
    x_ref[...] = turn[...].reshape(x_ref.shape).astype(jnp.bfloat16)

    pl.semaphore_wait(barrier, len(peers))
    following = {"ep": lax.rem(me + 1, count)}
    halo = [
        remote(
            buffer.at[:, pl.ds(seq_rows, WINDOW)],
            buffer.at[:, pl.ds(0, WINDOW)],
            hs_sem.at[index],
            hr_sem.at[index],
            following,
        )
        for index, buffer in enumerate((keys, values))
    ]
    for copy in halo:
        copy.start()
    for step in range(1, ring):
        table_copy(step).start()
    for number in range(1, count):
        out_copy(number).start()
    shared = [
        remote(
            gate_ref.at[0], w1.at[:, pl.ds(inner, inner)], ws_sem.at[0], wr_sem.at[0], partner
        ),
        remote(
            up_ref.at[0], w1.at[:, pl.ds(3 * inner, inner)], ws_sem.at[1], wr_sem.at[1], partner
        ),
        remote(down_ref.at[0], w2.at[pl.ds(inner, inner)], ws_sem.at[2], wr_sem.at[2], partner),
    ]
    for copy in shared:
        copy.start()
    abuf[0] = x_ref[me]

    for head in range(group_heads):
        hat = head_norm(
            query_ref[head * head_size : (head + 1) * head_size, :],
            query_gain_ref[head : head + 1, :],
        )
        for block in range(blocks):
            queries[block, :, head * WINDOW : (head + 1) * WINDOW] = hat[
                :, block * WINDOW : (block + 1) * WINDOW
            ]
    band = (2 * WINDOW, WINDOW)
    key_pos = lax.broadcasted_iota(jnp.int32, band, 0)
    distance = lax.broadcasted_iota(jnp.int32, band, 1) + WINDOW - key_pos
    inside = (distance >= 0) & (distance < WINDOW)
    inside_first = inside & ((key_pos >= WINDOW) | (me > 0))

    def attend(block):
        at = pl.ds(block * WINDOW, 2 * WINDOW)
        scores = contract_rows(keys[:, at], queries[block]) * head_size**-0.5
        allowed = inside_first if block == 0 else inside
        for head in range(group_heads):
            lanes = slice(head * WINDOW, (head + 1) * WINDOW)
            own = jnp.where(allowed, scores[:, lanes], NEGATIVE)
            sink = jnp.full((1, WINDOW), sink_ref[0, head], jnp.float32)
            highest = jnp.maximum(jnp.max(own, axis=0, keepdims=True), sink)
            weights = jnp.exp(own - highest)
            total = jnp.sum(weights, axis=0, keepdims=True) + jnp.exp(sink - highest)
            mixed = jnp.dot(
                values[:, at], weights.astype(jnp.bfloat16), preferred_element_type=jnp.float32
            )
            heads[head * head_size : (head + 1) * head_size, block * WINDOW : (block + 1) * WINDOW] = (
                mixed / total
            ).astype(jnp.bfloat16)

    def project(block):
        owners = WINDOW // tokens // 2
        rows_in = heads[:, block * WINDOW : (block + 1) * WINDOW]
        for at in range(0, width, stride):
            part_ref[block * owners : (block + 1) * owners, :, :, at : at + stride] = (
                contract_rows(rows_in, project_ref[:, at : at + stride])
                .astype(jnp.bfloat16)
                .reshape(owners, 2, tokens, stride)
            )

    swap = remote(part_ref.at[:, 1 - core], swapped, swap_sem.at[0], swap_sem.at[1], partner)
    weights_wait = [copy.wait for copy in local] + [copy.wait_recv for copy in shared]
    for name, *rest in plan():
        if name == "attend":
            attend(*rest)
            project(*rest)
        elif name == "halo":
            for copy in halo:
                copy.wait_recv()
        elif name == "swap":
            swap.start()
        elif name == "swapped":
            swap.wait_recv()
            for slot in (4, 3, 5, 2, 6, 1, 7, 0):
                owner = lax.rem(spot + slot, ring)
                pair[slot] = (
                    part_ref[owner, core].astype(jnp.float32) + swapped[owner].astype(jnp.float32)
                ).astype(jnp.bfloat16)
                for half, way, far in CHAINS:
                    if (way * far) % ring == slot:
                        pair_copy(half, way, far).start()
        elif name == "arrive":
            arrive(*rest)
        elif name == "experts":
            while weights_wait:
                weights_wait.pop()()
            compute(*rest)
        elif name == "start":
            sum_copy(*rest).start()
        elif name == "gather":
            group, half, way, hop = rest
            gather_copy(group, half, way, hop).wait_recv()
            if (half, way, hop + 1) in HOPS:
                gather_copy(group, half, way, hop + 1).start()
        elif name == "pair":
            carry_on(pair, prbuf, pair_copy, half_columns, *rest[1:])
        elif name == "home":
            carry_on(mixed_part, qbuf, home_copy, home_columns, *rest[1:])
        elif name == "tables":
            spread_tables()
        elif name == "send_far":
            send_far(*rest)
        elif name == "far":
            for number in range(rest[0] * members, (rest[0] + 1) * members):
                if number > 0:
                    far_copy(number).wait_recv()
        elif name == "relay":
            relay()
            for half, way, far in CHAINS:
                home_copy(half, way, far).start()
        elif name == "sum":
            group = rest[0]
            carry_on(
                pbuf.at[group],
                rbuf.at[group],
                lambda half, way, hop, group=group: sum_copy(group, half, way, hop),
                low_columns,
                *rest[1:],
            )
        elif name == "finish":
            if rest[0] == "pair":
                for half in range(2):
                    attended_ref[:, half_columns(half)] = summed(
                        pair, prbuf, half_columns, half
                    ).astype(jnp.bfloat16)
            elif rest[0] == "home":
                for half in range(2):
                    at = pl.ds(low + half * (FAR // 2), FAR // 2)
                    mix_ref[:, at] = summed(mixed_part, qbuf, home_columns, half, spot).astype(
                        jnp.bfloat16
                    )
            else:
                give_back(rest[1])
    back_ref[me] = sbuf[0]
    swap.wait_send()
    for copy in shared + halo:
        copy.wait_send()
    for half, way, hop in HOPS:
        pair_copy(half, way, hop).wait_send()
        home_copy(half, way, hop).wait_send()
        for group in range(GROUPS):
            gather_copy(group, half, way, hop).wait_send()
            sum_copy(group, half, way, hop).wait_send()
    for number in range(1, count):
        out_copy(number).wait_send()
        far_copy(number).wait_send()
        back_copy(number).wait()
    for step in range(1, ring):
        table_copy(step).wait_send()
    turn[: slots * low_strip] = back_ref[...].astype(jnp.float32).reshape(-1, LANES)
    for at in range(low_strip):
        came = turn[pl.ds(at, slots, stride=low_strip), :].astype(jnp.bfloat16)
        mix_ref[:, at * LANES : (at + 1) * LANES] = (
            contract_rows(coarse, came) + contract_rows(fine, came)
        ).astype(jnp.bfloat16)


def on_device(
    query_rows,
    key_rows,
    value_rows,
    query_gain,
    key_gain,
    sink_logits,
    out_weight,
    expert_input,
    expert_gain,
    routes,
    route_logits,
    gate_weight,
    up_weight,
    down_weight,
):
    own, width = expert_input.shape
    fanout = routes.shape[1]
    count = lax.axis_size("ep")
    capacity = (3 * own * fanout + 2 * count - 1) // (2 * count)
    inner = down_weight.shape[1]
    ring = lax.axis_size("tp") // 2
    rows = count * capacity // GROUPS
    seq_rows, query_width = query_rows.shape
    head_size = key_rows.shape[1]
    message = (count, capacity * width // LANES, LANES)
    low_message = (count, capacity * (width - FAR) // LANES, LANES)
    hops = len(HOPS)
    dma = pltpu.SemaphoreType.DMA
    vmem = pl.BlockSpec(memory_space=pltpu.VMEM)

    def scratch(*shape):
        return pltpu.VMEM(shape, jnp.bfloat16)

    return pl.pallas_call(
        layer_kernel,
        out_shape=(jax.ShapeDtypeStruct((own, width), jnp.bfloat16),) * 2,
        in_specs=[vmem] * 5
        + [pl.BlockSpec(memory_space=pltpu.SMEM)]
        + [vmem] * 5
        + [pl.BlockSpec(memory_space=pl.ANY)] * 3,
        out_specs=[vmem] * 2,
        scratch_shapes=[
            scratch(*message),
            scratch(*low_message),
            scratch(head_size, seq_rows + WINDOW),
            scratch(head_size, seq_rows + WINDOW),
            scratch(seq_rows // WINDOW, head_size, query_width // head_size * WINDOW),
            scratch(query_width, seq_rows),
            scratch(ring, 2, own, width),
            scratch(width, 4 * inner),
            scratch(2 * inner, width),
            scratch(*message),
            pltpu.VMEM((count * capacity * width // LANES, LANES), jnp.float32),
            scratch(GROUPS, ring, rows, width),
            scratch(GROUPS, ring, rows, width),
            scratch(GROUPS, hops, rows, (width - FAR) // 2),
            scratch(*low_message),
            scratch(ring, own, width),
            scratch(ring, own, width),
            scratch(hops, own, width // 2),
            dma((3,)),
            dma((3,)),
            dma((3,)),
            dma((count,)),
            dma((count,)),
            dma((count,)),
            dma((count,)),
            dma((GROUPS, hops)),
            dma((GROUPS, hops)),
            dma((GROUPS, hops)),
            dma((GROUPS, hops)),
            dma((2,)),
            dma((hops,)),
            dma((hops,)),
            dma((2,)),
            dma((2,)),
            pltpu.VMEM((FAR // LANES, ring * rows, LANES), jnp.float32),
            scratch(count, ring * capacity, FAR),
            scratch(count, PAD, FAR),
            pltpu.VMEM((ring, 8, ring * own), jnp.float32),
            scratch(count * PAD, ring * own),
            scratch(count * PAD, ring * own),
            scratch(ring, own, FAR),
            scratch(hops, own, FAR // 2),
            dma((count,)),
            dma((count,)),
            dma((ring,)),
            dma((ring,)),
            dma((hops,)),
            dma((hops,)),
        ],
        compiler_params=pltpu.CompilerParams(
            collective_id=1, has_side_effects=True, vmem_limit_bytes=VMEM_LIMIT
        ),
        name="layer",
    )(
        query_rows.T,
        key_rows.T,
        value_rows.T,
        query_gain,
        key_gain,
        sink_logits.reshape(1, -1),
        out_weight,
        expert_input,
        expert_gain.reshape(1, -1),
        routes.T,
        route_logits.T,
        gate_weight,
        up_weight,
        down_weight,
    )


def solution(mesh):
    placed = (
        P("ep", "tp"),
        P("ep", "tp"),
        P("ep", "tp"),
        P("tp", None),
        P("tp", None),
        P("tp"),
        P("tp", None),
        P(("ep", "tp"), None),
        P(),
        P(("ep", "tp"), None),
        P(("ep", "tp"), None),
        P("ep", None, "tp"),
        P("ep", None, "tp"),
        P("ep", "tp", None),
    )
    return jax.shard_map(
        on_device,
        mesh=mesh,
        in_specs=placed,
        out_specs=(P(("ep", "tp"), None), P(("ep", "tp"), None)),
        check_vma=False,
    )
```

```python
import heapq

import jax
import jax.numpy as jnp
from jax import lax
from jax.experimental import pallas as pl
from jax.experimental.pallas import tpu as pltpu
from jax.sharding import PartitionSpec as P

WINDOW = 128
EPSILON = 1e-06
CLAMP_LIMIT = 7.0
ACT_SLOPE = 1.702
NEGATIVE = -1e30
CHAINS = ((0, 1, 4), (1, -1, 4), (1, 1, 3), (0, -1, 3))
HOPS = {}
for _half, _way, _far in CHAINS:
    for _hop in range(1, _far + 1):
        HOPS[_half, _way, _hop] = len(HOPS)
X_RING = 4
GROUPS = 4
LANES = 128
FAR = 512
PAD = 32
VMEM_LIMIT = 60 * 1024 * 1024


def remote(source, target, send_sem, recv_sem, where):
    return pltpu.make_async_remote_copy(
        src_ref=source,
        dst_ref=target,
        send_sem=send_sem,
        recv_sem=recv_sem,
        device_id=where,
        device_id_type=pl.DeviceIdType.MESH,
    )


def column(row):
    size = row.shape[1]
    square = (size, size)
    diagonal = lax.broadcasted_iota(jnp.int32, square, 0) == lax.broadcasted_iota(
        jnp.int32, square, 1
    )
    return jnp.sum(jnp.where(diagonal, jnp.broadcast_to(row, square), 0.0), axis=1, keepdims=True)


def head_norm(rows, gain_row):
    widened = rows.astype(jnp.float32)
    scaled = widened * lax.rsqrt(jnp.mean(widened * widened, axis=0, keepdims=True) + EPSILON)
    return (scaled * column(gain_row)).astype(jnp.bfloat16)


def contract_rows(left, right):
    return lax.dot_general(
        left, right, (((0,), (0,)), ((), ())), preferred_element_type=jnp.float32
    )


def exchange_order(count):
    long = count // X_RING
    order = [(0, across) for across in (0, 1, X_RING - 1, 2)]
    for level in range(1, long // 2):
        for across in (0, 1, X_RING - 1, 2):
            order += [(level, across), (long - level, across)]
    order += [(long // 2, across) for across in (0, 1, X_RING - 1, 2)]
    quarter = count // 4
    return order[:quarter] + order[2 * quarter :] + order[quarter : 2 * quarter]


def plan():
    low = 1.0 - FAR / 2048
    wire = {
        "gather": 2.25 * 2 / GROUPS,
        "sum": 2.25 * 2 / GROUPS * low,
        "pair": 1.5,
        "home": 1.5 * (1.0 - low),
    }
    plane = 13.0
    arrived_far = 0
    delay = 2.0
    free = {1: 0.0, -1: 0.0}
    coming, ready, steps = [], [], []
    serial = iter(range(1 << 20))
    done = set()
    left = {}

    def send(now, kind, group, half, way, hop):
        free[way] = max(free[way], now) + wire[kind]
        heapq.heappush(coming, (free[way] + delay, next(serial), (kind, group, half, way, hop)))

    def task(rank, name, cost):
        heapq.heappush(ready, (rank, next(serial), name, cost))

    for group in range(GROUPS):
        when = 3.0 + 10.0 * group / (GROUPS - 1)
        heapq.heappush(coming, (when, next(serial), ("arrive", group)))
    heapq.heappush(coming, (4.0, next(serial), ("halo",)))
    heapq.heappush(coming, (7.0, next(serial), ("tables",)))
    for block in (1, 2, 3):
        task(0, ("attend", block), 1.7)
    attended = 0
    now = 0.0
    blocked = []
    while coming or ready or blocked:
        arrived = coming and coming[0][0] <= now
        if not arrived and ready:
            rank, _, name, cost = heapq.heappop(ready)
            steps.append(name)
            now += cost
            done.add(name)
            if name[0] == "attend":
                attended += 1
                if attended == 4:
                    steps.append(("swap",))
                    heapq.heappush(coming, (now + 3.5, next(serial), ("swapped",)))
            elif name[0] == "experts":
                _, group, hop = name
                left[group] = left.get(group, 0) + 1
                if left[group] == 5:
                    steps.append(("send_far", group))
                    now += 0.5
                    plane = max(plane, now) + 69.0 / GROUPS * (1.0 - low)
                    heapq.heappush(coming, (plane + 4.0, next(serial), ("far", group)))
                for half, way, far in CHAINS:
                    if hop and far == hop:
                        steps.append(("start", group, half, way, far))
                        send(now, "sum", group, half, way, far)
            elif name[0] == "relay":
                for half, way, far in CHAINS:
                    send(now, "home", 0, half, way, far)
            for entry in blocked:
                heapq.heappush(coming, entry)
            blocked = []
            continue
        if not coming:
            break
        when, number, event = heapq.heappop(coming)
        now = max(now, when)
        if event[0] == "sum":
            _, group, half, way, hop = event
            if ("experts", group, hop - 1) not in done:
                blocked.append((when, number, event))
                continue
        steps.append(event)
        if event[0] == "arrive":
            now += 0.6
            for half, way, far in CHAINS:
                send(now, "gather", event[1], half, way, 1)
            task(2 + event[1], ("experts", event[1], 0), 0.9)
        elif event[0] == "halo":
            task(1, ("attend", 0), 1.7)
        elif event[0] == "tables":
            now += 1.0
        elif event[0] == "far":
            arrived_far += 1
            if arrived_far == GROUPS:
                task(1, ("relay",), 3.0)
        elif event[0] == "swapped":
            now += 0.6
            for half, way, far in CHAINS:
                send(now, "pair", 0, half, way, far)
        elif event[0] == "gather":
            _, group, half, way, hop = event
            now += 0.05
            if (half, way, hop + 1) in HOPS:
                send(now, "gather", group, half, way, hop + 1)
            key = ("gather", group, hop)
            left[key] = left.get(key, 0) + 1
            if left[key] == (4 if hop < 4 else 2):
                task(2 + group, ("experts", group, hop), 1.6 if hop < 4 else 0.9)
        else:
            kind, group, half, way, hop = event
            now += 0.2
            if hop > 1:
                send(now, kind, group, half, way, hop - 1)
            else:
                key = (kind, group)
                left[key] = left.get(key, 0) + 1
                if left[key] == 4:
                    steps.append(("finish", kind, group))
                    now += 0.8
    return steps


def ep_place(me, offset, sign=1):
    across_count = X_RING
    along_count = lax.axis_size("ep") // X_RING
    z, x = lax.div(me, across_count), lax.rem(me, across_count)
    along = (sign * offset[0]) % along_count
    across = (sign * offset[1]) % across_count
    return lax.rem(z + along, along_count) * across_count + lax.rem(x + across, across_count)


def layer_kernel(
    query_ref,
    key_ref,
    value_ref,
    query_gain_ref,
    key_gain_ref,
    sink_ref,
    project_ref,
    input_ref,
    input_gain_ref,
    routes_ref,
    logits_ref,
    gate_ref,
    up_ref,
    down_ref,
    attended_ref,
    mix_ref,
    x_ref,
    back_ref,
    keys,
    values,
    queries,
    heads,
    part_ref,
    w1,
    w2,
    abuf,
    turn,
    xbuf,
    pbuf,
    rbuf,
    sbuf,
    swapped,
    pair,
    prbuf,
    wl_sem,
    ws_sem,
    wr_sem,
    es_sem,
    er_sem,
    bs_sem,
    br_sem,
    gs_sem,
    gr_sem,
    ss_sem,
    sr_sem,
    swap_sem,
    ps_sem,
    pr_sem,
    hs_sem,
    hr_sem,
    wide,
    fsend,
    fbuf,
    tables,
    coarse_all,
    fine_all,
    mixed_part,
    qbuf,
    fs_sem,
    fr_sem,
    ts_sem,
    tr_sem,
    qs_sem,
    qr_sem,
):
    me = lax.axis_index("ep")
    count = lax.axis_size("ep")
    tp = lax.axis_index("tp")
    ring = lax.axis_size("tp") // 2
    core, spot = lax.rem(tp, 2), lax.div(tp, 2)
    ahead = {"tp": lax.rem(spot + 1, ring) * 2 + core}
    behind = {"tp": lax.rem(spot + ring - 1, ring) * 2 + core}
    partner = {"tp": spot * 2 + (1 - core)}
    order = exchange_order(count)
    inner = down_ref.shape[1]
    members = count // GROUPS
    rows, width = xbuf.shape[2], xbuf.shape[3]
    strip = width // LANES
    low = width - FAR
    low_strip = low // LANES

    def around(step):
        return {"tp": lax.rem(spot + step, ring) * 2 + core}

    local = [
        pltpu.make_async_copy(gate_ref.at[0], w1.at[:, pl.ds(0, inner)], wl_sem.at[0]),
        pltpu.make_async_copy(up_ref.at[0], w1.at[:, pl.ds(2 * inner, inner)], wl_sem.at[1]),
        pltpu.make_async_copy(down_ref.at[0], w2.at[pl.ds(0, inner)], wl_sem.at[2]),
    ]
    for copy in local:
        copy.start()
    peers = [around(step) for step in range(1, ring)] + [partner]
    peers += [{"ep": ep_place(me, offset)} for offset in order[1:]]
    barrier = pltpu.get_barrier_semaphore()
    for place in peers:
        pl.semaphore_signal(
            barrier, inc=1, device_id=place, device_id_type=pl.DeviceIdType.MESH
        )

    def out_copy(number):
        peer = ep_place(me, order[number])
        return remote(
            x_ref.at[peer], abuf.at[number], es_sem.at[number], er_sem.at[number], {"ep": peer}
        )

    def back_copy(number):
        peer = ep_place(me, order[number], -1)
        return remote(
            sbuf.at[number], back_ref.at[me], bs_sem.at[number], br_sem.at[number], {"ep": peer}
        )

    def half_columns(half):
        return pl.ds(half * (width // 2), width // 2)

    def low_columns(half):
        return pl.ds(half * (low // 2), low // 2)

    def toward(way):
        return ahead if way == 1 else behind

    def gather_copy(group, half, way, hop):
        number = HOPS[half, way, hop]
        return remote(
            xbuf.at[group, (-way * (hop - 1)) % ring, :, half_columns(half)],
            xbuf.at[group, (-way * hop) % ring, :, half_columns(half)],
            gs_sem.at[group, number],
            gr_sem.at[group, number],
            toward(way),
        )

    def sum_copy(group, half, way, hop):
        number = HOPS[half, way, hop]
        return remote(
            pbuf.at[group, (way * hop) % ring, :, low_columns(half)],
            rbuf.at[group, number],
            ss_sem.at[group, number],
            sr_sem.at[group, number],
            toward(way),
        )

    def pair_copy(half, way, hop):
        number = HOPS[half, way, hop]
        return remote(
            pair.at[(way * hop) % ring, :, half_columns(half)],
            prbuf.at[number],
            ps_sem.at[number],
            pr_sem.at[number],
            toward(way),
        )

    def far_copy(number):
        peer = ep_place(me, order[number], -1)
        return remote(
            fsend.at[number],
            fbuf.at[me, pl.ds(0, fsend.shape[1])],
            fs_sem.at[number],
            fr_sem.at[number],
            {"ep": peer},
        )

    def home_copy(half, way, hop):
        number = HOPS[half, way, hop]
        at = pl.ds(half * (FAR // 2), FAR // 2)
        return remote(
            mixed_part.at[lax.rem(spot + (way * hop) % ring, ring), :, at],
            qbuf.at[number],
            qs_sem.at[number],
            qr_sem.at[number],
            toward(way),
        )

    def table_copy(step):
        return remote(
            tables.at[0], tables.at[step], ts_sem.at[step], tr_sem.at[step], around(step)
        )

    def carry_on(buffer, received, copy_of, columns, half, way, hop):
        copy_of(half, way, hop).wait_recv()
        if hop > 1:
            slot = (way * (hop - 1)) % ring
            if columns is home_columns:
                slot = lax.rem(spot + slot, ring)
            at = columns(half)
            buffer[slot, :, at] = (
                buffer[slot, :, at].astype(jnp.float32)
                + received[HOPS[half, way, hop]].astype(jnp.float32)
            ).astype(jnp.bfloat16)
            copy_of(half, way, hop - 1).start()

    def home_columns(half):
        return pl.ds(half * (FAR // 2), FAR // 2)

    def summed(buffer, received, columns, half, own=0):
        return (
            buffer[own, :, columns(half)].astype(jnp.float32)
            + received[HOPS[half, 1, 1]].astype(jnp.float32)
            + received[HOPS[half, -1, 1]].astype(jnp.float32)
        )

    def experts(group, slot):
        pre = jnp.dot(xbuf[group, slot], w1[...], preferred_element_type=jnp.float32)
        clipped = jnp.minimum(pre[:, : 2 * inner], CLAMP_LIMIT)
        linear = jnp.clip(pre[:, 2 * inner :], -CLAMP_LIMIT, CLAMP_LIMIT)
        hidden = (clipped * jax.nn.sigmoid(ACT_SLOPE * clipped) * (linear + 1.0)).astype(
            jnp.bfloat16
        )
        step = width // 4
        for at in range(0, width, step):
            pbuf[group, slot, :, at : at + step] = jnp.dot(
                hidden, w2[:, at : at + step], preferred_element_type=jnp.float32
            ).astype(jnp.bfloat16)

    def arrive(group):
        for number in range(group * members, (group + 1) * members):
            if number > 0:
                out_copy(number).wait_recv()
        messages = abuf[group * members : (group + 1) * members]
        turn[: rows * strip] = messages.astype(jnp.float32).reshape(rows * strip, LANES)
        for at in range(strip):
            xbuf[group, 0, :, at * LANES : (at + 1) * LANES] = turn[
                pl.ds(at, rows, stride=strip), :
            ].astype(jnp.bfloat16)
        for half, way, far in CHAINS:
            gather_copy(group, half, way, 1).start()

    def compute(group, hop):
        if hop in (0, 4):
            experts(group, hop)
            return

        def both(index, carry):
            experts(group, hop + index * (ring - 2 * hop))
            return carry

        lax.fori_loop(0, 2, both, 0)

    def give_back(group):
        for half in range(2):
            total = summed(pbuf.at[group], rbuf.at[group], low_columns, half)
            for at in range(low_strip // 2):
                turn[pl.ds(half * (low_strip // 2) + at, rows, stride=low_strip), :] = total[
                    :, at * LANES : (at + 1) * LANES
                ]
        sbuf[group * members : (group + 1) * members] = (
            turn[: rows * low_strip].reshape(members, -1, LANES).astype(jnp.bfloat16)
        )
        for number in range(group * members, (group + 1) * members):
            if number > 0:
                back_copy(number).start()

    def send_far(group):
        for slot in range(ring):
            for at in range(FAR // LANES):
                wide[at, slot * rows : (slot + 1) * rows, :] = pbuf[
                    group, slot, :, low + at * LANES : low + (at + 1) * LANES
                ].astype(jnp.float32)
        for member in range(members):
            number = group * members + member
            for at in range(FAR // LANES):
                fsend[number, :, at * LANES : (at + 1) * LANES] = jnp.concatenate(
                    [
                        wide[at, pl.ds(member * capacity + place, ring, stride=rows), :]
                        for place in range(capacity)
                    ],
                    axis=0,
                ).astype(jnp.bfloat16)
            if number > 0:
                far_copy(number).start()
        if group == 0:
            fbuf[me, : fsend.shape[1]] = fsend[0]

    def relay():
        everything = fbuf[...].reshape(count * PAD, FAR)
        for at in range(0, FAR, 256):
            part = everything[:, at : at + 256]
            mixed_part[:, :, at : at + 256] = (
                (contract_rows(coarse_all[...], part) + contract_rows(fine_all[...], part))
                .astype(jnp.bfloat16)
                .reshape(ring, tokens, 256)
            )

    def spread_tables():
        table = tables[0]
        for step in range(1, ring):
            table_copy(step).wait_recv()
            table = table + tables[step]
        lane = lax.broadcasted_iota(jnp.int32, (1, ring * tokens), 1)
        turned = lax.rem(lax.div(lane, tokens) + ring - spot, ring).astype(jnp.float32)
        block = 256
        for at in range(0, count * PAD, block):
            spot_row = lax.broadcasted_iota(jnp.int32, (block, ring * tokens), 0).astype(
                jnp.float32
            ) + float(at)
            total = jnp.zeros((block, ring * tokens), jnp.float32)
            for copy in range(2):
                target = (
                    float(PAD) * table[copy : copy + 1]
                    + float(ring) * table[2 + copy : 3 + copy]
                    + turned
                )
                total += jnp.where(spot_row == target, table[4 + copy : 5 + copy], 0.0)
            rounded = total.astype(jnp.bfloat16)
            coarse_all[at : at + block] = rounded
            fine_all[at : at + block] = (total - rounded.astype(jnp.float32)).astype(jnp.bfloat16)

    head_size = key_ref.shape[0]
    group_heads = query_ref.shape[0] // head_size
    seq_rows = key_ref.shape[1]
    blocks = seq_rows // WINDOW
    slots = count * x_ref.shape[1] // strip
    capacity = x_ref.shape[1] // strip
    tokens = input_ref.shape[0]

    keys[:, WINDOW:] = head_norm(key_ref[...], key_gain_ref[...])
    values[:, WINDOW:] = value_ref[...]

    given = input_ref[...].astype(jnp.float32)
    normed = (
        given
        * lax.rsqrt(jnp.mean(given * given, axis=-1, keepdims=True) + EPSILON)
        * input_gain_ref[...]
    ).astype(jnp.bfloat16)
    place = lax.broadcasted_iota(jnp.int32, (slots, tokens), 0)
    offset = [place - capacity * routes_ref[copy : copy + 1, :] for copy in range(2)]
    named = [(gap >= 0) & (gap < capacity) for gap in offset]
    hot = [jnp.where(flag, 1.0, 0.0) for flag in named]
    square = (tokens, tokens)
    before = jnp.where(
        lax.broadcasted_iota(jnp.int32, square, 0) < lax.broadcasted_iota(jnp.int32, square, 1),
        1.0,
        0.0,
    ).astype(jnp.bfloat16)
    taken = jnp.dot(
        (hot[0] + hot[1]).astype(jnp.bfloat16), before, preferred_element_type=jnp.float32
    )
    picked = [
        jnp.where(flag & (taken == gap.astype(jnp.float32)), 1.0, 0.0)
        for flag, gap in zip(named, offset)
    ]
    logits = logits_ref[...]
    top_logit = jnp.max(logits, axis=0, keepdims=True)
    raised = jnp.exp(logits - top_logit)
    share = raised / jnp.sum(raised, axis=0, keepdims=True)
    weighted = picked[0] * share[0:1, :] + picked[1] * share[1:2, :]
    coarse = weighted.astype(jnp.bfloat16)
    fine = (weighted - coarse.astype(jnp.float32)).astype(jnp.bfloat16)
    sender = (picked[0] + picked[1]).astype(jnp.bfloat16)
    earlier = [
        jnp.sum(jnp.where(gap == 0, taken, 0.0), axis=0, keepdims=True) for gap in offset
    ]
    lines = [routes_ref[copy : copy + 1, :].astype(jnp.float32) for copy in range(2)]
    lines += earlier + [share[0:1, :], share[1:2, :]]
    line = lax.broadcasted_iota(jnp.int32, (8, tokens), 0)
    own_table = jnp.zeros((8, tokens), jnp.float32)
    for index, values_line in enumerate(lines):
        own_table = jnp.where(line == index, values_line, own_table)
    lane_owner = lax.div(lax.broadcasted_iota(jnp.int32, (8, ring * tokens), 1), tokens)
    tables[0] = jnp.where(lane_owner == spot, jnp.concatenate([own_table] * ring, axis=1), 0.0)
    fbuf[:, fsend.shape[1] :, :] = jnp.zeros(
        (count, PAD - fsend.shape[1], FAR), jnp.bfloat16
    )
    stride = width // 4
    for at in range(0, width, stride):
        slot_rows = jnp.dot(sender, normed[:, at : at + stride], preferred_element_type=jnp.float32)
        for lane in range(0, stride, LANES):
            turn[pl.ds((at + lane) // LANES, slots, stride=strip), :] = slot_rows[
                :, lane : lane + LANES
            ]
    x_ref[...] = turn[...].reshape(x_ref.shape).astype(jnp.bfloat16)

    pl.semaphore_wait(barrier, len(peers))
    following = {"ep": lax.rem(me + 1, count)}
    halo = [
        remote(
            buffer.at[:, pl.ds(seq_rows, WINDOW)],
            buffer.at[:, pl.ds(0, WINDOW)],
            hs_sem.at[index],
            hr_sem.at[index],
            following,
        )
        for index, buffer in enumerate((keys, values))
    ]
    for copy in halo:
        copy.start()
    for step in range(1, ring):
        table_copy(step).start()
    for number in range(1, count):
        out_copy(number).start()
    shared = [
        remote(
            gate_ref.at[0], w1.at[:, pl.ds(inner, inner)], ws_sem.at[0], wr_sem.at[0], partner
        ),
        remote(
            up_ref.at[0], w1.at[:, pl.ds(3 * inner, inner)], ws_sem.at[1], wr_sem.at[1], partner
        ),
        remote(down_ref.at[0], w2.at[pl.ds(inner, inner)], ws_sem.at[2], wr_sem.at[2], partner),
    ]
    for copy in shared:
        copy.start()
    abuf[0] = x_ref[me]

    for head in range(group_heads):
        hat = head_norm(
            query_ref[head * head_size : (head + 1) * head_size, :],
            query_gain_ref[head : head + 1, :],
        )
        for block in range(blocks):
            queries[block, :, head * WINDOW : (head + 1) * WINDOW] = hat[
                :, block * WINDOW : (block + 1) * WINDOW
            ]
    band = (2 * WINDOW, WINDOW)
    key_pos = lax.broadcasted_iota(jnp.int32, band, 0)
    distance = lax.broadcasted_iota(jnp.int32, band, 1) + WINDOW - key_pos
    inside = (distance >= 0) & (distance < WINDOW)
    inside_first = inside & ((key_pos >= WINDOW) | (me > 0))

    def attend(block):
        at = pl.ds(block * WINDOW, 2 * WINDOW)
        scores = contract_rows(keys[:, at], queries[block]) * head_size**-0.5
        allowed = inside_first if block == 0 else inside
        for head in range(group_heads):
            lanes = slice(head * WINDOW, (head + 1) * WINDOW)
            own = jnp.where(allowed, scores[:, lanes], NEGATIVE)
            sink = jnp.full((1, WINDOW), sink_ref[0, head], jnp.float32)
            highest = jnp.maximum(jnp.max(own, axis=0, keepdims=True), sink)
            weights = jnp.exp(own - highest)
            total = jnp.sum(weights, axis=0, keepdims=True) + jnp.exp(sink - highest)
            mixed = jnp.dot(
                values[:, at], weights.astype(jnp.bfloat16), preferred_element_type=jnp.float32
            )
            heads[head * head_size : (head + 1) * head_size, block * WINDOW : (block + 1) * WINDOW] = (
                mixed / total
            ).astype(jnp.bfloat16)

    def project(block):
        owners = WINDOW // tokens // 2
        rows_in = heads[:, block * WINDOW : (block + 1) * WINDOW]
        for at in range(0, width, stride):
            part_ref[block * owners : (block + 1) * owners, :, :, at : at + stride] = (
                contract_rows(rows_in, project_ref[:, at : at + stride])
                .astype(jnp.bfloat16)
                .reshape(owners, 2, tokens, stride)
            )

    swap = remote(part_ref.at[:, 1 - core], swapped, swap_sem.at[0], swap_sem.at[1], partner)
    weights_wait = [copy.wait for copy in local] + [copy.wait_recv for copy in shared]
    for name, *rest in plan():
        if name == "attend":
            attend(*rest)
            project(*rest)
        elif name == "halo":
            for copy in halo:
                copy.wait_recv()
        elif name == "swap":
            swap.start()
        elif name == "swapped":
            swap.wait_recv()
            for slot in (4, 3, 5, 2, 6, 1, 7, 0):
                owner = lax.rem(spot + slot, ring)
                pair[slot] = (
                    part_ref[owner, core].astype(jnp.float32) + swapped[owner].astype(jnp.float32)
                ).astype(jnp.bfloat16)
                for half, way, far in CHAINS:
                    if (way * far) % ring == slot:
                        pair_copy(half, way, far).start()
        elif name == "arrive":
            arrive(*rest)
        elif name == "experts":
            while weights_wait:
                weights_wait.pop()()
            compute(*rest)
        elif name == "start":
            sum_copy(*rest).start()
        elif name == "gather":
            group, half, way, hop = rest
            gather_copy(group, half, way, hop).wait_recv()
            if (half, way, hop + 1) in HOPS:
                gather_copy(group, half, way, hop + 1).start()
        elif name == "pair":
            carry_on(pair, prbuf, pair_copy, half_columns, *rest[1:])
        elif name == "home":
            carry_on(mixed_part, qbuf, home_copy, home_columns, *rest[1:])
        elif name == "tables":
            spread_tables()
        elif name == "send_far":
            send_far(*rest)
        elif name == "far":
            for number in range(rest[0] * members, (rest[0] + 1) * members):
                if number > 0:
                    far_copy(number).wait_recv()
        elif name == "relay":
            relay()
            for half, way, far in CHAINS:
                home_copy(half, way, far).start()
        elif name == "sum":
            group = rest[0]
            carry_on(
                pbuf.at[group],
                rbuf.at[group],
                lambda half, way, hop, group=group: sum_copy(group, half, way, hop),
                low_columns,
                *rest[1:],
            )
        elif name == "finish":
            if rest[0] == "pair":
                for half in range(2):
                    attended_ref[:, half_columns(half)] = summed(
                        pair, prbuf, half_columns, half
                    ).astype(jnp.bfloat16)
            elif rest[0] == "home":
                for half in range(2):
                    at = pl.ds(low + half * (FAR // 2), FAR // 2)
                    mix_ref[:, at] = summed(mixed_part, qbuf, home_columns, half, spot).astype(
                        jnp.bfloat16
                    )
            else:
                give_back(rest[1])
    back_ref[me] = sbuf[0]
    swap.wait_send()
    for copy in shared + halo:
        copy.wait_send()
    for half, way, hop in HOPS:
        pair_copy(half, way, hop).wait_send()
        home_copy(half, way, hop).wait_send()
        for group in range(GROUPS):
            gather_copy(group, half, way, hop).wait_send()
            sum_copy(group, half, way, hop).wait_send()
    for number in range(1, count):
        out_copy(number).wait_send()
        far_copy(number).wait_send()
        back_copy(number).wait()
    for step in range(1, ring):
        table_copy(step).wait_send()
    turn[: slots * low_strip] = back_ref[...].astype(jnp.float32).reshape(-1, LANES)
    for at in range(low_strip):
        came = turn[pl.ds(at, slots, stride=low_strip), :].astype(jnp.bfloat16)
        mix_ref[:, at * LANES : (at + 1) * LANES] = (
            contract_rows(coarse, came) + contract_rows(fine, came)
        ).astype(jnp.bfloat16)


def on_device(
    query_rows,
    key_rows,
    value_rows,
    query_gain,
    key_gain,
    sink_logits,
    out_weight,
    expert_input,
    expert_gain,
    routes,
    route_logits,
    gate_weight,
    up_weight,
    down_weight,
):
    own, width = expert_input.shape
    fanout = routes.shape[1]
    count = lax.axis_size("ep")
    capacity = (3 * own * fanout + 2 * count - 1) // (2 * count)
    inner = down_weight.shape[1]
    ring = lax.axis_size("tp") // 2
    rows = count * capacity // GROUPS
    seq_rows, query_width = query_rows.shape
    head_size = key_rows.shape[1]
    message = (count, capacity * width // LANES, LANES)
    low_message = (count, capacity * (width - FAR) // LANES, LANES)
    hops = len(HOPS)
    dma = pltpu.SemaphoreType.DMA
    vmem = pl.BlockSpec(memory_space=pltpu.VMEM)

    def scratch(*shape):
        return pltpu.VMEM(shape, jnp.bfloat16)

    return pl.pallas_call(
        layer_kernel,
        out_shape=(jax.ShapeDtypeStruct((own, width), jnp.bfloat16),) * 2,
        in_specs=[vmem] * 5
        + [pl.BlockSpec(memory_space=pltpu.SMEM)]
        + [vmem] * 5
        + [pl.BlockSpec(memory_space=pl.ANY)] * 3,
        out_specs=[vmem] * 2,
        scratch_shapes=[
            scratch(*message),
            scratch(*low_message),
            scratch(head_size, seq_rows + WINDOW),
            scratch(head_size, seq_rows + WINDOW),
            scratch(seq_rows // WINDOW, head_size, query_width // head_size * WINDOW),
            scratch(query_width, seq_rows),
            scratch(ring, 2, own, width),
            scratch(width, 4 * inner),
            scratch(2 * inner, width),
            scratch(*message),
            pltpu.VMEM((count * capacity * width // LANES, LANES), jnp.float32),
            scratch(GROUPS, ring, rows, width),
            scratch(GROUPS, ring, rows, width),
            scratch(GROUPS, hops, rows, (width - FAR) // 2),
            scratch(*low_message),
            scratch(ring, own, width),
            scratch(ring, own, width),
            scratch(hops, own, width // 2),
            dma((3,)),
            dma((3,)),
            dma((3,)),
            dma((count,)),
            dma((count,)),
            dma((count,)),
            dma((count,)),
            dma((GROUPS, hops)),
            dma((GROUPS, hops)),
            dma((GROUPS, hops)),
            dma((GROUPS, hops)),
            dma((2,)),
            dma((hops,)),
            dma((hops,)),
            dma((2,)),
            dma((2,)),
            pltpu.VMEM((FAR // LANES, ring * rows, LANES), jnp.float32),
            scratch(count, ring * capacity, FAR),
            scratch(count, PAD, FAR),
            pltpu.VMEM((ring, 8, ring * own), jnp.float32),
            scratch(count * PAD, ring * own),
            scratch(count * PAD, ring * own),
            scratch(ring, own, FAR),
            scratch(hops, own, FAR // 2),
            dma((count,)),
            dma((count,)),
            dma((ring,)),
            dma((ring,)),
            dma((hops,)),
            dma((hops,)),
        ],
        compiler_params=pltpu.CompilerParams(
            collective_id=1, has_side_effects=True, vmem_limit_bytes=VMEM_LIMIT
        ),
        name="layer",
    )(
        query_rows.T,
        key_rows.T,
        value_rows.T,
        query_gain,
        key_gain,
        sink_logits.reshape(1, -1),
        out_weight,
        expert_input,
        expert_gain.reshape(1, -1),
        routes.T,
        route_logits.T,
        gate_weight,
        up_weight,
        down_weight,
    )


def solution(mesh):
    placed = (
        P("ep", "tp"),
        P("ep", "tp"),
        P("ep", "tp"),
        P("tp", None),
        P("tp", None),
        P("tp"),
        P("tp", None),
        P(("ep", "tp"), None),
        P(),
        P(("ep", "tp"), None),
        P(("ep", "tp"), None),
        P("ep", None, "tp"),
        P("ep", None, "tp"),
        P("ep", "tp", None),
    )
    return jax.shard_map(
        on_device,
        mesh=mesh,
        in_specs=placed,
        out_specs=(P(("ep", "tp"), None), P(("ep", "tp"), None)),
        check_vma=False,
    )
```

```python
import heapq

import jax
import jax.numpy as jnp
from jax import lax
from jax.experimental import pallas as pl
from jax.experimental.pallas import tpu as pltpu
from jax.sharding import PartitionSpec as P

WINDOW = 128
EPSILON = 1e-06
CLAMP_LIMIT = 7.0
ACT_SLOPE = 1.702
NEGATIVE = -1e30
CHAINS = ((0, 1, 4), (1, -1, 4), (1, 1, 3), (0, -1, 3))
HOPS = {}
for _half, _way, _far in CHAINS:
    for _hop in range(1, _far + 1):
        HOPS[_half, _way, _hop] = len(HOPS)
X_RING = 4
GROUPS = 4
LANES = 128
FAR = 512
PAD = 32
VMEM_LIMIT = 60 * 1024 * 1024


def remote(source, target, send_sem, recv_sem, where):
    return pltpu.make_async_remote_copy(
        src_ref=source,
        dst_ref=target,
        send_sem=send_sem,
        recv_sem=recv_sem,
        device_id=where,
        device_id_type=pl.DeviceIdType.MESH,
    )


def column(row):
    size = row.shape[1]
    square = (size, size)
    diagonal = lax.broadcasted_iota(jnp.int32, square, 0) == lax.broadcasted_iota(
        jnp.int32, square, 1
    )
    return jnp.sum(jnp.where(diagonal, jnp.broadcast_to(row, square), 0.0), axis=1, keepdims=True)


def head_norm(rows, gain_row):
    widened = rows.astype(jnp.float32)
    scaled = widened * lax.rsqrt(jnp.mean(widened * widened, axis=0, keepdims=True) + EPSILON)
    return (scaled * column(gain_row)).astype(jnp.bfloat16)


def contract_rows(left, right):
    return lax.dot_general(
        left, right, (((0,), (0,)), ((), ())), preferred_element_type=jnp.float32
    )


def exchange_order(count):
    long = count // X_RING
    order = [(0, across) for across in (0, 1, X_RING - 1, 2)]
    for level in range(1, long // 2):
        for across in (0, 1, X_RING - 1, 2):
            order += [(level, across), (long - level, across)]
    order += [(long // 2, across) for across in (0, 1, X_RING - 1, 2)]
    quarter = count // 4
    return order[: 2 * quarter] + order[3 * quarter :] + order[2 * quarter : 3 * quarter]


def plan():
    low = 1.0 - FAR / 2048
    wire = {
        "gather": 2.25 * 2 / GROUPS,
        "sum": 2.25 * 2 / GROUPS * low,
        "pair": 1.5,
        "home": 1.5 * (1.0 - low),
    }
    plane = 13.0
    arrived_far = 0
    delay = 2.0
    free = {1: 0.0, -1: 0.0}
    coming, ready, steps = [], [], []
    serial = iter(range(1 << 20))
    done = set()
    left = {}

    def send(now, kind, group, half, way, hop):
        free[way] = max(free[way], now) + wire[kind]
        heapq.heappush(coming, (free[way] + delay, next(serial), (kind, group, half, way, hop)))

    def task(rank, name, cost):
        heapq.heappush(ready, (rank, next(serial), name, cost))

    for group in range(GROUPS):
        when = 3.0 + 10.0 * group / (GROUPS - 1)
        heapq.heappush(coming, (when, next(serial), ("arrive", group)))
    heapq.heappush(coming, (4.0, next(serial), ("halo",)))
    heapq.heappush(coming, (7.0, next(serial), ("tables",)))
    for block in (1, 2, 3):
        task(0, ("attend", block), 1.7)
    attended = 0
    now = 0.0
    blocked = []
    while coming or ready or blocked:
        arrived = coming and coming[0][0] <= now
        if not arrived and ready:
            rank, _, name, cost = heapq.heappop(ready)
            steps.append(name)
            now += cost
            done.add(name)
            if name[0] == "attend":
                attended += 1
                if attended == 4:
                    steps.append(("swap",))
                    heapq.heappush(coming, (now + 3.5, next(serial), ("swapped",)))
            elif name[0] == "experts":
                _, group, hop = name
                left[group] = left.get(group, 0) + 1
                if left[group] == 5:
                    steps.append(("send_far", group))
                    now += 0.5
                    plane = max(plane, now) + 69.0 / GROUPS * (1.0 - low)
                    heapq.heappush(coming, (plane + 4.0, next(serial), ("far", group)))
                for half, way, far in CHAINS:
                    if hop and far == hop:
                        steps.append(("start", group, half, way, far))
                        send(now, "sum", group, half, way, far)
            elif name[0] == "relay":
                for half, way, far in CHAINS:
                    send(now, "home", 0, half, way, far)
            for entry in blocked:
                heapq.heappush(coming, entry)
            blocked = []
            continue
        if not coming:
            break
        when, number, event = heapq.heappop(coming)
        now = max(now, when)
        if event[0] == "sum":
            _, group, half, way, hop = event
            if ("experts", group, hop - 1) not in done:
                blocked.append((when, number, event))
                continue
        steps.append(event)
        if event[0] == "arrive":
            now += 0.6
            for half, way, far in CHAINS:
                send(now, "gather", event[1], half, way, 1)
            task(2 + event[1], ("experts", event[1], 0), 0.9)
        elif event[0] == "halo":
            task(1, ("attend", 0), 1.7)
        elif event[0] == "tables":
            now += 1.0
        elif event[0] == "far":
            arrived_far += 1
            if arrived_far == GROUPS:
                task(1, ("relay",), 3.0)
        elif event[0] == "swapped":
            now += 0.6
            for half, way, far in CHAINS:
                send(now, "pair", 0, half, way, far)
        elif event[0] == "gather":
            _, group, half, way, hop = event
            now += 0.05
            if (half, way, hop + 1) in HOPS:
                send(now, "gather", group, half, way, hop + 1)
            key = ("gather", group, hop)
            left[key] = left.get(key, 0) + 1
            if left[key] == (4 if hop < 4 else 2):
                task(2 + group, ("experts", group, hop), 1.6 if hop < 4 else 0.9)
        else:
            kind, group, half, way, hop = event
            now += 0.2
            if hop > 1:
                send(now, kind, group, half, way, hop - 1)
            else:
                key = (kind, group)
                left[key] = left.get(key, 0) + 1
                if left[key] == 4:
                    steps.append(("finish", kind, group))
                    now += 0.8
    return steps


def ep_place(me, offset, sign=1):
    across_count = X_RING
    along_count = lax.axis_size("ep") // X_RING
    z, x = lax.div(me, across_count), lax.rem(me, across_count)
    along = (sign * offset[0]) % along_count
    across = (sign * offset[1]) % across_count
    return lax.rem(z + along, along_count) * across_count + lax.rem(x + across, across_count)


def layer_kernel(
    query_ref,
    key_ref,
    value_ref,
    query_gain_ref,
    key_gain_ref,
    sink_ref,
    project_ref,
    input_ref,
    input_gain_ref,
    routes_ref,
    logits_ref,
    gate_ref,
    up_ref,
    down_ref,
    attended_ref,
    mix_ref,
    x_ref,
    back_ref,
    keys,
    values,
    queries,
    heads,
    part_ref,
    w1,
    w2,
    abuf,
    turn,
    xbuf,
    pbuf,
    rbuf,
    sbuf,
    swapped,
    pair,
    prbuf,
    wl_sem,
    ws_sem,
    wr_sem,
    es_sem,
    er_sem,
    bs_sem,
    br_sem,
    gs_sem,
    gr_sem,
    ss_sem,
    sr_sem,
    swap_sem,
    ps_sem,
    pr_sem,
    hs_sem,
    hr_sem,
    wide,
    fsend,
    fbuf,
    tables,
    coarse_all,
    fine_all,
    mixed_part,
    qbuf,
    fs_sem,
    fr_sem,
    ts_sem,
    tr_sem,
    qs_sem,
    qr_sem,
):
    me = lax.axis_index("ep")
    count = lax.axis_size("ep")
    tp = lax.axis_index("tp")
    ring = lax.axis_size("tp") // 2
    core, spot = lax.rem(tp, 2), lax.div(tp, 2)
    ahead = {"tp": lax.rem(spot + 1, ring) * 2 + core}
    behind = {"tp": lax.rem(spot + ring - 1, ring) * 2 + core}
    partner = {"tp": spot * 2 + (1 - core)}
    order = exchange_order(count)
    inner = down_ref.shape[1]
    members = count // GROUPS
    rows, width = xbuf.shape[2], xbuf.shape[3]
    strip = width // LANES
    low = width - FAR
    low_strip = low // LANES

    def around(step):
        return {"tp": lax.rem(spot + step, ring) * 2 + core}

    local = [
        pltpu.make_async_copy(gate_ref.at[0], w1.at[:, pl.ds(0, inner)], wl_sem.at[0]),
        pltpu.make_async_copy(up_ref.at[0], w1.at[:, pl.ds(2 * inner, inner)], wl_sem.at[1]),
        pltpu.make_async_copy(down_ref.at[0], w2.at[pl.ds(0, inner)], wl_sem.at[2]),
    ]
    for copy in local:
        copy.start()
    peers = [around(step) for step in range(1, ring)] + [partner]
    peers += [{"ep": ep_place(me, offset)} for offset in order[1:]]
    barrier = pltpu.get_barrier_semaphore()
    for place in peers:
        pl.semaphore_signal(
            barrier, inc=1, device_id=place, device_id_type=pl.DeviceIdType.MESH
        )

    def out_copy(number):
        peer = ep_place(me, order[number])
        return remote(
            x_ref.at[peer], abuf.at[number], es_sem.at[number], er_sem.at[number], {"ep": peer}
        )

    def back_copy(number):
        peer = ep_place(me, order[number], -1)
        return remote(
            sbuf.at[number], back_ref.at[me], bs_sem.at[number], br_sem.at[number], {"ep": peer}
        )

    def half_columns(half):
        return pl.ds(half * (width // 2), width // 2)

    def low_columns(half):
        return pl.ds(half * (low // 2), low // 2)

    def toward(way):
        return ahead if way == 1 else behind

    def gather_copy(group, half, way, hop):
        number = HOPS[half, way, hop]
        return remote(
            xbuf.at[group, (-way * (hop - 1)) % ring, :, half_columns(half)],
            xbuf.at[group, (-way * hop) % ring, :, half_columns(half)],
            gs_sem.at[group, number],
            gr_sem.at[group, number],
            toward(way),
        )

    def sum_copy(group, half, way, hop):
        number = HOPS[half, way, hop]
        return remote(
            pbuf.at[group, (way * hop) % ring, :, low_columns(half)],
            rbuf.at[group, number],
            ss_sem.at[group, number],
            sr_sem.at[group, number],
            toward(way),
        )

    def pair_copy(half, way, hop):
        number = HOPS[half, way, hop]
        return remote(
            pair.at[(way * hop) % ring, :, half_columns(half)],
            prbuf.at[number],
            ps_sem.at[number],
            pr_sem.at[number],
            toward(way),
        )

    def far_copy(number):
        peer = ep_place(me, order[number], -1)
        return remote(
            fsend.at[number],
            fbuf.at[me, pl.ds(0, fsend.shape[1])],
            fs_sem.at[number],
            fr_sem.at[number],
            {"ep": peer},
        )

    def home_copy(half, way, hop):
        number = HOPS[half, way, hop]
        at = pl.ds(half * (FAR // 2), FAR // 2)
        return remote(
            mixed_part.at[lax.rem(spot + (way * hop) % ring, ring), :, at],
            qbuf.at[number],
            qs_sem.at[number],
            qr_sem.at[number],
            toward(way),
        )

    def table_copy(step):
        return remote(
            tables.at[0], tables.at[step], ts_sem.at[step], tr_sem.at[step], around(step)
        )

    def carry_on(buffer, received, copy_of, columns, half, way, hop):
        copy_of(half, way, hop).wait_recv()
        if hop > 1:
            slot = (way * (hop - 1)) % ring
            if columns is home_columns:
                slot = lax.rem(spot + slot, ring)
            at = columns(half)
            buffer[slot, :, at] = (
                buffer[slot, :, at].astype(jnp.float32)
                + received[HOPS[half, way, hop]].astype(jnp.float32)
            ).astype(jnp.bfloat16)
            copy_of(half, way, hop - 1).start()

    def home_columns(half):
        return pl.ds(half * (FAR // 2), FAR // 2)

    def summed(buffer, received, columns, half, own=0):
        return (
            buffer[own, :, columns(half)].astype(jnp.float32)
            + received[HOPS[half, 1, 1]].astype(jnp.float32)
            + received[HOPS[half, -1, 1]].astype(jnp.float32)
        )

    def experts(group, slot):
        pre = jnp.dot(xbuf[group, slot], w1[...], preferred_element_type=jnp.float32)
        clipped = jnp.minimum(pre[:, : 2 * inner], CLAMP_LIMIT)
        linear = jnp.clip(pre[:, 2 * inner :], -CLAMP_LIMIT, CLAMP_LIMIT)
        hidden = (clipped * jax.nn.sigmoid(ACT_SLOPE * clipped) * (linear + 1.0)).astype(
            jnp.bfloat16
        )
        step = width // 4
        for at in range(0, width, step):
            pbuf[group, slot, :, at : at + step] = jnp.dot(
                hidden, w2[:, at : at + step], preferred_element_type=jnp.float32
            ).astype(jnp.bfloat16)

    def arrive(group):
        for number in range(group * members, (group + 1) * members):
            if number > 0:
                out_copy(number).wait_recv()
        messages = abuf[group * members : (group + 1) * members]
        turn[: rows * strip] = messages.astype(jnp.float32).reshape(rows * strip, LANES)
        for at in range(strip):
            xbuf[group, 0, :, at * LANES : (at + 1) * LANES] = turn[
                pl.ds(at, rows, stride=strip), :
            ].astype(jnp.bfloat16)
        for half, way, far in CHAINS:
            gather_copy(group, half, way, 1).start()

    def compute(group, hop):
        if hop in (0, 4):
            experts(group, hop)
            return

        def both(index, carry):
            experts(group, hop + index * (ring - 2 * hop))
            return carry

        lax.fori_loop(0, 2, both, 0)

    def give_back(group):
        for half in range(2):
            total = summed(pbuf.at[group], rbuf.at[group], low_columns, half)
            for at in range(low_strip // 2):
                turn[pl.ds(half * (low_strip // 2) + at, rows, stride=low_strip), :] = total[
                    :, at * LANES : (at + 1) * LANES
                ]
        sbuf[group * members : (group + 1) * members] = (
            turn[: rows * low_strip].reshape(members, -1, LANES).astype(jnp.bfloat16)
        )
        for number in range(group * members, (group + 1) * members):
            if number > 0:
                back_copy(number).start()

    def send_far(group):
        for slot in range(ring):
            for at in range(FAR // LANES):
                wide[at, slot * rows : (slot + 1) * rows, :] = pbuf[
                    group, slot, :, low + at * LANES : low + (at + 1) * LANES
                ].astype(jnp.float32)
        for member in range(members):
            number = group * members + member
            for at in range(FAR // LANES):
                fsend[number, :, at * LANES : (at + 1) * LANES] = jnp.concatenate(
                    [
                        wide[at, pl.ds(member * capacity + place, ring, stride=rows), :]
                        for place in range(capacity)
                    ],
                    axis=0,
                ).astype(jnp.bfloat16)
            if number > 0:
                far_copy(number).start()
        if group == 0:
            fbuf[me, : fsend.shape[1]] = fsend[0]

    def relay():
        everything = fbuf[...].reshape(count * PAD, FAR)
        for at in range(0, FAR, 256):
            part = everything[:, at : at + 256]
            mixed_part[:, :, at : at + 256] = (
                (contract_rows(coarse_all[...], part) + contract_rows(fine_all[...], part))
                .astype(jnp.bfloat16)
                .reshape(ring, tokens, 256)
            )

    def spread_tables():
        table = tables[0]
        for step in range(1, ring):
            table_copy(step).wait_recv()
            table = table + tables[step]
        lane = lax.broadcasted_iota(jnp.int32, (1, ring * tokens), 1)
        turned = lax.rem(lax.div(lane, tokens) + ring - spot, ring).astype(jnp.float32)
        block = 256
        for at in range(0, count * PAD, block):
            spot_row = lax.broadcasted_iota(jnp.int32, (block, ring * tokens), 0).astype(
                jnp.float32
            ) + float(at)
            total = jnp.zeros((block, ring * tokens), jnp.float32)
            for copy in range(2):
                target = (
                    float(PAD) * table[copy : copy + 1]
                    + float(ring) * table[2 + copy : 3 + copy]
                    + turned
                )
                total += jnp.where(spot_row == target, table[4 + copy : 5 + copy], 0.0)
            rounded = total.astype(jnp.bfloat16)
            coarse_all[at : at + block] = rounded
            fine_all[at : at + block] = (total - rounded.astype(jnp.float32)).astype(jnp.bfloat16)

    head_size = key_ref.shape[0]
    group_heads = query_ref.shape[0] // head_size
    seq_rows = key_ref.shape[1]
    blocks = seq_rows // WINDOW
    slots = count * x_ref.shape[1] // strip
    capacity = x_ref.shape[1] // strip
    tokens = input_ref.shape[0]

    keys[:, WINDOW:] = head_norm(key_ref[...], key_gain_ref[...])
    values[:, WINDOW:] = value_ref[...]

    given = input_ref[...].astype(jnp.float32)
    normed = (
        given
        * lax.rsqrt(jnp.mean(given * given, axis=-1, keepdims=True) + EPSILON)
        * input_gain_ref[...]
    ).astype(jnp.bfloat16)
    place = lax.broadcasted_iota(jnp.int32, (slots, tokens), 0)
    offset = [place - capacity * routes_ref[copy : copy + 1, :] for copy in range(2)]
    named = [(gap >= 0) & (gap < capacity) for gap in offset]
    hot = [jnp.where(flag, 1.0, 0.0) for flag in named]
    square = (tokens, tokens)
    before = jnp.where(
        lax.broadcasted_iota(jnp.int32, square, 0) < lax.broadcasted_iota(jnp.int32, square, 1),
        1.0,
        0.0,
    ).astype(jnp.bfloat16)
    taken = jnp.dot(
        (hot[0] + hot[1]).astype(jnp.bfloat16), before, preferred_element_type=jnp.float32
    )
    picked = [
        jnp.where(flag & (taken == gap.astype(jnp.float32)), 1.0, 0.0)
        for flag, gap in zip(named, offset)
    ]
    logits = logits_ref[...]
    top_logit = jnp.max(logits, axis=0, keepdims=True)
    raised = jnp.exp(logits - top_logit)
    share = raised / jnp.sum(raised, axis=0, keepdims=True)
    weighted = picked[0] * share[0:1, :] + picked[1] * share[1:2, :]
    coarse = weighted.astype(jnp.bfloat16)
    fine = (weighted - coarse.astype(jnp.float32)).astype(jnp.bfloat16)
    sender = (picked[0] + picked[1]).astype(jnp.bfloat16)
    earlier = [
        jnp.sum(jnp.where(gap == 0, taken, 0.0), axis=0, keepdims=True) for gap in offset
    ]
    lines = [routes_ref[copy : copy + 1, :].astype(jnp.float32) for copy in range(2)]
    lines += earlier + [share[0:1, :], share[1:2, :]]
    line = lax.broadcasted_iota(jnp.int32, (8, tokens), 0)
    own_table = jnp.zeros((8, tokens), jnp.float32)
    for index, values_line in enumerate(lines):
        own_table = jnp.where(line == index, values_line, own_table)
    lane_owner = lax.div(lax.broadcasted_iota(jnp.int32, (8, ring * tokens), 1), tokens)
    tables[0] = jnp.where(lane_owner == spot, jnp.concatenate([own_table] * ring, axis=1), 0.0)
    fbuf[:, fsend.shape[1] :, :] = jnp.zeros(
        (count, PAD - fsend.shape[1], FAR), jnp.bfloat16
    )
    stride = width // 4
    for at in range(0, width, stride):
        slot_rows = jnp.dot(sender, normed[:, at : at + stride], preferred_element_type=jnp.float32)
        for lane in range(0, stride, LANES):
            turn[pl.ds((at + lane) // LANES, slots, stride=strip), :] = slot_rows[
                :, lane : lane + LANES
            ]
    x_ref[...] = turn[...].reshape(x_ref.shape).astype(jnp.bfloat16)

    pl.semaphore_wait(barrier, len(peers))
    following = {"ep": lax.rem(me + 1, count)}
    halo = [
        remote(
            buffer.at[:, pl.ds(seq_rows, WINDOW)],
            buffer.at[:, pl.ds(0, WINDOW)],
            hs_sem.at[index],
            hr_sem.at[index],
            following,
        )
        for index, buffer in enumerate((keys, values))
    ]
    for copy in halo:
        copy.start()
    for step in range(1, ring):
        table_copy(step).start()
    for number in range(1, count):
        out_copy(number).start()
    shared = [
        remote(
            gate_ref.at[0], w1.at[:, pl.ds(inner, inner)], ws_sem.at[0], wr_sem.at[0], partner
        ),
        remote(
            up_ref.at[0], w1.at[:, pl.ds(3 * inner, inner)], ws_sem.at[1], wr_sem.at[1], partner
        ),
        remote(down_ref.at[0], w2.at[pl.ds(inner, inner)], ws_sem.at[2], wr_sem.at[2], partner),
    ]
    for copy in shared:
        copy.start()
    abuf[0] = x_ref[me]

    for head in range(group_heads):
        hat = head_norm(
            query_ref[head * head_size : (head + 1) * head_size, :],
            query_gain_ref[head : head + 1, :],
        )
        for block in range(blocks):
            queries[block, :, head * WINDOW : (head + 1) * WINDOW] = hat[
                :, block * WINDOW : (block + 1) * WINDOW
            ]
    band = (2 * WINDOW, WINDOW)
    key_pos = lax.broadcasted_iota(jnp.int32, band, 0)
    distance = lax.broadcasted_iota(jnp.int32, band, 1) + WINDOW - key_pos
    inside = (distance >= 0) & (distance < WINDOW)
    inside_first = inside & ((key_pos >= WINDOW) | (me > 0))

    def attend(block):
        at = pl.ds(block * WINDOW, 2 * WINDOW)
        scores = contract_rows(keys[:, at], queries[block]) * head_size**-0.5
        allowed = inside_first if block == 0 else inside
        for head in range(group_heads):
            lanes = slice(head * WINDOW, (head + 1) * WINDOW)
            own = jnp.where(allowed, scores[:, lanes], NEGATIVE)
            sink = jnp.full((1, WINDOW), sink_ref[0, head], jnp.float32)
            highest = jnp.maximum(jnp.max(own, axis=0, keepdims=True), sink)
            weights = jnp.exp(own - highest)
            total = jnp.sum(weights, axis=0, keepdims=True) + jnp.exp(sink - highest)
            mixed = jnp.dot(
                values[:, at], weights.astype(jnp.bfloat16), preferred_element_type=jnp.float32
            )
            heads[head * head_size : (head + 1) * head_size, block * WINDOW : (block + 1) * WINDOW] = (
                mixed / total
            ).astype(jnp.bfloat16)

    def project(block):
        owners = WINDOW // tokens // 2
        rows_in = heads[:, block * WINDOW : (block + 1) * WINDOW]
        for at in range(0, width, stride):
            part_ref[block * owners : (block + 1) * owners, :, :, at : at + stride] = (
                contract_rows(rows_in, project_ref[:, at : at + stride])
                .astype(jnp.bfloat16)
                .reshape(owners, 2, tokens, stride)
            )

    swap = remote(part_ref.at[:, 1 - core], swapped, swap_sem.at[0], swap_sem.at[1], partner)
    weights_wait = [copy.wait for copy in local] + [copy.wait_recv for copy in shared]
    for name, *rest in plan():
        if name == "attend":
            attend(*rest)
            project(*rest)
        elif name == "halo":
            for copy in halo:
                copy.wait_recv()
        elif name == "swap":
            swap.start()
        elif name == "swapped":
            swap.wait_recv()
            for slot in (4, 3, 5, 2, 6, 1, 7, 0):
                owner = lax.rem(spot + slot, ring)
                pair[slot] = (
                    part_ref[owner, core].astype(jnp.float32) + swapped[owner].astype(jnp.float32)
                ).astype(jnp.bfloat16)
                for half, way, far in CHAINS:
                    if (way * far) % ring == slot:
                        pair_copy(half, way, far).start()
        elif name == "arrive":
            arrive(*rest)
        elif name == "experts":
            while weights_wait:
                weights_wait.pop()()
            compute(*rest)
        elif name == "start":
            sum_copy(*rest).start()
        elif name == "gather":
            group, half, way, hop = rest
            gather_copy(group, half, way, hop).wait_recv()
            if (half, way, hop + 1) in HOPS:
                gather_copy(group, half, way, hop + 1).start()
        elif name == "pair":
            carry_on(pair, prbuf, pair_copy, half_columns, *rest[1:])
        elif name == "home":
            carry_on(mixed_part, qbuf, home_copy, home_columns, *rest[1:])
        elif name == "tables":
            spread_tables()
        elif name == "send_far":
            send_far(*rest)
        elif name == "far":
            for number in range(rest[0] * members, (rest[0] + 1) * members):
                if number > 0:
                    far_copy(number).wait_recv()
        elif name == "relay":
            relay()
            for half, way, far in CHAINS:
                home_copy(half, way, far).start()
        elif name == "sum":
            group = rest[0]
            carry_on(
                pbuf.at[group],
                rbuf.at[group],
                lambda half, way, hop, group=group: sum_copy(group, half, way, hop),
                low_columns,
                *rest[1:],
            )
        elif name == "finish":
            if rest[0] == "pair":
                for half in range(2):
                    attended_ref[:, half_columns(half)] = summed(
                        pair, prbuf, half_columns, half
                    ).astype(jnp.bfloat16)
            elif rest[0] == "home":
                for half in range(2):
                    at = pl.ds(low + half * (FAR // 2), FAR // 2)
                    mix_ref[:, at] = summed(mixed_part, qbuf, home_columns, half, spot).astype(
                        jnp.bfloat16
                    )
            else:
                give_back(rest[1])
    back_ref[me] = sbuf[0]
    swap.wait_send()
    for copy in shared + halo:
        copy.wait_send()
    for half, way, hop in HOPS:
        pair_copy(half, way, hop).wait_send()
        home_copy(half, way, hop).wait_send()
        for group in range(GROUPS):
            gather_copy(group, half, way, hop).wait_send()
            sum_copy(group, half, way, hop).wait_send()
    for number in range(1, count):
        out_copy(number).wait_send()
        far_copy(number).wait_send()
        back_copy(number).wait()
    for step in range(1, ring):
        table_copy(step).wait_send()
    turn[: slots * low_strip] = back_ref[...].astype(jnp.float32).reshape(-1, LANES)
    for at in range(0, low_strip, 4):
        came = jnp.concatenate(
            [turn[pl.ds(at + i, slots, stride=low_strip), :].astype(jnp.bfloat16) for i in range(4)],
            axis=1,
        )
        mix_ref[:, at * LANES : (at + 4) * LANES] = (
            contract_rows(coarse, came) + contract_rows(fine, came)
        ).astype(jnp.bfloat16)


def on_device(
    query_rows,
    key_rows,
    value_rows,
    query_gain,
    key_gain,
    sink_logits,
    out_weight,
    expert_input,
    expert_gain,
    routes,
    route_logits,
    gate_weight,
    up_weight,
    down_weight,
):
    own, width = expert_input.shape
    fanout = routes.shape[1]
    count = lax.axis_size("ep")
    capacity = (3 * own * fanout + 2 * count - 1) // (2 * count)
    inner = down_weight.shape[1]
    ring = lax.axis_size("tp") // 2
    rows = count * capacity // GROUPS
    seq_rows, query_width = query_rows.shape
    head_size = key_rows.shape[1]
    message = (count, capacity * width // LANES, LANES)
    low_message = (count, capacity * (width - FAR) // LANES, LANES)
    hops = len(HOPS)
    dma = pltpu.SemaphoreType.DMA
    vmem = pl.BlockSpec(memory_space=pltpu.VMEM)

    def scratch(*shape):
        return pltpu.VMEM(shape, jnp.bfloat16)

    return pl.pallas_call(
        layer_kernel,
        out_shape=(jax.ShapeDtypeStruct((own, width), jnp.bfloat16),) * 2,
        in_specs=[vmem] * 5
        + [pl.BlockSpec(memory_space=pltpu.SMEM)]
        + [vmem] * 5
        + [pl.BlockSpec(memory_space=pl.ANY)] * 3,
        out_specs=[vmem] * 2,
        scratch_shapes=[
            scratch(*message),
            scratch(*low_message),
            scratch(head_size, seq_rows + WINDOW),
            scratch(head_size, seq_rows + WINDOW),
            scratch(seq_rows // WINDOW, head_size, query_width // head_size * WINDOW),
            scratch(query_width, seq_rows),
            scratch(ring, 2, own, width),
            scratch(width, 4 * inner),
            scratch(2 * inner, width),
            scratch(*message),
            pltpu.VMEM((count * capacity * width // LANES, LANES), jnp.float32),
            scratch(GROUPS, ring, rows, width),
            scratch(GROUPS, ring, rows, width),
            scratch(GROUPS, hops, rows, (width - FAR) // 2),
            scratch(*low_message),
            scratch(ring, own, width),
            scratch(ring, own, width),
            scratch(hops, own, width // 2),
            dma((3,)),
            dma((3,)),
            dma((3,)),
            dma((count,)),
            dma((count,)),
            dma((count,)),
            dma((count,)),
            dma((GROUPS, hops)),
            dma((GROUPS, hops)),
            dma((GROUPS, hops)),
            dma((GROUPS, hops)),
            dma((2,)),
            dma((hops,)),
            dma((hops,)),
            dma((2,)),
            dma((2,)),
            pltpu.VMEM((FAR // LANES, ring * rows, LANES), jnp.float32),
            scratch(count, ring * capacity, FAR),
            scratch(count, PAD, FAR),
            pltpu.VMEM((ring, 8, ring * own), jnp.float32),
            scratch(count * PAD, ring * own),
            scratch(count * PAD, ring * own),
            scratch(ring, own, FAR),
            scratch(hops, own, FAR // 2),
            dma((count,)),
            dma((count,)),
            dma((ring,)),
            dma((ring,)),
            dma((hops,)),
            dma((hops,)),
        ],
        compiler_params=pltpu.CompilerParams(
            collective_id=1, has_side_effects=True, vmem_limit_bytes=VMEM_LIMIT
        ),
        name="layer",
    )(
        query_rows.T,
        key_rows.T,
        value_rows.T,
        query_gain,
        key_gain,
        sink_logits.reshape(1, -1),
        out_weight,
        expert_input,
        expert_gain.reshape(1, -1),
        routes.T,
        route_logits.T,
        gate_weight,
        up_weight,
        down_weight,
    )


def solution(mesh):
    placed = (
        P("ep", "tp"),
        P("ep", "tp"),
        P("ep", "tp"),
        P("tp", None),
        P("tp", None),
        P("tp"),
        P("tp", None),
        P(("ep", "tp"), None),
        P(),
        P(("ep", "tp"), None),
        P(("ep", "tp"), None),
        P("ep", None, "tp"),
        P("ep", None, "tp"),
        P("ep", "tp", None),
    )
    return jax.shard_map(
        on_device,
        mesh=mesh,
        in_specs=placed,
        out_specs=(P(("ep", "tp"), None), P(("ep", "tp"), None)),
        check_vma=False,
    )
```
